32 devices in a mesh: sp: 8 (over z, y), tp: 4 (over x, core).
Axes of the slice: x: 2, y: 2, z: 4, core: 2. Of those that a mesh axis runs over, the one named last changes fastest.
Arguments:
- queries: bfloat16 [4096, 2048], P('sp', 'tp'), may hold values from -6 to 6
- keys: bfloat16 [4096, 512], P('sp', 'tp'), may hold values from -6 to 6
- values: bfloat16 [4096, 512], P('sp', 'tp'), may hold values from -6 to 6
- residual: bfloat16 [4096, 2048], P(('sp', 'tp')), may hold values from -0.119628906 to 0.119628906
- out_proj: bfloat16 [2048, 2048], replicated, may hold values from -0.125 to 0.125
- query_gain: float32 [128], replicated, may hold values from 0.7 to 7
- key_gain: float32 [128], replicated, may hold values from 0.7 to 7
- norm_gain: float32 [2048], replicated, may hold values from 0.1 to 1.9
- routes: int32 [4096, 4], P(('sp', 'tp')), may hold values from 0 to 31, all different within a row; in each aligned block of 128 rows (0 to 127, 128 to 255, ...) at most 32 rows name the same one
- route_weight: float32 [4096, 4], P(('sp', 'tp')), may hold values from 0.1 to 1
- expert_gate: bfloat16 [32, 2048, 256], P(('sp', 'tp')), may hold values from -0.125 to 0.125
- expert_up: bfloat16 [32, 2048, 256], P(('sp', 'tp')), may hold values from -0.125 to 0.125
- expert_down: bfloat16 [32, 256, 2048], P(('sp', 'tp')), may hold values from -0.375 to 0.375
- shared_gate: bfloat16 [2048, 256], replicated, may hold values from -0.125 to 0.125
- shared_up: bfloat16 [2048, 256], replicated, may hold values from -0.125 to 0.125
- shared_down: bfloat16 [256, 2048], replicated, may hold values from -0.375 to 0.375
Outputs:
- layer_out: bfloat16 [4096, 2048], P(('sp', 'tp'))
The draws below stay inside these ranges and needn't reach their ends.
Inputs may be any that keep to these rules, and one draw needn't show every extreme that they name: In the rows of one device (aligned blocks of 128 tokens), no expert is named by more than 32 routes; some expert is named by exactly 32 routes of some device; the 4 experts of a token differ.
All inputs are finite; a program needn't handle non-finite values.
Results may differ from the reference program's by a relative error of at most 0.023.
The reference program's roundings to bfloat16 on the way count: a program that leaves them out, or rounds other values in their place, can miss the bound.
Values may be sent and summed in bfloat16 or wider, within the bound.
A program may use at most 128 MiB of HBM per device.

```python
import math
import jax
import jax.numpy as jnp
import numpy as np
from jax import lax

D = 2048
HEADS = 16
KV_HEADS = 4
HD = 128
EFF = 256
SFF = 256
GRID_W = 64
TOP = 4
SEQ = 4096
ROWS_DEV = 128
EXPERTS = 32
CAP = 32
N_SP = 8
N_TP = 4


def paired_draw(key):
    key_rows = jax.random.normal(jax.random.fold_in(key, 11), (SEQ, KV_HEADS * HD), jnp.float32)
    query_rows = jax.random.normal(jax.random.fold_in(key, 12), (SEQ, HEADS * HD), jnp.float32)
    return (jnp.clip(query_rows, -6.0, 6.0), jnp.clip(key_rows, -6.0, 6.0))


def draw_queries(key, part):
    return paired_draw(key)[0].astype(jnp.bfloat16)


def draw_keys(key, part):
    return paired_draw(key)[1].astype(jnp.bfloat16)


def gain_draw(key):
    return jax.random.uniform(key, (HD,), jnp.float32, 0.7, 1.3)


def draw_query_gain(key, part):
    return gain_draw(jax.random.fold_in(key, 21))


def draw_key_gain(key, part):
    return gain_draw(jax.random.fold_in(key, 22))


def block_scale(rng, shape, cuts, low, largest):
    def one(dim, blocks):
        heights = jax.random.uniform(jax.random.fold_in(jax.random.fold_in(rng, 6), dim), (blocks,), jnp.float32, low / len(cuts), largest / len(cuts))
        return jnp.repeat(jnp.exp(heights), shape[dim] // blocks).reshape((-1,) + (1,) * (len(shape) - dim - 1))

    loudness = one(*cuts[0])
    for cut in cuts[1:]:
        loudness = loudness * one(*cut)
    return loudness


def deal_out(own_key, own, number, rows, amount, top, limit, slope):
    ranking = jax.random.permutation(own_key, amount)
    heavy_load, common = portions_of(amount, rows * top, limit, slope, True), portions_of(amount, rows * top, limit, slope, False)
    places = jnp.arange(amount)

    def named(sizes, rotation):
        used = int((sizes > 0).sum())
        fixed = max(1, used // 4)
        passed = fixed + (places - fixed + rotation * (used - fixed)) % max(1, amount - fixed)
        return jnp.zeros((amount,), jnp.int32).at[ranking[jnp.where(places < fixed, places, passed)]].set(jnp.asarray(sizes, jnp.int32))

    sizes = jnp.where(number % 4 == 0, named(heavy_load, number // 4), named(common, number - number // 4 - 1))
    mixed = jax.random.permutation(jax.random.fold_in(own, 3), amount)
    source_of, taker = mixed[0:amount // 2 * 2:2], mixed[1:amount // 2 * 2:2]
    margin = jnp.minimum(sizes[source_of] - 1, limit - sizes[taker]) // 2
    margin = jnp.where((source_of == ranking[0]) | (taker == ranking[0]) | (sizes[taker] == 0), 0, jnp.maximum(margin, 0))
    passed = jax.random.randint(jax.random.fold_in(own, 4), (amount // 2,), 0, 1 << 20) % (margin + 1)
    sizes = sizes.at[source_of].add(-passed).at[taker].add(passed)
    members = jnp.searchsorted(jnp.cumsum(sizes), jnp.arange(rows * top), side="right").astype(jnp.int32)
    listing = members.reshape(top, rows).T
    listing = listing[jax.random.permutation(jax.random.fold_in(own, 1), rows)]
    rotation = jax.random.randint(jax.random.fold_in(own, 2), (rows, 1), 0, top)
    return jnp.take_along_axis(listing, (jnp.arange(top)[None, :] + rotation) % top, axis=1)


def portions_of(count, total, limit, lean, full):
    portions = [(1 << 20) // math.isqrt(standing ** lean) + 1 for standing in range(1, count + 1)]
    largest = limit if full else min(limit, max(-(-total // count), total * portions[0] // sum(portions)))
    least = 1 if total - largest >= count - 1 else 0
    given, rest = [largest] + [least] * (count - 1), total - largest - least * (count - 1)
    while rest > 0:
        movable = [i for i in range(1, count) if given[i] < largest] or [i for i in range(1, count) if given[i] < limit]
        pool, remaining = sum([portions[i] for i in movable]), rest
        for i in movable:
            extra = min(limit - given[i], max(1, remaining * portions[i] // pool), rest)
            given[i] = given[i] + extra
            rest = rest - extra
    return np.array(given)


def gaussian(key, shape, spread, reach, cuts=(), kind=jnp.bfloat16):
    loudness = block_scale(key, shape, cuts, -0.22, 0.18) if cuts else 1.0
    values = jax.random.normal(key, shape, jnp.float32) * spread * loudness
    return jnp.minimum(jnp.maximum(values, -reach), reach).astype(kind)


def setup_inputs(seed: int = 0) -> dict:
    key_of = jax.random.split(jax.random.key(seed), 17)
    queries = draw_queries(jax.random.fold_in(key_of[16], 71), 0)
    keys = draw_keys(jax.random.fold_in(key_of[16], 71), 0)
    values = gaussian(key_of[2], (SEQ, KV_HEADS * HD), 1.0, 6.0, ((0, 8), (1, 4)))
    residual = gaussian(key_of[3], (SEQ, D), 0.02, 0.119628906, ((0, 32),))
    out_proj = gaussian(key_of[4], (HEADS * HD, D), (HEADS * HD) ** -0.5, 0.125)
    query_gain = draw_query_gain(jax.random.fold_in(key_of[16], 71), 0)
    key_gain = draw_key_gain(jax.random.fold_in(key_of[16], 71), 0)
    norm_gain = jnp.clip(1.0 + 0.18 * jax.random.normal(key_of[7], (D,), jnp.float32), 0.1, 1.9)
    routes_keys = jax.random.split(jax.random.fold_in(key_of[8], 1), SEQ // ROWS_DEV)
    routes_turns = jax.random.permutation(jax.random.fold_in(key_of[8], 3), SEQ // ROWS_DEV)
    routes = jax.vmap(lambda own, number: deal_out(jax.random.fold_in(key_of[8], 2), own, number, ROWS_DEV, EXPERTS, TOP, CAP, 2))(routes_keys, routes_turns).reshape((SEQ, TOP))
    route_weight = jnp.clip(jnp.exp(math.log(1.0) - 2.3025851 * jax.random.uniform(key_of[9], (SEQ, TOP), jnp.float32) ** block_scale(key_of[9], (SEQ, TOP), ((0, 32),), -0.2, 0.2)), 0.1, 1.0)
    expert_gate = gaussian(key_of[10], (EXPERTS, D, EFF), D ** -0.5, 0.125, ((0, 32),))
    expert_up = gaussian(key_of[11], (EXPERTS, D, EFF), D ** -0.5, 0.125, ((0, 32),))
    expert_down = gaussian(key_of[12], (EXPERTS, EFF, D), EFF ** -0.5, 0.375, ((0, 32),))
    shared_gate = gaussian(key_of[13], (D, SFF), D ** -0.5, 0.125)
    shared_up = gaussian(key_of[14], (D, SFF), D ** -0.5, 0.125)
    shared_down = gaussian(key_of[15], (SFF, D), SFF ** -0.5, 0.375)
    return dict(queries=queries, keys=keys, values=values, residual=residual, out_proj=out_proj, query_gain=query_gain, key_gain=key_gain, norm_gain=norm_gain, routes=routes, route_weight=route_weight, expert_gate=expert_gate, expert_up=expert_up, expert_down=expert_down, shared_gate=shared_gate, shared_up=shared_up, shared_down=shared_down)


EPS = 1e-06
THETA = 10000.0

def rotate_pairs(block, cosine, sine):
    first, second = jnp.split(block, 2, axis=-1)
    return jnp.concatenate([first * cosine - second * sine, second * cosine + first * sine], axis=-1)

def normed_rotary(source, gain, heads, offset):
    count = source.shape[0]
    width = gain.shape[0]
    values_f = source.astype(jnp.float32).reshape(count, heads, width)
    values_f = values_f * lax.rsqrt(lax.optimization_barrier(jnp.mean(values_f * values_f, axis=-1, keepdims=True)) + EPS) * gain
    position = offset + jnp.arange(count, dtype=jnp.int32)
    grid_row = (position // GRID_W).astype(jnp.float32)
    grid_col = (position % GRID_W).astype(jnp.float32)
    quarter = width // 4
    inverse = jnp.power(THETA, -4.0 * jnp.arange(quarter, dtype=jnp.float32) / width)
    row_angle = (grid_row[:, None] * inverse[None, :])[:, None, :]
    col_angle = (grid_col[:, None] * inverse[None, :])[:, None, :]
    row_half, col_half = jnp.split(values_f, 2, axis=-1)
    turned = jnp.concatenate([rotate_pairs(row_half, jnp.cos(row_angle), jnp.sin(row_angle)), rotate_pairs(col_half, jnp.cos(col_angle), jnp.sin(col_angle))], axis=-1)
    return turned.reshape(count, heads * width).astype(jnp.bfloat16)

def reference(queries, keys, values, residual, out_proj, query_gain, key_gain, norm_gain, routes, route_weight, expert_gate, expert_up, expert_down, shared_gate, shared_up, shared_down):
    tokens = queries.shape[0]
    width = query_gain.shape[0]
    group = HEADS // KV_HEADS
    scale = 1.0 / math.sqrt(width)
    q_rot = normed_rotary(queries, query_gain, HEADS, 0)
    k_rot = normed_rotary(keys, key_gain, KV_HEADS, 0)
    key_f = k_rot.reshape(tokens, KV_HEADS, width).astype(jnp.float32).transpose(1, 0, 2)
    value_f = values.reshape(tokens, KV_HEADS, width).astype(jnp.float32).transpose(1, 0, 2)
    block = math.gcd(tokens, 512)
    q_blocks = q_rot.reshape(tokens // block, block, KV_HEADS, group, width).transpose(0, 2, 3, 1, 4)

    def attend_head(operands):
        query_part, key_part, value_part = operands
        scores = jnp.einsum('gqd,kd->gqk', query_part.astype(jnp.float32), key_part) * scale
        top = lax.optimization_barrier(jnp.max(scores, axis=-1, keepdims=True))
        weights = jnp.exp(scores - top)
        denom = lax.optimization_barrier(jnp.sum(weights, axis=-1, keepdims=True))
        rounded = weights.astype(jnp.bfloat16).astype(jnp.float32)
        summed = jnp.einsum('gqk,kd->gqd', rounded, value_part)
        return (summed / denom).astype(jnp.bfloat16)

    def attend_block(query_block):
        return lax.map(attend_head, (query_block, key_f, value_f))
    outputs = lax.map(attend_block, q_blocks)
    attn_heads = outputs.transpose(0, 3, 1, 2, 4).reshape(tokens, HEADS * width)
    projected = jnp.dot(attn_heads, out_proj, preferred_element_type=jnp.float32)
    hidden1 = (residual.astype(jnp.float32) + projected).astype(jnp.bfloat16)
    hidden_f = hidden1.astype(jnp.float32)
    normed = (hidden_f * lax.rsqrt(lax.optimization_barrier(jnp.mean(hidden_f * hidden_f, axis=-1, keepdims=True)) + EPS) * norm_gain).astype(jnp.bfloat16)
    shared_hidden = (jax.nn.silu(jnp.dot(normed, shared_gate, preferred_element_type=jnp.float32)) * jnp.dot(normed, shared_up, preferred_element_type=jnp.float32)).astype(jnp.bfloat16)
    shared_out = jnp.dot(shared_hidden, shared_down, preferred_element_type=jnp.float32)
    pairs = tokens * TOP
    flat_routes = routes.reshape(pairs)
    bound = N_SP * N_TP * CAP
    padded = jnp.concatenate([normed, jnp.zeros((1, normed.shape[1]), jnp.bfloat16)], axis=0)

    def one_expert(expert, buffer):
        picked = jnp.nonzero(flat_routes == expert, size=bound, fill_value=pairs)[0].astype(jnp.int32)
        rows = padded[picked // TOP]
        hidden_e = (jax.nn.silu(jnp.dot(rows, expert_gate[expert], preferred_element_type=jnp.float32)) * jnp.dot(rows, expert_up[expert], preferred_element_type=jnp.float32)).astype(jnp.bfloat16)
        result = jnp.dot(hidden_e, expert_down[expert], preferred_element_type=jnp.float32).astype(jnp.bfloat16)
        return buffer.at[picked].set(result)
    buffer = lax.fori_loop(0, EXPERTS, one_expert, jnp.zeros((pairs + 1, normed.shape[1]), jnp.bfloat16))
    routed = buffer[:pairs].reshape(tokens, TOP, normed.shape[1]).astype(jnp.float32)
    mixed = jnp.einsum('tk,tkd->td', route_weight, routed) + shared_out
    return (hidden_f + mixed).astype(jnp.bfloat16)
```

```python
import functools
import math

import jax
import jax.numpy as jnp
from jax import lax
from jax.experimental import pallas as pl
from jax.experimental.pallas import tpu as pltpu
from jax.sharding import PartitionSpec as P

GRID_W = 64
MESH = pl.DeviceIdType.MESH


EPS = 1e-06
THETA = 10000.0


def norm_rotate(block, gain, cosine, sine):
    mean = jnp.mean(block * block, axis=-1, keepdims=True)
    block = block * lax.rsqrt(mean + EPS) * gain
    quarter = block.shape[-1] // 4
    lane = lax.broadcasted_iota(jnp.int32, block.shape, 1)
    after = pltpu.roll(block, 3 * quarter, 1)
    before = pltpu.roll(block, quarter, 1)
    partner = jnp.where((lane // quarter) % 2 == 0, after, before)
    return (block * cosine + partner * sine).astype(jnp.bfloat16)


def plane_peer(z, d, planes):
    if planes == 4:
        return (z + 1 - 2 * (z % 2), z + 2 - 4 * (z // 2), 3 - z)[d - 1]
    return planes - 1 - z


def attention_kernel(
    n_sp, n_tp, planes, group, trade,
    q_ref, k_ref, v_ref, cos_ref, sin_ref, qg_ref, kg_ref, *rest,
):
    if trade:
        own_weights, out_ref, new_weights, rest = rest[:3], rest[3], rest[4:7], rest[7:]
    else:
        out_ref, rest = rest[0], rest[1:]
    (
        held, q_rot, top, total, accum, rows_out,
        send_z, send_y, recv_kv, send_o, recv_o,
    ) = rest[:11]
    per = n_sp // planes
    me_sp = lax.axis_index("sp")
    me_tp = lax.axis_index("tp")
    z, y = me_sp // per, me_sp % per
    tok, width = k_ref.shape
    piece = tok // n_tp
    lanes = group * width
    held[me_sp, 0] = norm_rotate(
        k_ref[...].astype(jnp.float32), kg_ref[...], cos_ref[...], sin_ref[...]
    )
    held[me_sp, 1] = v_ref[...]
    barrier = pltpu.get_barrier_semaphore()
    for d in range(1, n_sp):
        pl.semaphore_signal(
            barrier, inc=1, device_id={"sp": lax.rem(me_sp + d, n_sp)}, device_id_type=MESH
        )
    for d in range(1, n_tp):
        pl.semaphore_signal(
            barrier, inc=1, device_id={"tp": lax.rem(me_tp + d, n_tp)}, device_id_type=MESH
        )
    pl.semaphore_wait(barrier, n_sp + n_tp - 2)

    def block_copy(block, target, sem):
        return pltpu.make_async_remote_copy(
            src_ref=held.at[block], dst_ref=held.at[block],
            send_sem=sem, recv_sem=recv_kv.at[block],
            device_id={"sp": target}, device_id_type=MESH,
        )

    def to_plane(slot, block):
        for d in range(1, per):
            block_copy(block, z * per + lax.rem(y + d, per), send_y.at[slot, d - 1]).start()

    def weight_copy(i, rows):
        x, k = me_tp // 2, lax.rem(me_tp, 2)
        return pltpu.make_async_remote_copy(
            src_ref=own_weights[i].at[:, rows], dst_ref=new_weights[i].at[:, rows],
            send_sem=rest[11].at[i], recv_sem=rest[12].at[i],
            device_id={
                "sp": z * per + y + k * (1 - 2 * y),
                "tp": (x + (1 - k) * (1 - 2 * x)) * 2 + k,
            },
            device_id_type=MESH,
        )

    def trade_weights(n):
        for piece_number in {0: (0, 1), n_sp - 1: ()}.get(n, (n + 1,)):
            for i in range(3 if trade else 0):
                size = own_weights[i].shape[1] // n_sp
                weight_copy(i, pl.ds(piece_number * size, size)).start()

    for d in range(1, planes):
        if d == 1:
            block_copy(me_sp, plane_peer(z, d, planes) * per + y, send_z.at[d - 1]).start()
            to_plane(0, me_sp)
        else:
            block_copy(me_sp, plane_peer(z, d, planes) * per + y, send_z.at[d - 1]).start()
    for j in range(n_tp):
        rows = pl.ds(j * piece, piece)
        for h in range(group):
            q_rot[j, pl.ds(h * piece, piece), :] = norm_rotate(
                q_ref[rows, pl.ds(h * width, width)].astype(jnp.float32),
                qg_ref[...], cos_ref[rows, :], sin_ref[rows, :],
            )
    top[...] = jnp.full(top.shape, -1e30, jnp.float32)
    total[...] = jnp.zeros(total.shape, jnp.float32)
    accum[...] = jnp.zeros(accum.shape, jnp.float32)
    factor = math.log2(math.e) / math.sqrt(width)
    repeat = tok // width

    def attend(block, j):
        scores = lax.dot_general(
            q_rot[j], held[block, 0], (((1,), (1,)), ((), ())),
            preferred_element_type=jnp.float32,
        )
        old = top[j]
        new = jnp.maximum(old, jnp.max(scores, axis=1, keepdims=True))
        weights = jnp.exp2((scores - jnp.concatenate([new] * repeat, axis=1)) * factor)
        alpha = jnp.exp2((old - new) * factor)
        part = weights[:, :width]
        for r in range(1, repeat):
            part = part + weights[:, r * width:(r + 1) * width]
        summed = total[j] * alpha + part
        added = jnp.dot(
            weights.astype(jnp.bfloat16), held[block, 1], preferred_element_type=jnp.float32
        )
        return new, summed, accum[j] * alpha + added

    def out_copy(j):
        return pltpu.make_async_remote_copy(
            src_ref=rows_out.at[j],
            dst_ref=out_ref.at[:, pl.ds(pl.multiple_of(me_tp * lanes, 128), lanes)],
            send_sem=send_o.at[j], recv_sem=recv_o.at[me_tp],
            device_id={"tp": j}, device_id_type=MESH,
        )

    def step(block):
        @pl.loop(0, n_tp)
        def _(j):
            new, summed, acc = attend(block, j)
            top[j] = new
            total[j] = summed
            accum[j] = acc

    def arrive(block):
        block_copy(block, me_sp, send_z.at[0]).wait_recv()

    def others(plane, n):
        for d in range(1, per):
            block = plane * per + lax.rem(y + d, per)
            arrive(block)
            trade_weights(n)
            step(block)

    trade_weights(0)
    step(me_sp)
    previous = z
    for d in range(1, planes):
        plane = plane_peer(z, d, planes)
        block = plane * per + y
        arrive(block)
        to_plane(d, block)
        others(previous, 2 * d - 1)
        trade_weights(2 * d)
        step(block)
        previous = plane
    others(previous, 2 * planes - 1)

    for d in range(n_tp):
        j = lax.rem(me_tp + 1 + d, n_tp)
        result = accum[j] / jnp.sum(total[j], axis=1, keepdims=True)
        result = result.astype(jnp.bfloat16)
        for h in range(group):
            rows_out[j, :, pl.ds(h * width, width)] = result[h * piece:(h + 1) * piece]
        if d < n_tp - 1:
            out_copy(j).start()
        else:
            for h in range(group):
                out_ref[:, pl.ds(pl.multiple_of(me_tp * lanes + h * width, 128), width)] = result[
                    h * piece:(h + 1) * piece
                ]
    for d in range(1, n_tp):
        source = lax.rem(me_tp + d, n_tp)
        pltpu.make_async_remote_copy(
            src_ref=rows_out.at[source],
            dst_ref=out_ref.at[:, pl.ds(pl.multiple_of(source * lanes, 128), lanes)],
            send_sem=send_o.at[source], recv_sem=recv_o.at[source],
            device_id={"tp": source}, device_id_type=MESH,
        ).wait()
    for d in range(1, planes):
        block_copy(me_sp, me_sp, send_z.at[d - 1]).wait_send()
    for slot in range(planes):
        for d in range(1, per):
            block_copy(me_sp, me_sp, send_y.at[slot, d - 1]).wait_send()
    for i in range(3 if trade else 0):
        weight_copy(i, pl.ds(0, own_weights[i].shape[1])).wait()


def attention(mesh_sp, mesh_tp, queries, keys, values, query_gain, key_gain, weights):
    tok, width = keys.shape
    group = queries.shape[1] // width
    planes = 4 if mesh_sp % 4 == 0 else 2
    per = mesh_sp // planes
    piece = tok // mesh_tp
    quarter = width // 4
    inverse = jnp.power(THETA, -4.0 * jnp.arange(quarter, dtype=jnp.float32) / width)
    start = lax.axis_index("sp") * tok
    grid_rows = tok // GRID_W
    row_angle = (start // GRID_W + jnp.arange(grid_rows)).astype(jnp.float32)[:, None] * inverse
    col_angle = jnp.arange(GRID_W).astype(jnp.float32)[:, None] * inverse

    def spread(row_part, col_part, sign):
        row_part = jnp.broadcast_to(row_part[:, None, :], (grid_rows, GRID_W, quarter))
        col_part = jnp.broadcast_to(col_part[None, :, :], (grid_rows, GRID_W, quarter))
        return jnp.concatenate(
            [sign * row_part, row_part, sign * col_part, col_part], axis=-1
        ).reshape(tok, width)

    tables = lax.optimization_barrier(
        (jnp.cos(row_angle), jnp.cos(col_angle), jnp.sin(row_angle), jnp.sin(col_angle))
    )
    cosine = spread(tables[0], tables[1], 1.0)
    sine = spread(tables[2], tables[3], -1.0)
    vmem = pl.BlockSpec(memory_space=pltpu.VMEM)
    anywhere = pl.BlockSpec(memory_space=pl.ANY)
    trade = bool(weights)
    return pl.pallas_call(
        functools.partial(attention_kernel, mesh_sp, mesh_tp, planes, group, trade),
        out_shape=[jax.ShapeDtypeStruct((piece, mesh_tp * group * width), jnp.bfloat16)]
        + [jax.ShapeDtypeStruct(w.shape, w.dtype) for w in weights],
        in_specs=[vmem] * 7 + [anywhere] * len(weights),
        out_specs=[vmem] + [anywhere] * len(weights),
        scratch_shapes=[
            pltpu.VMEM((mesh_sp, 2, tok, width), jnp.bfloat16),
            pltpu.VMEM((mesh_tp, group * piece, width), jnp.bfloat16),
            pltpu.VMEM((mesh_tp, group * piece, width), jnp.float32),
            pltpu.VMEM((mesh_tp, group * piece, width), jnp.float32),
            pltpu.VMEM((mesh_tp, group * piece, width), jnp.float32),
            pltpu.VMEM((mesh_tp, piece, group * width), jnp.bfloat16),
            pltpu.SemaphoreType.DMA((planes - 1,)),
            pltpu.SemaphoreType.DMA((planes, max(per - 1, 1))),
            pltpu.SemaphoreType.DMA((mesh_sp,)),
            pltpu.SemaphoreType.DMA((mesh_tp,)),
            pltpu.SemaphoreType.DMA((mesh_tp,)),
        ] + [pltpu.SemaphoreType.DMA((3,))] * (2 if trade else 0),
        compiler_params=pltpu.CompilerParams(
            collective_id=0, has_side_effects=True, vmem_limit_bytes=40 * 2**20
        ),
        name="attention",
    )(
        queries, keys, values, cosine, sine,
        query_gain.reshape(1, width), key_gain.reshape(1, width), *weights,
    )


def expert_kernel(
    n_sp, n_tp, planes, cap, top_count, chunks,
    info_ref, normed_ref, hidden_ref, gate_ref, up_ref, down_ref,
    sgate_ref, sup_ref, sdown_ref, out_ref,
    info, gathered, sent, arrived, answers, returned, partial, sums,
    place, combine, acc, hid,
    s_info, r_info, s_z, r_z, s_in, r_in, s_back, r_back, s_sum, r_sum,
):
    per = n_sp // planes
    team = per * n_tp
    me_sp = lax.axis_index("sp")
    me_tp = lax.axis_index("tp")
    z, y = me_sp // per, me_sp % per
    me = y * n_tp + me_tp
    rows = normed_ref.shape[0]
    wide = normed_ref.shape[1] // chunks
    share = planes * cap
    slots = team * share
    tile = math.gcd(slots, 256)

    def in_plane(p):
        return {"sp": z * per + p // n_tp, "tp": p % n_tp}

    def at_plane(d):
        return {"sp": plane_peer(z, d, planes) * per + y}

    def block(p, size):
        return pl.ds(pl.multiple_of(p * size, size), size)

    def remote(src, dst, send, recv, target):
        return pltpu.make_async_remote_copy(
            src_ref=src, dst_ref=dst, send_sem=send, recv_sem=recv,
            device_id=target, device_id_type=MESH,
        )

    def cols(c):
        return pl.ds(c * wide, wide)

    barrier = pltpu.get_barrier_semaphore()

    @pl.loop(1, team)
    def _(d):
        pl.semaphore_signal(
            barrier, inc=1, device_id=in_plane(lax.rem(me + d, team)), device_id_type=MESH
        )

    for d in range(1, planes):
        pl.semaphore_signal(barrier, inc=1, device_id=at_plane(d), device_id_type=MESH)
    pl.semaphore_wait(barrier, team + planes - 2)

    def info_copy(d, source):
        return remote(info_ref, info.at[source], s_info.at[d], r_info.at[source], at_plane(d))

    def z_copy(c, d, source):
        return remote(
            normed_ref.at[:, cols(c)], gathered.at[c, block(source, rows)],
            s_z.at[c, d], r_z.at[c, source], at_plane(d),
        )

    def in_copy(c, p, source):
        return remote(
            sent.at[c, block(p, share)], arrived.at[c, block(source, share)],
            s_in.at[c, p], r_in.at[c, source], in_plane(p),
        )

    def back_copy(c, p, source):
        return remote(
            answers.at[c, block(p, share)], returned.at[c, block(source, share)],
            s_back.at[c, p], r_back.at[c, source], in_plane(p),
        )

    def sum_copy(c, d, source):
        return remote(
            partial.at[c, block(plane_peer(z, d, planes), rows)], sums.at[c, source],
            s_sum.at[c, d], r_sum.at[c, source], at_plane(d),
        )

    for d in range(1, planes):
        info_copy(d, z).start()
    for c in range(chunks):
        for d in range(1, planes):
            z_copy(c, d, z).start()
        gathered[c, block(z, rows)] = normed_ref[:, cols(c)]
    info[z] = info_ref[...]

    shared_gate = jnp.dot(normed_ref[...], sgate_ref[...], preferred_element_type=jnp.float32)
    shared_up = jnp.dot(normed_ref[...], sup_ref[...], preferred_element_type=jnp.float32)
    shared_hid = (jax.nn.silu(shared_gate) * shared_up).astype(jnp.bfloat16)
    for c in range(chunks):
        out_ref[:, cols(c)] = jnp.dot(
            shared_hid, sdown_ref[:, cols(c)], preferred_element_type=jnp.float32
        ) + hidden_ref[:, cols(c)].astype(jnp.float32)

    number = lax.broadcasted_iota(jnp.int32, (slots, rows), 0)
    owner = (number // cap) % planes
    slot = ((z * team + number // share) * cap + number % cap).astype(jnp.float32)
    for d in range(1, planes):
        info_copy(d, plane_peer(z, d, planes)).wait_recv()
    for plane in range(planes):
        wanted = jnp.where(owner == plane, slot, -1.0)
        ones = jnp.zeros((slots, rows), jnp.float32)
        shares = jnp.zeros((slots, rows), jnp.float32)
        for k in range(top_count):
            match = wanted == info[plane, k:k + 1, :]
            ones = jnp.where(match, 1.0, ones)
            shares = jnp.where(match, info[plane, top_count + k:top_count + k + 1, :], shares)
        place[:, pl.ds(plane * rows, rows)] = ones.astype(jnp.bfloat16)
        combine[pl.ds(plane * rows, rows), :] = shares.T.astype(jnp.bfloat16)

    for c in range(chunks):
        for d in range(1, planes):
            z_copy(c, d, plane_peer(z, d, planes)).wait_recv()

        @pl.loop(0, slots // tile)
        def _(i):
            sent[c, block(i, tile)] = jnp.dot(
                place[block(i, tile), :], gathered[c], preferred_element_type=jnp.float32
            ).astype(jnp.bfloat16)

        @pl.loop(1, team)
        def _(d):
            in_copy(c, lax.rem(me + d, team), me).start()

        arrived[c, block(me, share)] = sent[c, block(me, share)]

    inner = gate_ref.shape[2]
    for c in range(chunks):
        @pl.loop(1, team)
        def _(d):
            source = lax.rem(me + d, team)
            in_copy(c, source, source).wait_recv()

        @pl.loop(0, slots // tile)
        def _(i):
            part = arrived[c, block(i, tile)]
            gate = jnp.dot(part, gate_ref[0, cols(c), :], preferred_element_type=jnp.float32)
            up = jnp.dot(part, up_ref[0, cols(c), :], preferred_element_type=jnp.float32)
            if c > 0:
                gate = gate + acc[block(i, tile), pl.ds(0, inner)]
                up = up + acc[block(i, tile), pl.ds(inner, inner)]
            if c < chunks - 1:
                acc[block(i, tile), pl.ds(0, inner)] = gate
                acc[block(i, tile), pl.ds(inner, inner)] = up
            else:
                hid[block(i, tile), :] = (jax.nn.silu(gate) * up).astype(jnp.bfloat16)

    for c in range(chunks):
        @pl.loop(0, slots // tile)
        def _(i):
            answers[c, block(i, tile)] = jnp.dot(
                hid[block(i, tile), :], down_ref[0, :, cols(c)],
                preferred_element_type=jnp.float32,
            ).astype(jnp.bfloat16)

        @pl.loop(1, team)
        def _(d):
            back_copy(c, lax.rem(me + d, team), me).start()

        returned[c, block(me, share)] = answers[c, block(me, share)]

    for c in range(chunks):
        @pl.loop(1, team)
        def _(d):
            source = lax.rem(me + d, team)
            back_copy(c, source, source).wait_recv()

        @pl.loop(0, planes)
        def _(i):
            partial[c, block(i, rows)] = jnp.dot(
                combine[block(i, rows), :], returned[c], preferred_element_type=jnp.float32
            ).astype(jnp.bfloat16)

        for d in range(1, planes):
            sum_copy(c, d, z).start()
        sums[c, z] = partial[c, block(z, rows)]

    for c in range(chunks):
        for d in range(1, planes):
            sum_copy(c, d, plane_peer(z, d, planes)).wait_recv()
        result = out_ref[:, cols(c)]
        for plane in range(planes):
            result = result + sums[c, plane].astype(jnp.float32)
        out_ref[:, cols(c)] = result

    for d in range(1, planes):
        info_copy(d, z).wait_send()
    for c in range(chunks):
        for d in range(1, planes):
            z_copy(c, d, z).wait_send()
            sum_copy(c, d, z).wait_send()

        @pl.loop(1, team)
        def _(d):
            p = lax.rem(me + d, team)
            in_copy(c, p, me).wait_send()
            back_copy(c, p, me).wait_send()


def routed_experts(
    info, normed, hidden1, gate, up, down, shared_gate, shared_up, shared_down, cap
):
    n_sp, n_tp = lax.axis_size("sp"), lax.axis_size("tp")
    rows, model = normed.shape
    planes = 4 if n_sp % 4 == 0 else 2
    team = n_sp // planes * n_tp
    chunks = 8
    wide = model // chunks
    slots = team * planes * cap
    inner = gate.shape[2]
    top_count = info.shape[0] // 2
    vmem = pl.BlockSpec(memory_space=pltpu.VMEM)
    dma = pltpu.SemaphoreType.DMA
    return pl.pallas_call(
        functools.partial(expert_kernel, n_sp, n_tp, planes, cap, top_count, chunks),
        out_shape=jax.ShapeDtypeStruct((rows, model), jnp.float32),
        in_specs=[vmem] * 9,
        out_specs=vmem,
        scratch_shapes=[
            pltpu.VMEM((planes,) + info.shape, jnp.float32),
            pltpu.VMEM((chunks, planes * rows, wide), jnp.bfloat16),
            pltpu.VMEM((chunks, slots, wide), jnp.bfloat16),
            pltpu.VMEM((chunks, slots, wide), jnp.bfloat16),
            pltpu.VMEM((chunks, slots, wide), jnp.bfloat16),
            pltpu.VMEM((chunks, slots, wide), jnp.bfloat16),
            pltpu.VMEM((chunks, planes * rows, wide), jnp.bfloat16),
            pltpu.VMEM((chunks, planes, rows, wide), jnp.bfloat16),
            pltpu.VMEM((slots, planes * rows), jnp.bfloat16),
            pltpu.VMEM((planes * rows, slots), jnp.bfloat16),
            pltpu.VMEM((slots, 2 * inner), jnp.float32),
            pltpu.VMEM((slots, inner), jnp.bfloat16),
            dma((planes,)), dma((planes,)),
            dma((chunks, planes)), dma((chunks, planes)),
            dma((chunks, team)), dma((chunks, team)),
            dma((chunks, team)), dma((chunks, team)),
            dma((chunks, planes)), dma((chunks, planes)),
        ],
        compiler_params=pltpu.CompilerParams(
            collective_id=1, has_side_effects=True, vmem_limit_bytes=56 * 2**20
        ),
        name="experts",
    )(info, normed, hidden1, gate, up, down, shared_gate, shared_up, shared_down)


def traded_kernel(
    n_tp, planes, cap, chunks,
    info_ref, normed_ref, hidden_ref, *rest,
):
    weights_in, shared_in, out_ref, rest = rest[:6], rest[6:9], rest[9], rest[10:]
    (
        w_gate, w_up, w_down, w_shared_gate, w_shared_up, w_shared_down,
        info, gathered, sent, arrived, answers, returned, partial, relayed, passed, sums,
        place, combine, acc, hid, base,
        s_load, s_info, r_info, s_z, r_z, s_in, r_in, s_back, r_back, s_sum, r_sum, s_far, r_far,
    ) = rest
    me_sp = lax.axis_index("sp")
    me_tp = lax.axis_index("tp")
    z, y = me_sp // 2, lax.rem(me_sp, 2)
    x, k = me_tp // 2, lax.rem(me_tp, 2)
    rows, model = normed_ref.shape
    wide = model // chunks
    middle = jnp.logical_or(z == 1, z == 2)
    edge = jnp.logical_or(z == 0, z == 3)

    def flip(bit, by):
        return bit + by * (1 - 2 * bit)

    def device(yy, xx, kk):
        return {"sp": z * 2 + yy, "tp": xx * 2 + kk}

    def at_plane(r):
        other = (z, flip(lax.rem(z, 2), 1) + z // 2 * 2, lax.rem(z + 2, 4), 3 - z)[r]
        return {"sp": other * 2 + y}

    def remote(src, dst, send, recv, target):
        return pltpu.make_async_remote_copy(
            src_ref=src, dst_ref=dst, send_sem=send, recv_sem=recv,
            device_id=target, device_id_type=MESH,
        )

    def cols(c):
        return pl.ds(c * wide, wide)

    loads = [
        pltpu.make_async_copy(src, dst, s_load.at[i])
        for i, (src, dst) in enumerate(
            zip(
                tuple(shared_in) + tuple(weights_in),
                (w_shared_gate, w_shared_up, w_shared_down)
                + tuple(w.at[pl.ds(n, 1)] for n in range(2) for w in (w_gate, w_up, w_down)),
            )
        )
    ]
    for load in loads:
        load.start()

    partner = device(y, x, 1 - k)
    far_y = device(1 - y, x, 0)
    far_x = device(y, 1 - x, 1)
    sources = [device(flip(y, 1 - k), flip(x, k), core) for core in range(2)]
    barrier = pltpu.get_barrier_semaphore()
    for target in (
        partner, far_y, far_x, device(flip(y, 1 - k), flip(x, k), 1 - k),
        at_plane(1), at_plane(2), at_plane(3),
    ):
        pl.semaphore_signal(barrier, inc=1, device_id=target, device_id_type=MESH)
    pl.semaphore_wait(barrier, 7)

    def info_copy(r):
        return remote(info_ref, info.at[r], s_info.at[r], r_info.at[r], at_plane(r))

    def z_copy(c, r):
        return remote(
            normed_ref.at[:, cols(c)], gathered.at[c, r], s_z.at[c, r], r_z.at[c, r], at_plane(r)
        )

    def z_pass(c):
        return remote(
            gathered.at[c, 2], gathered.at[c, 3], s_far.at[c], r_z.at[c, 3], at_plane(1)
        )

    def in_copy(c, t):
        place_there = 1 if t == 1 else 2 + k
        return remote(
            sent.at[c, t - 1], arrived.at[c, :, place_there],
            s_in.at[c, t], r_in.at[c, place_there], (None, partner, far_y, far_x)[t],
        )

    def back_copy(c, i):
        place_there = 1 if i == 1 else 2 + k
        return remote(
            answers.at[c, :, i], returned.at[c, place_there],
            s_back.at[c, i], r_back.at[c, place_there],
            partner if i == 1 else sources[i - 2],
        )

    def sum_copy(c, r, src):
        return remote(src, sums.at[c, r], s_sum.at[c, r], r_sum.at[c, r], at_plane(r))

    def far_copy(c):
        return remote(partial.at[c, 3], relayed.at[c], s_sum.at[c, 3], r_far.at[c], at_plane(1))

    for r in range(1, planes):
        info_copy(r).start()

    def z_start(c):
        z_copy(c, 1).start()
        z_copy(c, 2).start()

        @pl.when(middle)
        def _():
            z_copy(c, 3).start()

    z_start(0)
    z_start(1)
    info[0] = info_ref[...]

    for i in range(3):
        loads[i].wait()
    shared_gate = jnp.dot(normed_ref[...], w_shared_gate[...], preferred_element_type=jnp.float32)
    shared_up = jnp.dot(normed_ref[...], w_shared_up[...], preferred_element_type=jnp.float32)
    shared_hid = (jax.nn.silu(shared_gate) * shared_up).astype(jnp.bfloat16)
    for c in range(chunks):
        base[:, cols(c)] = jnp.dot(
            shared_hid, w_shared_down[:, cols(c)], preferred_element_type=jnp.float32
        ) + hidden_ref[:, cols(c)].astype(jnp.float32)

    before = (
        lax.broadcasted_iota(jnp.int32, (rows, rows), 0)
        < lax.broadcasted_iota(jnp.int32, (rows, rows), 1)
    ).astype(jnp.float32).astype(jnp.bfloat16)
    count = lax.broadcasted_iota(jnp.int32, (cap, rows), 0).astype(jnp.float32)
    top_count = info_ref.shape[0] // 2
    members = []
    for t in range(4):
        core = (k, 1 - k, 0, 1)[t]
        far = t // 2
        for e in range(2):
            yy = flip(y, far * (1 - core) + e * core)
            xx = flip(x, far * core + e * (1 - core))
            members.append((z * 2 + yy) * n_tp + xx * 2 + core)
    for r in range(1, planes):
        info_copy(r).wait_recv()
    for r in range(planes):
        hits, shares = [], []
        for member in members:
            wanted = jnp.full((1, rows), member, jnp.int32).astype(jnp.float32)
            hit = jnp.zeros((1, rows), jnp.float32)
            share = jnp.zeros((1, rows), jnp.float32)
            for j in range(top_count):
                match = info[r, j:j + 1, :] == wanted
                hit = jnp.where(match, 1.0, hit)
                share = jnp.where(match, info[r, top_count + j:top_count + j + 1, :], share)
            hits.append(hit)
            shares.append(share)
        stacked = jnp.concatenate(hits, axis=0)
        earlier = jnp.dot(stacked.astype(jnp.bfloat16), before, preferred_element_type=jnp.float32)
        earlier = jnp.where(stacked > 0.5, earlier, -1.0)
        spread = []
        for n in range(len(members)):
            ones = (earlier[n:n + 1, :] == count).astype(jnp.float32)
            place[r, pl.ds(n * cap, cap), :] = ones.astype(jnp.bfloat16)
            spread.append(ones * shares[n])
        combine[r] = jnp.concatenate(spread, axis=0).T.astype(jnp.bfloat16)

    inner = w_gate.shape[2]

    def open_chunks(first, last):
        for c in range(first, last):
            remote(
                sent.at[c, 0], arrived.at[c, :, 1], s_in.at[c, 1], r_in.at[c, 1], partner
            ).wait_recv()
            for i in (2, 3):
                remote(
                    sent.at[c, 0], arrived.at[c, :, i], s_in.at[c, 1], r_in.at[c, i], partner
                ).wait_recv()
        for e in range(2):
            @pl.loop(0, 2)
            def _(h):
                gate = up = None
                for c in range(first, last):
                    part = arrived[c, e, pl.ds(h * 2, 2)].reshape(2 * planes * cap, wide)
                    more_gate = jnp.dot(
                        part, w_gate[e, cols(c), :], preferred_element_type=jnp.float32
                    )
                    more_up = jnp.dot(
                        part, w_up[e, cols(c), :], preferred_element_type=jnp.float32
                    )
                    gate = more_gate if gate is None else gate + more_gate
                    up = more_up if up is None else up + more_up
                if first > 0:
                    gate = gate + acc[e, h, :, pl.ds(0, inner)]
                    up = up + acc[e, h, :, pl.ds(inner, inner)]
                if last < chunks:
                    acc[e, h, :, pl.ds(0, inner)] = gate
                    acc[e, h, :, pl.ds(inner, inner)] = up
                else:
                    hid[e, h] = (jax.nn.silu(gate) * up).astype(jnp.bfloat16)

    for c in range(chunks):
        if c + 2 < chunks:
            z_start(c + 2)
        z_copy(c, 2).wait_recv()

        @pl.when(middle)
        def _():
            z_pass(c).start()

        z_copy(c, 1).wait_recv()
        z_copy(c, 3).wait_recv()
        for r in range(planes):
            source = normed_ref[:, cols(c)] if r == 0 else gathered[c, r]
            picked = jnp.dot(place[r], source, preferred_element_type=jnp.float32).astype(
                jnp.bfloat16
            )
            for t in range(4):
                for e in range(2):
                    part = picked[(2 * t + e) * cap:(2 * t + e + 1) * cap]
                    if t == 0:
                        arrived[c, e, 0, r] = part
                    else:
                        sent[c, t - 1, e, r] = part
        for t in (2, 3, 1):
            in_copy(c, t).start()
        if c == 1:
            for load in loads[3:]:
                load.wait()
        if c % 2 == 1 and c > 1:
            open_chunks(c - 3, c - 1)
    open_chunks(chunks - 2, chunks)

    for c in range(chunks):
        for e in range(2):
            @pl.loop(0, 2)
            def _(h):
                result = jnp.dot(
                    hid[e, h], w_down[e, :, cols(c)], preferred_element_type=jnp.float32
                ).astype(jnp.bfloat16).reshape(2, planes, cap, wide)
                answers[c, e, pl.ds(h * 2, 2)] = result
        for i in (2, 3, 1):
            back_copy(c, i).start()
        for e in range(2):
            returned[c, 0, e] = answers[c, e, 0]

    def sum_relay(c):
        @pl.when(middle)
        def _():
            far_copy(c).wait_recv()
            passed[c] = (
                partial[c, 2].astype(jnp.float32) + relayed[c].astype(jnp.float32)
            ).astype(jnp.bfloat16)
            sum_copy(c, 2, passed.at[c]).start()

    for c in range(chunks):
        for t in range(1, 4):
            remote(
                answers.at[c, :, 1], returned.at[c, t], s_back.at[c, 1], r_back.at[c, t], partner
            ).wait_recv()
        for r in (3, 2, 1, 0):
            back = jnp.concatenate(
                [returned[c, t, e, r] for t in range(4) for e in range(2)], axis=0
            )
            partial[c, r] = jnp.dot(
                combine[r], back, preferred_element_type=jnp.float32
            ).astype(jnp.bfloat16)

        @pl.when(edge)
        def _():
            far_copy(c).start()
            sum_copy(c, 2, partial.at[c, 2]).start()

        @pl.when(middle)
        def _():
            sum_copy(c, 3, partial.at[c, 3]).start()

        sum_copy(c, 1, partial.at[c, 1]).start()
        if c > 0:
            sum_relay(c - 1)
    sum_relay(chunks - 1)

    for c in range(chunks):
        sum_copy(c, 1, partial.at[c, 1]).wait_recv()
        sum_copy(c, 2, partial.at[c, 2]).wait_recv()
        base[:, cols(c)] = base[:, cols(c)] + (
            partial[c, 0].astype(jnp.float32)
            + sums[c, 1].astype(jnp.float32)
            + sums[c, 2].astype(jnp.float32)
        )

        @pl.when(middle)
        def _():
            sum_copy(c, 3, partial.at[c, 3]).wait_recv()
            base[:, cols(c)] = base[:, cols(c)] + sums[c, 3].astype(jnp.float32)

        out_ref[:, cols(c)] = base[:, cols(c)].astype(jnp.bfloat16)

    for r in range(1, planes):
        info_copy(r).wait_send()
    for c in range(chunks):
        z_copy(c, 1).wait_send()
        z_copy(c, 2).wait_send()
        for n in (1, 2, 3):
            in_copy(c, n).wait_send()
            back_copy(c, n).wait_send()
            sum_copy(c, n, partial.at[c, n]).wait_send()

        @pl.when(middle)
        def _():
            z_copy(c, 3).wait_send()
            z_pass(c).wait_send()


def traded_experts(
    info, normed, hidden1, gate, up, down, new_gate, new_up, new_down,
    shared_gate, shared_up, shared_down, cap,
):
    n_tp = lax.axis_size("tp")
    rows, model = normed.shape
    planes, chunks = 4, 8
    wide = model // chunks
    inner = gate.shape[2]
    vmem = pl.BlockSpec(memory_space=pltpu.VMEM)
    anywhere = pl.BlockSpec(memory_space=pl.ANY)
    dma = pltpu.SemaphoreType.DMA
    low = jnp.bfloat16
    return pl.pallas_call(
        functools.partial(traded_kernel, n_tp, planes, cap, chunks),
        out_shape=jax.ShapeDtypeStruct((rows, model), low),
        in_specs=[vmem] * 3 + [anywhere] * 9,
        out_specs=vmem,
        scratch_shapes=[
            pltpu.VMEM((2,) + gate.shape[1:], low),
            pltpu.VMEM((2,) + up.shape[1:], low),
            pltpu.VMEM((2,) + down.shape[1:], low),
            pltpu.VMEM(shared_gate.shape, low),
            pltpu.VMEM(shared_up.shape, low),
            pltpu.VMEM(shared_down.shape, low),
            pltpu.VMEM((planes,) + info.shape, jnp.float32),
            pltpu.VMEM((chunks, planes, rows, wide), low),
            pltpu.VMEM((chunks, 3, 2, planes, cap, wide), low),
            pltpu.VMEM((chunks, 2, 4, planes, cap, wide), low),
            pltpu.VMEM((chunks, 2, 4, planes, cap, wide), low),
            pltpu.VMEM((chunks, 4, 2, planes, cap, wide), low),
            pltpu.VMEM((chunks, planes, rows, wide), low),
            pltpu.VMEM((chunks, rows, wide), low),
            pltpu.VMEM((chunks, rows, wide), low),
            pltpu.VMEM((chunks, planes, rows, wide), low),
            pltpu.VMEM((planes, 8 * cap, rows), low),
            pltpu.VMEM((planes, rows, 8 * cap), low),
            pltpu.VMEM((2, 2, 2 * planes * cap, 2 * inner), jnp.float32),
            pltpu.VMEM((2, 2, 2 * planes * cap, inner), low),
            pltpu.VMEM((rows, model), jnp.float32),
            dma((9,)), dma((planes,)), dma((planes,)),
            dma((chunks, planes)), dma((chunks, planes)),
            dma((chunks, 4)), dma((chunks, 4)),
            dma((chunks, 4)), dma((chunks, 4)),
            dma((chunks, 4)), dma((chunks, 4)),
            dma((chunks,)), dma((chunks,)),
        ],
        compiler_params=pltpu.CompilerParams(
            collective_id=1, has_side_effects=True, vmem_limit_bytes=56 * 2**20
        ),
        name="experts",
    )(
        info, normed, hidden1, gate, up, down, new_gate, new_up, new_down,
        shared_gate, shared_up, shared_down,
    )


def body(
    queries,
    keys,
    values,
    residual,
    out_proj,
    query_gain,
    key_gain,
    norm_gain,
    routes,
    route_weight,
    expert_gate,
    expert_up,
    expert_down,
    shared_gate,
    shared_up,
    shared_down,
):
    n_sp, n_tp = lax.axis_size("sp"), lax.axis_size("tp")
    rows_local, top_count = routes.shape
    expert_total = expert_gate.shape[0] * n_sp * n_tp
    capacity = max(2, 2 * rows_local * top_count // expert_total)
    traded = n_sp == 8 and n_tp == 4 and expert_gate.shape[0] == 1 and capacity % 16 == 0
    all_heads, *new_weights = attention(
        n_sp, n_tp, queries, keys, values, query_gain, key_gain,
        (expert_gate, expert_up, expert_down) if traded else (),
    )
    projected = jnp.dot(all_heads, out_proj, preferred_element_type=jnp.float32)
    hidden1 = (residual.astype(jnp.float32) + projected).astype(jnp.bfloat16)
    hidden_f = hidden1.astype(jnp.float32)
    normed = (
        hidden_f
        * lax.rsqrt(jnp.mean(hidden_f * hidden_f, axis=-1, keepdims=True) + EPS)
        * norm_gain
    ).astype(jnp.bfloat16)
    if traded:
        info = jnp.concatenate([routes.T.astype(jnp.float32), route_weight.T], axis=0)
        return traded_experts(
            info, normed, hidden1, expert_gate, expert_up, expert_down, *new_weights,
            shared_gate, shared_up, shared_down, capacity,
        )
    pair_count = rows_local * top_count
    flat_routes = routes.reshape(pair_count)
    one_hot = (flat_routes[:, None] == jnp.arange(expert_total, dtype=jnp.int32)[None, :]).astype(
        jnp.float32
    )
    lower = (jnp.arange(pair_count)[:, None] >= jnp.arange(pair_count)[None, :]).astype(jnp.float32)
    running_count = jnp.dot(lower, one_hot, precision=lax.Precision.HIGHEST)
    slot_place = (jnp.sum(running_count * one_hot, axis=1) - 1.0).astype(jnp.int32)
    slot_index = flat_routes * capacity + slot_place
    slots = slot_index.reshape(rows_local, top_count).astype(jnp.float32)
    info = jnp.concatenate([slots.T, route_weight.T], axis=0)
    layer_out = routed_experts(
        info, normed, hidden1, expert_gate, expert_up, expert_down,
        shared_gate, shared_up, shared_down, capacity,
    )
    return layer_out.astype(jnp.bfloat16)


def solution(mesh):
    placed = (
        P("sp", "tp"),
        P("sp", "tp"),
        P("sp", "tp"),
        P(("sp", "tp"), None),
        P(),
        P(),
        P(),
        P(),
        P(("sp", "tp"), None),
        P(("sp", "tp"), None),
        P(("sp", "tp"), None, None),
        P(("sp", "tp"), None, None),
        P(("sp", "tp"), None, None),
        P(),
        P(),
        P(),
    )
    return jax.shard_map(
        body, mesh=mesh, in_specs=placed, out_specs=P(("sp", "tp"), None), check_vma=False
    )
```

```python
import functools
import math

import jax
import jax.numpy as jnp
from jax import lax
from jax.experimental import pallas as pl
from jax.experimental.pallas import tpu as pltpu
from jax.sharding import PartitionSpec as P

GRID_W = 64
MESH = pl.DeviceIdType.MESH


EPS = 1e-06
THETA = 10000.0


def norm_rotate(block, gain, cosine, sine):
    mean = jnp.mean(block * block, axis=-1, keepdims=True)
    block = block * lax.rsqrt(mean + EPS) * gain
    quarter = block.shape[-1] // 4
    lane = lax.broadcasted_iota(jnp.int32, block.shape, 1)
    after = pltpu.roll(block, 3 * quarter, 1)
    before = pltpu.roll(block, quarter, 1)
    partner = jnp.where((lane // quarter) % 2 == 0, after, before)
    return (block * cosine + partner * sine).astype(jnp.bfloat16)


def plane_peer(z, d, planes):
    if planes == 4:
        return (z + 1 - 2 * (z % 2), z + 2 - 4 * (z // 2), 3 - z)[d - 1]
    return planes - 1 - z


def attention_kernel(
    n_sp, n_tp, planes, group,
    q_ref, k_ref, v_ref, cos_ref, sin_ref, qg_ref, kg_ref, out_ref,
    held, q_rot, top, total, accum, rows_out,
    send_z, send_y, recv_kv, send_o, recv_o,
):
    per = n_sp // planes
    me_sp = lax.axis_index("sp")
    me_tp = lax.axis_index("tp")
    z, y = me_sp // per, me_sp % per
    tok, width = k_ref.shape
    piece = tok // n_tp
    lanes = group * width
    held[me_sp, 0] = norm_rotate(
        k_ref[...].astype(jnp.float32), kg_ref[...], cos_ref[...], sin_ref[...]
    )
    held[me_sp, 1] = v_ref[...]
    barrier = pltpu.get_barrier_semaphore()
    for d in range(1, n_sp):
        pl.semaphore_signal(
            barrier, inc=1, device_id={"sp": lax.rem(me_sp + d, n_sp)}, device_id_type=MESH
        )
    for d in range(1, n_tp):
        pl.semaphore_signal(
            barrier, inc=1, device_id={"tp": lax.rem(me_tp + d, n_tp)}, device_id_type=MESH
        )
    pl.semaphore_wait(barrier, n_sp + n_tp - 2)

    def block_copy(block, target, sem):
        return pltpu.make_async_remote_copy(
            src_ref=held.at[block], dst_ref=held.at[block],
            send_sem=sem, recv_sem=recv_kv.at[block],
            device_id={"sp": target}, device_id_type=MESH,
        )

    def to_plane(slot, block):
        for d in range(1, per):
            block_copy(block, z * per + lax.rem(y + d, per), send_y.at[slot, d - 1]).start()

    for d in range(1, planes):
        if d == 1:
            block_copy(me_sp, plane_peer(z, d, planes) * per + y, send_z.at[d - 1]).start()
            to_plane(0, me_sp)
        else:
            block_copy(me_sp, plane_peer(z, d, planes) * per + y, send_z.at[d - 1]).start()
    for j in range(n_tp):
        rows = pl.ds(j * piece, piece)
        for h in range(group):
            q_rot[j, pl.ds(h * piece, piece), :] = norm_rotate(
                q_ref[rows, pl.ds(h * width, width)].astype(jnp.float32),
                qg_ref[...], cos_ref[rows, :], sin_ref[rows, :],
            )
    top[...] = jnp.full(top.shape, -1e30, jnp.float32)
    total[...] = jnp.zeros(total.shape, jnp.float32)
    accum[...] = jnp.zeros(accum.shape, jnp.float32)
    factor = math.log2(math.e) / math.sqrt(width)
    repeat = tok // width

    def attend(block, j):
        scores = lax.dot_general(
            q_rot[j], held[block, 0], (((1,), (1,)), ((), ())),
            preferred_element_type=jnp.float32,
        )
        old = top[j]
        new = jnp.maximum(old, jnp.max(scores, axis=1, keepdims=True))
        weights = jnp.exp2((scores - jnp.concatenate([new] * repeat, axis=1)) * factor)
        alpha = jnp.exp2((old - new) * factor)
        part = weights[:, :width]
        for r in range(1, repeat):
            part = part + weights[:, r * width:(r + 1) * width]
        summed = total[j] * alpha + part
        added = jnp.dot(
            weights.astype(jnp.bfloat16), held[block, 1], preferred_element_type=jnp.float32
        )
        return new, summed, accum[j] * alpha + added

    def out_copy(j):
        return pltpu.make_async_remote_copy(
            src_ref=rows_out.at[j],
            dst_ref=out_ref.at[:, pl.ds(pl.multiple_of(me_tp * lanes, 128), lanes)],
            send_sem=send_o.at[j], recv_sem=recv_o.at[me_tp],
            device_id={"tp": j}, device_id_type=MESH,
        )

    def step(block):
        @pl.loop(0, n_tp)
        def _(j):
            new, summed, acc = attend(block, j)
            top[j] = new
            total[j] = summed
            accum[j] = acc

    def arrive(block):
        block_copy(block, me_sp, send_z.at[0]).wait_recv()

    def others(plane, finish=False):
        for d in range(1, per):
            block = plane * per + lax.rem(y + d, per)
            arrive(block)
            step(block)

    step(me_sp)
    previous = z
    for d in range(1, planes):
        plane = plane_peer(z, d, planes)
        block = plane * per + y
        arrive(block)
        to_plane(d, block)
        others(previous)
        step(block)
        previous = plane
    others(previous)

    for d in range(n_tp):
        j = lax.rem(me_tp + 1 + d, n_tp)
        result = accum[j] / jnp.sum(total[j], axis=1, keepdims=True)
        result = result.astype(jnp.bfloat16)
        for h in range(group):
            rows_out[j, :, pl.ds(h * width, width)] = result[h * piece:(h + 1) * piece]
        if d < n_tp - 1:
            out_copy(j).start()
        else:
            for h in range(group):
                out_ref[:, pl.ds(pl.multiple_of(me_tp * lanes + h * width, 128), width)] = result[
                    h * piece:(h + 1) * piece
                ]
    for d in range(1, n_tp):
        source = lax.rem(me_tp + d, n_tp)
        pltpu.make_async_remote_copy(
            src_ref=rows_out.at[source],
            dst_ref=out_ref.at[:, pl.ds(pl.multiple_of(source * lanes, 128), lanes)],
            send_sem=send_o.at[source], recv_sem=recv_o.at[source],
            device_id={"tp": source}, device_id_type=MESH,
        ).wait()
    for d in range(1, planes):
        block_copy(me_sp, me_sp, send_z.at[d - 1]).wait_send()
    for slot in range(planes):
        for d in range(1, per):
            block_copy(me_sp, me_sp, send_y.at[slot, d - 1]).wait_send()


def angle_tables(tok, width):
    quarter = width // 4
    inverse = jnp.power(THETA, -4.0 * jnp.arange(quarter, dtype=jnp.float32) / width)
    start = lax.axis_index("sp") * tok
    grid_rows = tok // GRID_W
    row_angle = (start // GRID_W + jnp.arange(grid_rows)).astype(jnp.float32)[:, None] * inverse
    col_angle = jnp.arange(GRID_W).astype(jnp.float32)[:, None] * inverse

    def spread(row_part, col_part, sign):
        row_part = jnp.broadcast_to(row_part[:, None, :], (grid_rows, GRID_W, quarter))
        col_part = jnp.broadcast_to(col_part[None, :, :], (grid_rows, GRID_W, quarter))
        return jnp.concatenate(
            [sign * row_part, row_part, sign * col_part, col_part], axis=-1
        ).reshape(tok, width)

    tables = lax.optimization_barrier(
        (jnp.cos(row_angle), jnp.cos(col_angle), jnp.sin(row_angle), jnp.sin(col_angle))
    )
    return spread(tables[0], tables[1], 1.0), spread(tables[2], tables[3], -1.0)


def attention(mesh_sp, mesh_tp, queries, keys, values, query_gain, key_gain):
    tok, width = keys.shape
    group = queries.shape[1] // width
    planes = 4 if mesh_sp % 4 == 0 else 2
    per = mesh_sp // planes
    piece = tok // mesh_tp
    cosine, sine = angle_tables(tok, width)
    vmem = pl.BlockSpec(memory_space=pltpu.VMEM)
    return pl.pallas_call(
        functools.partial(attention_kernel, mesh_sp, mesh_tp, planes, group),
        out_shape=jax.ShapeDtypeStruct((piece, mesh_tp * group * width), jnp.bfloat16),
        in_specs=[vmem] * 7,
        out_specs=vmem,
        scratch_shapes=[
            pltpu.VMEM((mesh_sp, 2, tok, width), jnp.bfloat16),
            pltpu.VMEM((mesh_tp, group * piece, width), jnp.bfloat16),
            pltpu.VMEM((mesh_tp, group * piece, width), jnp.float32),
            pltpu.VMEM((mesh_tp, group * piece, width), jnp.float32),
            pltpu.VMEM((mesh_tp, group * piece, width), jnp.float32),
            pltpu.VMEM((mesh_tp, piece, group * width), jnp.bfloat16),
            pltpu.SemaphoreType.DMA((planes - 1,)),
            pltpu.SemaphoreType.DMA((planes, max(per - 1, 1))),
            pltpu.SemaphoreType.DMA((mesh_sp,)),
            pltpu.SemaphoreType.DMA((mesh_tp,)),
            pltpu.SemaphoreType.DMA((mesh_tp,)),
        ],
        compiler_params=pltpu.CompilerParams(
            collective_id=0, has_side_effects=True, vmem_limit_bytes=40 * 2**20
        ),
        name="attention",
    )(queries, keys, values, cosine, sine, query_gain.reshape(1, width), key_gain.reshape(1, width))


def expert_kernel(
    n_sp, n_tp, planes, cap, top_count, chunks,
    info_ref, normed_ref, hidden_ref, gate_ref, up_ref, down_ref,
    sgate_ref, sup_ref, sdown_ref, out_ref,
    info, gathered, sent, arrived, answers, returned, partial, sums,
    place, combine, acc, hid,
    s_info, r_info, s_z, r_z, s_in, r_in, s_back, r_back, s_sum, r_sum,
):
    per = n_sp // planes
    team = per * n_tp
    me_sp = lax.axis_index("sp")
    me_tp = lax.axis_index("tp")
    z, y = me_sp // per, me_sp % per
    me = y * n_tp + me_tp
    rows = normed_ref.shape[0]
    wide = normed_ref.shape[1] // chunks
    share = planes * cap
    slots = team * share
    tile = math.gcd(slots, 256)

    def in_plane(p):
        return {"sp": z * per + p // n_tp, "tp": p % n_tp}

    def at_plane(d):
        return {"sp": plane_peer(z, d, planes) * per + y}

    def block(p, size):
        return pl.ds(pl.multiple_of(p * size, size), size)

    def remote(src, dst, send, recv, target):
        return pltpu.make_async_remote_copy(
            src_ref=src, dst_ref=dst, send_sem=send, recv_sem=recv,
            device_id=target, device_id_type=MESH,
        )

    def cols(c):
        return pl.ds(c * wide, wide)

    barrier = pltpu.get_barrier_semaphore()

    @pl.loop(1, team)
    def _(d):
        pl.semaphore_signal(
            barrier, inc=1, device_id=in_plane(lax.rem(me + d, team)), device_id_type=MESH
        )

    for d in range(1, planes):
        pl.semaphore_signal(barrier, inc=1, device_id=at_plane(d), device_id_type=MESH)
    pl.semaphore_wait(barrier, team + planes - 2)

    def info_copy(d, source):
        return remote(info_ref, info.at[source], s_info.at[d], r_info.at[source], at_plane(d))

    def z_copy(c, d, source):
        return remote(
            normed_ref.at[:, cols(c)], gathered.at[c, block(source, rows)],
            s_z.at[c, d], r_z.at[c, source], at_plane(d),
        )

    def in_copy(c, p, source):
        return remote(
            sent.at[c, block(p, share)], arrived.at[c, block(source, share)],
            s_in.at[c, p], r_in.at[c, source], in_plane(p),
        )

    def back_copy(c, p, source):
        return remote(
            answers.at[c, block(p, share)], returned.at[c, block(source, share)],
            s_back.at[c, p], r_back.at[c, source], in_plane(p),
        )

    def sum_copy(c, d, source):
        return remote(
            partial.at[c, block(plane_peer(z, d, planes), rows)], sums.at[c, source],
            s_sum.at[c, d], r_sum.at[c, source], at_plane(d),
        )

    for d in range(1, planes):
        info_copy(d, z).start()
    for c in range(chunks):
        for d in range(1, planes):
            z_copy(c, d, z).start()
        gathered[c, block(z, rows)] = normed_ref[:, cols(c)]
    info[z] = info_ref[...]

    shared_gate = jnp.dot(normed_ref[...], sgate_ref[...], preferred_element_type=jnp.float32)
    shared_up = jnp.dot(normed_ref[...], sup_ref[...], preferred_element_type=jnp.float32)
    shared_hid = (jax.nn.silu(shared_gate) * shared_up).astype(jnp.bfloat16)
    for c in range(chunks):
        out_ref[:, cols(c)] = jnp.dot(
            shared_hid, sdown_ref[:, cols(c)], preferred_element_type=jnp.float32
        ) + hidden_ref[:, cols(c)].astype(jnp.float32)

    number = lax.broadcasted_iota(jnp.int32, (slots, rows), 0)
    owner = (number // cap) % planes
    slot = ((z * team + number // share) * cap + number % cap).astype(jnp.float32)
    for d in range(1, planes):
        info_copy(d, plane_peer(z, d, planes)).wait_recv()
    for plane in range(planes):
        wanted = jnp.where(owner == plane, slot, -1.0)
        ones = jnp.zeros((slots, rows), jnp.float32)
        shares = jnp.zeros((slots, rows), jnp.float32)
        for k in range(top_count):
            match = wanted == info[plane, k:k + 1, :]
            ones = jnp.where(match, 1.0, ones)
            shares = jnp.where(match, info[plane, top_count + k:top_count + k + 1, :], shares)
        place[:, pl.ds(plane * rows, rows)] = ones.astype(jnp.bfloat16)
        combine[pl.ds(plane * rows, rows), :] = shares.T.astype(jnp.bfloat16)

    for c in range(chunks):
        for d in range(1, planes):
            z_copy(c, d, plane_peer(z, d, planes)).wait_recv()

        @pl.loop(0, slots // tile)
        def _(i):
            sent[c, block(i, tile)] = jnp.dot(
                place[block(i, tile), :], gathered[c], preferred_element_type=jnp.float32
            ).astype(jnp.bfloat16)

        @pl.loop(1, team)
        def _(d):
            in_copy(c, lax.rem(me + d, team), me).start()

        arrived[c, block(me, share)] = sent[c, block(me, share)]

    inner = gate_ref.shape[2]
    for c in range(chunks):
        @pl.loop(1, team)
        def _(d):
            source = lax.rem(me + d, team)
            in_copy(c, source, source).wait_recv()

        @pl.loop(0, slots // tile)
        def _(i):
            part = arrived[c, block(i, tile)]
            gate = jnp.dot(part, gate_ref[0, cols(c), :], preferred_element_type=jnp.float32)
            up = jnp.dot(part, up_ref[0, cols(c), :], preferred_element_type=jnp.float32)
            if c > 0:
                gate = gate + acc[block(i, tile), pl.ds(0, inner)]
                up = up + acc[block(i, tile), pl.ds(inner, inner)]
            if c < chunks - 1:
                acc[block(i, tile), pl.ds(0, inner)] = gate
                acc[block(i, tile), pl.ds(inner, inner)] = up
            else:
                hid[block(i, tile), :] = (jax.nn.silu(gate) * up).astype(jnp.bfloat16)

    for c in range(chunks):
        @pl.loop(0, slots // tile)
        def _(i):
            answers[c, block(i, tile)] = jnp.dot(
                hid[block(i, tile), :], down_ref[0, :, cols(c)],
                preferred_element_type=jnp.float32,
            ).astype(jnp.bfloat16)

        @pl.loop(1, team)
        def _(d):
            back_copy(c, lax.rem(me + d, team), me).start()

        returned[c, block(me, share)] = answers[c, block(me, share)]

    for c in range(chunks):
        @pl.loop(1, team)
        def _(d):
            source = lax.rem(me + d, team)
            back_copy(c, source, source).wait_recv()

        @pl.loop(0, planes)
        def _(i):
            partial[c, block(i, rows)] = jnp.dot(
                combine[block(i, rows), :], returned[c], preferred_element_type=jnp.float32
            ).astype(jnp.bfloat16)

        for d in range(1, planes):
            sum_copy(c, d, z).start()
        sums[c, z] = partial[c, block(z, rows)]

    for c in range(chunks):
        for d in range(1, planes):
            sum_copy(c, d, plane_peer(z, d, planes)).wait_recv()
        result = out_ref[:, cols(c)]
        for plane in range(planes):
            result = result + sums[c, plane].astype(jnp.float32)
        out_ref[:, cols(c)] = result

    for d in range(1, planes):
        info_copy(d, z).wait_send()
    for c in range(chunks):
        for d in range(1, planes):
            z_copy(c, d, z).wait_send()
            sum_copy(c, d, z).wait_send()

        @pl.loop(1, team)
        def _(d):
            p = lax.rem(me + d, team)
            in_copy(c, p, me).wait_send()
            back_copy(c, p, me).wait_send()


def routed_experts(
    info, normed, hidden1, gate, up, down, shared_gate, shared_up, shared_down, cap
):
    n_sp, n_tp = lax.axis_size("sp"), lax.axis_size("tp")
    rows, model = normed.shape
    planes = 4 if n_sp % 4 == 0 else 2
    team = n_sp // planes * n_tp
    chunks = 8
    wide = model // chunks
    slots = team * planes * cap
    inner = gate.shape[2]
    top_count = info.shape[0] // 2
    vmem = pl.BlockSpec(memory_space=pltpu.VMEM)
    dma = pltpu.SemaphoreType.DMA
    return pl.pallas_call(
        functools.partial(expert_kernel, n_sp, n_tp, planes, cap, top_count, chunks),
        out_shape=jax.ShapeDtypeStruct((rows, model), jnp.float32),
        in_specs=[vmem] * 9,
        out_specs=vmem,
        scratch_shapes=[
            pltpu.VMEM((planes,) + info.shape, jnp.float32),
            pltpu.VMEM((chunks, planes * rows, wide), jnp.bfloat16),
            pltpu.VMEM((chunks, slots, wide), jnp.bfloat16),
            pltpu.VMEM((chunks, slots, wide), jnp.bfloat16),
            pltpu.VMEM((chunks, slots, wide), jnp.bfloat16),
            pltpu.VMEM((chunks, slots, wide), jnp.bfloat16),
            pltpu.VMEM((chunks, planes * rows, wide), jnp.bfloat16),
            pltpu.VMEM((chunks, planes, rows, wide), jnp.bfloat16),
            pltpu.VMEM((slots, planes * rows), jnp.bfloat16),
            pltpu.VMEM((planes * rows, slots), jnp.bfloat16),
            pltpu.VMEM((slots, 2 * inner), jnp.float32),
            pltpu.VMEM((slots, inner), jnp.bfloat16),
            dma((planes,)), dma((planes,)),
            dma((chunks, planes)), dma((chunks, planes)),
            dma((chunks, team)), dma((chunks, team)),
            dma((chunks, team)), dma((chunks, team)),
            dma((chunks, planes)), dma((chunks, planes)),
        ],
        compiler_params=pltpu.CompilerParams(
            collective_id=1, has_side_effects=True, vmem_limit_bytes=56 * 2**20
        ),
        name="experts",
    )(info, normed, hidden1, gate, up, down, shared_gate, shared_up, shared_down)


def layer_kernel(
    n_sp, n_tp, planes, cap, chunks,
    cos_ref, sin_ref, qg_ref, kg_ref, ng_ref, routes_ref, share_ref,
    q_any, k_any, v_any, residual_any, proj_any, *rest,
):
    own_any, shared_any, out_ref, rest = rest[:3], rest[3:6], rest[6], rest[7:]
    (
        q_ref, k_ref, v_ref, residual, w_proj, w_gate, w_up, w_down,
        w_shared_gate, w_shared_up, w_shared_down,
        held, q_rot, top, total, accum, rows_out, heads, normed,
        info, gathered, sent, arrived, returned, partial, relayed, passed, sums,
        place, combine, acc, hid, base,
        s_load, s_kv, r_kv, s_o, r_o, s_trade, r_trade,
        s_info, r_info, s_z, r_z, s_in, r_in, s_back, r_back, s_sum, r_sum, s_far, r_far,
    ) = rest
    answers = arrived
    me_sp = lax.axis_index("sp")
    me_tp = lax.axis_index("tp")
    z, y = me_sp // 2, lax.rem(me_sp, 2)
    x, k = me_tp // 2, lax.rem(me_tp, 2)
    middle = jnp.logical_or(z == 1, z == 2)
    edge = jnp.logical_or(z == 0, z == 3)
    tok, width = k_ref.shape
    group = q_ref.shape[1] // width
    rows = tok // n_tp
    lanes = group * width
    model = w_proj.shape[1]
    wide = model // chunks

    def flip(bit, by):
        return bit + by * (1 - 2 * bit)

    def device(yy, xx, kk):
        return {"sp": z * 2 + yy, "tp": xx * 2 + kk}

    def plane_of(r):
        return (z, flip(lax.rem(z, 2), 1) + z // 2 * 2, lax.rem(z + 2, 4), 3 - z)[r]

    def at_plane(r):
        return {"sp": plane_of(r) * 2 + y}

    def remote(src, dst, send, recv, target):
        return pltpu.make_async_remote_copy(
            src_ref=src, dst_ref=dst, send_sem=send, recv_sem=recv,
            device_id=target, device_id_type=MESH,
        )

    def cols(c):
        return pl.ds(c * wide, wide)

    pairs = [
        (k_any, k_ref), (v_any, held.at[0, 0, 1]), (q_any, q_ref), (residual_any, residual),
        (proj_any, w_proj),
        (shared_any[0], w_shared_gate), (shared_any[1], w_shared_up), (shared_any[2], w_shared_down),
        (own_any[0], w_gate.at[pl.ds(0, 1)]), (own_any[1], w_up.at[pl.ds(0, 1)]),
        (own_any[2], w_down.at[pl.ds(0, 1)]),
    ]
    loads = [pltpu.make_async_copy(src, dst, s_load.at[i]) for i, (src, dst) in enumerate(pairs)]
    for load in loads:
        load.start()

    partner = device(y, x, 1 - k)
    far_y = device(1 - y, x, 0)
    far_x = device(y, 1 - x, 1)
    sources = [device(flip(y, 1 - k), flip(x, k), core) for core in range(2)]
    across = {"sp": z * 2 + 1 - y}
    traded_to = device(flip(y, k), flip(x, 1 - k), k)
    barrier = pltpu.get_barrier_semaphore()
    for d in range(1, n_sp):
        pl.semaphore_signal(
            barrier, inc=1, device_id={"sp": lax.rem(me_sp + d, n_sp)}, device_id_type=MESH
        )
    for d in range(1, n_tp):
        pl.semaphore_signal(
            barrier, inc=1, device_id={"tp": lax.rem(me_tp + d, n_tp)}, device_id_type=MESH
        )
    pl.semaphore_signal(barrier, inc=1, device_id=device(1 - y, x, 1 - k), device_id_type=MESH)

    loads[0].wait()
    held[0, 0, 0] = norm_rotate(
        k_ref[...].astype(jnp.float32), kg_ref[...], cos_ref[...], sin_ref[...]
    )
    info[0, pl.ds(0, routes_ref.shape[0]), :] = routes_ref[...].astype(jnp.float32)
    info[0, pl.ds(routes_ref.shape[0], routes_ref.shape[0]), :] = share_ref[...]
    loads[1].wait()
    pl.semaphore_wait(barrier, n_sp + n_tp - 1)

    def trade(i):
        ref = (w_gate, w_up, w_down)[i]
        return remote(own_any[i], ref.at[pl.ds(1, 1)], s_trade.at[i], r_trade.at[i], traded_to)

    def kv_plane(r):
        return remote(held.at[0, 0], held.at[r, 0], s_kv.at[r], r_kv.at[r, 0], at_plane(r))

    def kv_pass():
        return remote(held.at[2, 0], held.at[3, 0], s_kv.at[0], r_kv.at[3, 0], at_plane(1))

    def kv_across(r):
        return remote(held.at[r, 0], held.at[r, 1], s_kv.at[planes + r], r_kv.at[r, 1], across)

    def info_copy(r):
        return remote(info.at[0], info.at[r], s_info.at[r], r_info.at[r], at_plane(r))

    kv_plane(1).start()
    kv_across(0).start()
    kv_plane(2).start()

    @pl.when(middle)
    def _():
        kv_plane(3).start()

    for r in range(1, planes):
        info_copy(r).start()

    @pl.when(k == 0)
    def _():
        trade(0).start()
        trade(1).start()

    loads[2].wait()
    for j in range(n_tp):
        part = pl.ds(j * rows, rows)
        for h in range(group):
            q_rot[j, pl.ds(h * rows, rows), :] = norm_rotate(
                q_ref[part, pl.ds(h * width, width)].astype(jnp.float32),
                qg_ref[...], cos_ref[part, :], sin_ref[part, :],
            )
    top[...] = jnp.full(top.shape, -1e30, jnp.float32)
    total[...] = jnp.zeros(total.shape, jnp.float32)
    accum[...] = jnp.zeros(accum.shape, jnp.float32)
    factor = math.log2(math.e) / math.sqrt(width)
    repeat = tok // width

    def attend(r, side, j):
        scores = lax.dot_general(
            q_rot[j], held[r, side, 0], (((1,), (1,)), ((), ())),
            preferred_element_type=jnp.float32,
        )
        old = top[j]
        new = jnp.maximum(old, jnp.max(scores, axis=1, keepdims=True))
        weights = jnp.exp2((scores - jnp.concatenate([new] * repeat, axis=1)) * factor)
        alpha = jnp.exp2((old - new) * factor)
        part = weights[:, :width]
        for i in range(1, repeat):
            part = part + weights[:, i * width:(i + 1) * width]
        summed = total[j] * alpha + part
        added = jnp.dot(
            weights.astype(jnp.bfloat16), held[r, side, 1], preferred_element_type=jnp.float32
        )
        return new, summed, accum[j] * alpha + added

    def step(r, side):
        @pl.loop(0, n_tp)
        def _(j):
            new, summed, added = attend(r, side, j)
            top[j] = new
            total[j] = summed
            accum[j] = added

    def out_copy(j):
        return remote(
            rows_out.at[j], heads.at[me_tp], s_o.at[j], r_o.at[me_tp], {"tp": j}
        )

    step(0, 0)
    kv_plane(1).wait_recv()
    kv_across(1).start()
    kv_across(0).wait_recv()
    step(0, 1)
    kv_plane(2).wait_recv()

    @pl.when(middle)
    def _():
        kv_pass().start()

    kv_across(2).start()
    step(1, 0)
    kv_across(1).wait_recv()
    step(1, 1)
    kv_plane(3).wait_recv()
    kv_across(3).start()

    @pl.when(k == 1)
    def _():
        trade(0).start()
        trade(1).start()

    step(2, 0)
    kv_across(2).wait_recv()
    step(2, 1)
    step(3, 0)
    kv_across(3).wait_recv()
    for d in range(n_tp):
        j = lax.rem(me_tp + (2, 3, 1, 0)[d], n_tp)
        new, summed, added = attend(3, 1, j)
        result = added / jnp.sum(summed, axis=1, keepdims=True)
        result = result.astype(jnp.bfloat16)
        for h in range(group):
            piece = result[h * rows:(h + 1) * rows]
            if d < n_tp - 1:
                rows_out[j, :, pl.ds(h * width, width)] = piece
            else:
                heads[j, :, pl.ds(h * width, width)] = piece
        if d < n_tp - 1:
            out_copy(j).start()

    @pl.when(k == 0)
    def _():
        trade(2).start()

    before = (
        lax.broadcasted_iota(jnp.int32, (rows, rows), 0)
        < lax.broadcasted_iota(jnp.int32, (rows, rows), 1)
    ).astype(jnp.float32).astype(jnp.bfloat16)
    count = lax.broadcasted_iota(jnp.int32, (cap, rows), 0).astype(jnp.float32)
    top_count = routes_ref.shape[0]
    members = []
    for t in range(4):
        core = (k, 1 - k, 0, 1)[t]
        far = t // 2
        for e in range(2):
            yy = flip(y, far * (1 - core) + e * core)
            xx = flip(x, far * core + e * (1 - core))
            members.append((z * 2 + yy) * n_tp + xx * 2 + core)
    for r in range(1, planes):
        info_copy(r).wait_recv()
    for r in range(planes):
        hits, shares = [], []
        for member in members:
            wanted = jnp.full((1, rows), member, jnp.int32).astype(jnp.float32)
            hit = jnp.zeros((1, rows), jnp.float32)
            share = jnp.zeros((1, rows), jnp.float32)
            for j in range(top_count):
                match = info[r, j:j + 1, :] == wanted
                hit = jnp.where(match, 1.0, hit)
                share = jnp.where(match, info[r, top_count + j:top_count + j + 1, :], share)
            hits.append(hit)
            shares.append(share)
        stacked = jnp.concatenate(hits, axis=0)
        earlier = jnp.dot(stacked.astype(jnp.bfloat16), before, preferred_element_type=jnp.float32)
        earlier = jnp.where(stacked > 0.5, earlier, -1.0)
        spread = []
        for n in range(len(members)):
            ones = (earlier[n:n + 1, :] == count).astype(jnp.float32)
            place[r, pl.ds(n * cap, cap), :] = ones.astype(jnp.bfloat16)
            spread.append(ones * shares[n])
        combine[r] = jnp.concatenate(spread, axis=0).T.astype(jnp.bfloat16)

    loads[3].wait()
    loads[4].wait()
    base[...] = residual[...].astype(jnp.float32)
    for d in range(n_tp):
        source = lax.rem(me_tp + (0, 1, 3, 2)[d], n_tp)
        if d > 0:
            remote(
                rows_out.at[source], heads.at[source], s_o.at[source], r_o.at[source],
                {"tp": source},
            ).wait()
        for c in range(chunks // 2):
            two = pl.ds(c * 2 * wide, 2 * wide)
            base[:, two] = base[:, two] + jnp.dot(
                heads[source],
                w_proj[pl.ds(pl.multiple_of(source * lanes, lanes), lanes), two],
                preferred_element_type=jnp.float32,
            )
    squares = jnp.zeros((rows, 1), jnp.float32)
    for c in range(chunks):
        hidden = base[:, cols(c)].astype(jnp.bfloat16).astype(jnp.float32)
        base[:, cols(c)] = hidden
        squares = squares + jnp.sum(hidden * hidden, axis=1, keepdims=True)
    scale = lax.rsqrt(squares / model + EPS)

    def z_copy(c, r):
        return remote(
            gathered.at[c, 0], gathered.at[c, r], s_z.at[c, r], r_z.at[c, r], at_plane(r)
        )

    def z_pass(c):
        return remote(
            gathered.at[c, 2], gathered.at[c, 3], s_far.at[c], r_z.at[c, 3], at_plane(1)
        )

    def in_copy(c, t):
        place_there = 1 if t == 1 else 2 + k
        return remote(
            sent.at[c, t - 1], arrived.at[c, :, place_there],
            s_in.at[c, t], r_in.at[c, place_there], (None, partner, far_y, far_x)[t],
        )

    def in_wait(c, i):
        remote(
            sent.at[c, 0], arrived.at[c, :, i], s_in.at[c, 1], r_in.at[c, i], partner
        ).wait_recv()

    def back_copy(c, i):
        place_there = 1 if i == 1 else 2 + k
        return remote(
            answers.at[c, :, i], returned.at[c, place_there],
            s_back.at[c, i], r_back.at[c, place_there],
            partner if i == 1 else sources[i - 2],
        )

    def sum_copy(c, r, src):
        return remote(src, sums.at[c, r], s_sum.at[c, r], r_sum.at[c, r], at_plane(r))

    def far_copy(c):
        return remote(partial.at[c, 3], relayed.at[c], s_sum.at[c, 3], r_far.at[c], at_plane(1))

    def z_start(c):
        z_copy(c, 1).start()
        z_copy(c, 2).start()

        @pl.when(middle)
        def _():
            z_copy(c, 3).start()

    for c in range(chunks):
        part = (base[:, cols(c)] * scale * ng_ref[:, cols(c)]).astype(jnp.bfloat16)
        normed[:, cols(c)] = part
        gathered[c, 0] = part
        if c < 2:
            z_start(c)

    for i in range(5, 8):
        loads[i].wait()
    shared_gate = jnp.dot(normed[...], w_shared_gate[...], preferred_element_type=jnp.float32)
    shared_up = jnp.dot(normed[...], w_shared_up[...], preferred_element_type=jnp.float32)
    shared_hid = (jax.nn.silu(shared_gate) * shared_up).astype(jnp.bfloat16)
    for c in range(chunks):
        base[:, cols(c)] = base[:, cols(c)] + jnp.dot(
            shared_hid, w_shared_down[:, cols(c)], preferred_element_type=jnp.float32
        )

    inner = w_gate.shape[2]

    def open_chunks(first, last):
        for c in range(first, last):
            for i in (1, 2, 3):
                in_wait(c, i)
        for e in range(2):
            if first == 0:
                if e == 0:
                    loads[8].wait()
                    loads[9].wait()
                else:
                    trade(0).wait_recv()
                    trade(1).wait_recv()

            @pl.loop(0, 2)
            def _(h):
                gate = up = None
                for c in range(first, last):
                    part = arrived[c, e, pl.ds(h * 2, 2)].reshape(2 * planes * cap, wide)
                    more_gate = jnp.dot(
                        part, w_gate[e, cols(c), :], preferred_element_type=jnp.float32
                    )
                    more_up = jnp.dot(
                        part, w_up[e, cols(c), :], preferred_element_type=jnp.float32
                    )
                    gate = more_gate if gate is None else gate + more_gate
                    up = more_up if up is None else up + more_up
                if first > 0:
                    gate = gate + acc[e, h, :, pl.ds(0, inner)]
                    up = up + acc[e, h, :, pl.ds(inner, inner)]
                if last < chunks:
                    acc[e, h, :, pl.ds(0, inner)] = gate
                    acc[e, h, :, pl.ds(inner, inner)] = up
                else:
                    hid[e, h] = (jax.nn.silu(gate) * up).astype(jnp.bfloat16)

    for c in range(chunks):
        if c + 2 < chunks:
            z_start(c + 2)
        z_copy(c, 2).wait_recv()

        @pl.when(middle)
        def _():
            z_pass(c).start()

        z_copy(c, 1).wait_recv()
        z_copy(c, 3).wait_recv()
        for r in range(planes):
            picked = jnp.dot(
                place[r], gathered[c, r], preferred_element_type=jnp.float32
            ).astype(jnp.bfloat16)
            for t in range(4):
                for e in range(2):
                    part = picked[(2 * t + e) * cap:(2 * t + e + 1) * cap]
                    if t == 0:
                        arrived[c, e, 0, r] = part
                    else:
                        sent[c, t - 1, e, r] = part
        for t in (2, 3, 1):
            in_copy(c, t).start()
        if c == chunks // 2 - 1:
            @pl.when(k == 1)
            def _():
                trade(2).start()
        if c % 2 == 1 and c > 1:
            open_chunks(c - 3, c - 1)
    open_chunks(chunks - 2, chunks)

    loads[10].wait()
    trade(2).wait_recv()
    for c in range(chunks):
        for e in range(2):
            @pl.loop(0, 2)
            def _(h):
                result = jnp.dot(
                    hid[e, h], w_down[e, :, cols(c)], preferred_element_type=jnp.float32
                ).astype(jnp.bfloat16).reshape(2, planes, cap, wide)
                answers[c, e, pl.ds(h * 2, 2)] = result
        for i in (2, 3, 1):
            back_copy(c, i).start()
        for e in range(2):
            returned[c, 0, e] = answers[c, e, 0]

    def sum_relay(c):
        @pl.when(middle)
        def _():
            far_copy(c).wait_recv()
            passed[c] = (
                partial[c, 2].astype(jnp.float32) + relayed[c].astype(jnp.float32)
            ).astype(jnp.bfloat16)
            sum_copy(c, 2, passed.at[c]).start()

    for c in range(chunks):
        for t in range(1, 4):
            remote(
                answers.at[c, :, 1], returned.at[c, t], s_back.at[c, 1], r_back.at[c, t], partner
            ).wait_recv()
        for r in (3, 2, 1, 0):
            back = jnp.concatenate(
                [returned[c, t, e, r] for t in range(4) for e in range(2)], axis=0
            )
            partial[c, r] = jnp.dot(
                combine[r], back, preferred_element_type=jnp.float32
            ).astype(jnp.bfloat16)

        @pl.when(edge)
        def _():
            far_copy(c).start()
            sum_copy(c, 2, partial.at[c, 2]).start()

        @pl.when(middle)
        def _():
            sum_copy(c, 3, partial.at[c, 3]).start()

        sum_copy(c, 1, partial.at[c, 1]).start()
        if c > 0:
            sum_relay(c - 1)
    sum_relay(chunks - 1)

    for c in range(chunks):
        sum_copy(c, 1, partial.at[c, 1]).wait_recv()
        sum_copy(c, 2, partial.at[c, 2]).wait_recv()
        base[:, cols(c)] = base[:, cols(c)] + (
            partial[c, 0].astype(jnp.float32)
            + sums[c, 1].astype(jnp.float32)
            + sums[c, 2].astype(jnp.float32)
        )

        @pl.when(middle)
        def _():
            sum_copy(c, 3, partial.at[c, 3]).wait_recv()
            base[:, cols(c)] = base[:, cols(c)] + sums[c, 3].astype(jnp.float32)

        out_ref[:, cols(c)] = base[:, cols(c)].astype(jnp.bfloat16)

    for i in range(3):
        trade(i).wait_send()
    for r in range(1, planes):
        info_copy(r).wait_send()
    kv_plane(1).wait_send()
    kv_plane(2).wait_send()
    for r in range(planes):
        kv_across(r).wait_send()

    @pl.when(middle)
    def _():
        kv_plane(3).wait_send()
        kv_pass().wait_send()

    for c in range(chunks):
        z_copy(c, 1).wait_send()
        z_copy(c, 2).wait_send()
        for n in (1, 2, 3):
            in_copy(c, n).wait_send()
            back_copy(c, n).wait_send()
            sum_copy(c, n, partial.at[c, n]).wait_send()

        @pl.when(middle)
        def _():
            z_copy(c, 3).wait_send()
            z_pass(c).wait_send()


def whole_layer(
    queries, keys, values, residual, out_proj, query_gain, key_gain, norm_gain,
    routes, route_weight, gate, up, down, shared_gate, shared_up, shared_down, cap,
):
    n_sp, n_tp = lax.axis_size("sp"), lax.axis_size("tp")
    tok, width = keys.shape
    lanes = queries.shape[1]
    group = lanes // width
    rows, model = residual.shape
    planes, chunks = 4, 8
    wide = model // chunks
    inner = gate.shape[2]
    cosine, sine = angle_tables(tok, width)
    vmem = pl.BlockSpec(memory_space=pltpu.VMEM)
    anywhere = pl.BlockSpec(memory_space=pl.ANY)
    dma = pltpu.SemaphoreType.DMA
    low, full = jnp.bfloat16, jnp.float32
    return pl.pallas_call(
        functools.partial(layer_kernel, n_sp, n_tp, planes, cap, chunks),
        out_shape=jax.ShapeDtypeStruct((rows, model), low),
        in_specs=[vmem] * 7 + [anywhere] * 11,
        out_specs=vmem,
        scratch_shapes=[
            pltpu.VMEM(queries.shape, low),
            pltpu.VMEM(keys.shape, low),
            pltpu.VMEM(values.shape, low),
            pltpu.VMEM(residual.shape, low),
            pltpu.VMEM(out_proj.shape, low),
            pltpu.VMEM((2,) + gate.shape[1:], low),
            pltpu.VMEM((2,) + up.shape[1:], low),
            pltpu.VMEM((2,) + down.shape[1:], low),
            pltpu.VMEM(shared_gate.shape, low),
            pltpu.VMEM(shared_up.shape, low),
            pltpu.VMEM(shared_down.shape, low),
            pltpu.VMEM((planes, 2, 2, tok, width), low),
            pltpu.VMEM((n_tp, group * rows, width), low),
            pltpu.VMEM((n_tp, group * rows, width), full),
            pltpu.VMEM((n_tp, group * rows, width), full),
            pltpu.VMEM((n_tp, group * rows, width), full),
            pltpu.VMEM((n_tp, rows, lanes), low),
            pltpu.VMEM((n_tp, rows, lanes), low),
            pltpu.VMEM((rows, model), low),
            pltpu.VMEM((planes, 2 * routes.shape[1], rows), full),
            pltpu.VMEM((chunks, planes, rows, wide), low),
            pltpu.VMEM((chunks, 3, 2, planes, cap, wide), low),
            pltpu.VMEM((chunks, 2, 4, planes, cap, wide), low),
            pltpu.VMEM((chunks, 4, 2, planes, cap, wide), low),
            pltpu.VMEM((chunks, planes, rows, wide), low),
            pltpu.VMEM((chunks, rows, wide), low),
            pltpu.VMEM((chunks, rows, wide), low),
            pltpu.VMEM((chunks, planes, rows, wide), low),
            pltpu.VMEM((planes, 8 * cap, rows), low),
            pltpu.VMEM((planes, rows, 8 * cap), low),
            pltpu.VMEM((2, 2, 2 * planes * cap, 2 * inner), full),
            pltpu.VMEM((2, 2, 2 * planes * cap, inner), low),
            pltpu.VMEM((rows, model), full),
            dma((11,)), dma((2 * planes,)), dma((planes, 2)),
            dma((n_tp,)), dma((n_tp,)), dma((3,)), dma((3,)),
            dma((planes,)), dma((planes,)),
            dma((chunks, planes)), dma((chunks, planes)),
            dma((chunks, 4)), dma((chunks, 4)),
            dma((chunks, 4)), dma((chunks, 4)),
            dma((chunks, 4)), dma((chunks, 4)),
            dma((chunks,)), dma((chunks,)),
        ],
        compiler_params=pltpu.CompilerParams(
            collective_id=2, has_side_effects=True, vmem_limit_bytes=61 * 2**20
        ),
        name="layer",
    )(
        cosine, sine, query_gain.reshape(1, width), key_gain.reshape(1, width),
        norm_gain.reshape(1, model), routes.T, route_weight.T,
        queries, keys, values, residual, out_proj,
        gate, up, down, shared_gate, shared_up, shared_down,
    )


def body(
    queries,
    keys,
    values,
    residual,
    out_proj,
    query_gain,
    key_gain,
    norm_gain,
    routes,
    route_weight,
    expert_gate,
    expert_up,
    expert_down,
    shared_gate,
    shared_up,
    shared_down,
):
    n_sp, n_tp = lax.axis_size("sp"), lax.axis_size("tp")
    rows_local, top_count = routes.shape
    expert_total = expert_gate.shape[0] * n_sp * n_tp
    capacity = max(2, 2 * rows_local * top_count // expert_total)
    if n_sp == 8 and n_tp == 4 and expert_gate.shape[0] == 1 and capacity % 16 == 0:
        return whole_layer(
            queries, keys, values, residual, out_proj, query_gain, key_gain, norm_gain,
            routes, route_weight, expert_gate, expert_up, expert_down,
            shared_gate, shared_up, shared_down, capacity,
        )
    all_heads = attention(n_sp, n_tp, queries, keys, values, query_gain, key_gain)
    projected = jnp.dot(all_heads, out_proj, preferred_element_type=jnp.float32)
    hidden1 = (residual.astype(jnp.float32) + projected).astype(jnp.bfloat16)
    hidden_f = hidden1.astype(jnp.float32)
    normed = (
        hidden_f
        * lax.rsqrt(jnp.mean(hidden_f * hidden_f, axis=-1, keepdims=True) + EPS)
        * norm_gain
    ).astype(jnp.bfloat16)
    pair_count = rows_local * top_count
    flat_routes = routes.reshape(pair_count)
    one_hot = (flat_routes[:, None] == jnp.arange(expert_total, dtype=jnp.int32)[None, :]).astype(
        jnp.float32
    )
    lower = (jnp.arange(pair_count)[:, None] >= jnp.arange(pair_count)[None, :]).astype(jnp.float32)
    running_count = jnp.dot(lower, one_hot, precision=lax.Precision.HIGHEST)
    slot_place = (jnp.sum(running_count * one_hot, axis=1) - 1.0).astype(jnp.int32)
    slot_index = flat_routes * capacity + slot_place
    slots = slot_index.reshape(rows_local, top_count).astype(jnp.float32)
    info = jnp.concatenate([slots.T, route_weight.T], axis=0)
    layer_out = routed_experts(
        info, normed, hidden1, expert_gate, expert_up, expert_down,
        shared_gate, shared_up, shared_down, capacity,
    )
    return layer_out.astype(jnp.bfloat16)


def solution(mesh):
    placed = (
        P("sp", "tp"),
        P("sp", "tp"),
        P("sp", "tp"),
        P(("sp", "tp"), None),
        P(),
        P(),
        P(),
        P(),
        P(("sp", "tp"), None),
        P(("sp", "tp"), None),
        P(("sp", "tp"), None, None),
        P(("sp", "tp"), None, None),
        P(("sp", "tp"), None, None),
        P(),
        P(),
        P(),
    )
    return jax.shard_map(
        body, mesh=mesh, in_specs=placed, out_specs=P(("sp", "tp"), None), check_vma=False
    )
```

```python
import functools
import math

import jax
import jax.numpy as jnp
from jax import lax
from jax.experimental import pallas as pl
from jax.experimental.pallas import tpu as pltpu
from jax.sharding import PartitionSpec as P

GRID_W = 64
MESH = pl.DeviceIdType.MESH


EPS = 1e-06
THETA = 10000.0


def norm_rotate(block, gain, cosine, sine):
    mean = jnp.mean(block * block, axis=-1, keepdims=True)
    block = block * lax.rsqrt(mean + EPS) * gain
    quarter = block.shape[-1] // 4
    lane = lax.broadcasted_iota(jnp.int32, block.shape, 1)
    after = pltpu.roll(block, 3 * quarter, 1)
    before = pltpu.roll(block, quarter, 1)
    partner = jnp.where((lane // quarter) % 2 == 0, after, before)
    return (block * cosine + partner * sine).astype(jnp.bfloat16)


def plane_peer(z, d, planes):
    if planes == 4:
        return (z + 1 - 2 * (z % 2), z + 2 - 4 * (z // 2), 3 - z)[d - 1]
    return planes - 1 - z


def attention_kernel(
    n_sp, n_tp, planes, group,
    q_ref, k_ref, v_ref, cos_ref, sin_ref, qg_ref, kg_ref, out_ref,
    held, q_rot, top, total, accum, rows_out,
    send_z, send_y, recv_kv, send_o, recv_o,
):
    per = n_sp // planes
    me_sp = lax.axis_index("sp")
    me_tp = lax.axis_index("tp")
    z, y = me_sp // per, me_sp % per
    tok, width = k_ref.shape
    piece = tok // n_tp
    lanes = group * width
    held[me_sp, 0] = norm_rotate(
        k_ref[...].astype(jnp.float32), kg_ref[...], cos_ref[...], sin_ref[...]
    )
    held[me_sp, 1] = v_ref[...]
    barrier = pltpu.get_barrier_semaphore()
    for d in range(1, n_sp):
        pl.semaphore_signal(
            barrier, inc=1, device_id={"sp": lax.rem(me_sp + d, n_sp)}, device_id_type=MESH
        )
    for d in range(1, n_tp):
        pl.semaphore_signal(
            barrier, inc=1, device_id={"tp": lax.rem(me_tp + d, n_tp)}, device_id_type=MESH
        )
    pl.semaphore_wait(barrier, n_sp + n_tp - 2)

    def block_copy(block, target, sem):
        return pltpu.make_async_remote_copy(
            src_ref=held.at[block], dst_ref=held.at[block],
            send_sem=sem, recv_sem=recv_kv.at[block],
            device_id={"sp": target}, device_id_type=MESH,
        )

    def to_plane(slot, block):
        for d in range(1, per):
            block_copy(block, z * per + lax.rem(y + d, per), send_y.at[slot, d - 1]).start()

    for d in range(1, planes):
        if d == 1:
            block_copy(me_sp, plane_peer(z, d, planes) * per + y, send_z.at[d - 1]).start()
            to_plane(0, me_sp)
        else:
            block_copy(me_sp, plane_peer(z, d, planes) * per + y, send_z.at[d - 1]).start()
    for j in range(n_tp):
        rows = pl.ds(j * piece, piece)
        for h in range(group):
            q_rot[j, pl.ds(h * piece, piece), :] = norm_rotate(
                q_ref[rows, pl.ds(h * width, width)].astype(jnp.float32),
                qg_ref[...], cos_ref[rows, :], sin_ref[rows, :],
            )
    top[...] = jnp.full(top.shape, -1e30, jnp.float32)
    total[...] = jnp.zeros(total.shape, jnp.float32)
    accum[...] = jnp.zeros(accum.shape, jnp.float32)
    factor = math.log2(math.e) / math.sqrt(width)
    repeat = tok // width

    def attend(block, j):
        scores = lax.dot_general(
            q_rot[j], held[block, 0], (((1,), (1,)), ((), ())),
            preferred_element_type=jnp.float32,
        )
        old = top[j]
        new = jnp.maximum(old, jnp.max(scores, axis=1, keepdims=True))
        weights = jnp.exp2((scores - jnp.concatenate([new] * repeat, axis=1)) * factor)
        alpha = jnp.exp2((old - new) * factor)
        part = weights[:, :width]
        for r in range(1, repeat):
            part = part + weights[:, r * width:(r + 1) * width]
        summed = total[j] * alpha + part
        added = jnp.dot(
            weights.astype(jnp.bfloat16), held[block, 1], preferred_element_type=jnp.float32
        )
        return new, summed, accum[j] * alpha + added

    def out_copy(j):
        return pltpu.make_async_remote_copy(
            src_ref=rows_out.at[j],
            dst_ref=out_ref.at[:, pl.ds(pl.multiple_of(me_tp * lanes, 128), lanes)],
            send_sem=send_o.at[j], recv_sem=recv_o.at[me_tp],
            device_id={"tp": j}, device_id_type=MESH,
        )

    def step(block):
        @pl.loop(0, n_tp)
        def _(j):
            new, summed, acc = attend(block, j)
            top[j] = new
            total[j] = summed
            accum[j] = acc

    def arrive(block):
        block_copy(block, me_sp, send_z.at[0]).wait_recv()

    def others(plane, finish=False):
        for d in range(1, per):
            block = plane * per + lax.rem(y + d, per)
            arrive(block)
            step(block)

    step(me_sp)
    previous = z
    for d in range(1, planes):
        plane = plane_peer(z, d, planes)
        block = plane * per + y
        arrive(block)
        to_plane(d, block)
        others(previous)
        step(block)
        previous = plane
    others(previous)

    for d in range(n_tp):
        j = lax.rem(me_tp + 1 + d, n_tp)
        result = accum[j] / jnp.sum(total[j], axis=1, keepdims=True)
        result = result.astype(jnp.bfloat16)
        for h in range(group):
            rows_out[j, :, pl.ds(h * width, width)] = result[h * piece:(h + 1) * piece]
        if d < n_tp - 1:
            out_copy(j).start()
        else:
            for h in range(group):
                out_ref[:, pl.ds(pl.multiple_of(me_tp * lanes + h * width, 128), width)] = result[
                    h * piece:(h + 1) * piece
                ]
    for d in range(1, n_tp):
        source = lax.rem(me_tp + d, n_tp)
        pltpu.make_async_remote_copy(
            src_ref=rows_out.at[source],
            dst_ref=out_ref.at[:, pl.ds(pl.multiple_of(source * lanes, 128), lanes)],
            send_sem=send_o.at[source], recv_sem=recv_o.at[source],
            device_id={"tp": source}, device_id_type=MESH,
        ).wait()
    for d in range(1, planes):
        block_copy(me_sp, me_sp, send_z.at[d - 1]).wait_send()
    for slot in range(planes):
        for d in range(1, per):
            block_copy(me_sp, me_sp, send_y.at[slot, d - 1]).wait_send()


def angle_tables(tok, width):
    quarter = width // 4
    inverse = jnp.power(THETA, -4.0 * jnp.arange(quarter, dtype=jnp.float32) / width)
    start = lax.axis_index("sp") * tok
    grid_rows = tok // GRID_W
    row_angle = (start // GRID_W + jnp.arange(grid_rows)).astype(jnp.float32)[:, None] * inverse
    col_angle = jnp.arange(GRID_W).astype(jnp.float32)[:, None] * inverse

    def spread(row_part, col_part, sign):
        row_part = jnp.broadcast_to(row_part[:, None, :], (grid_rows, GRID_W, quarter))
        col_part = jnp.broadcast_to(col_part[None, :, :], (grid_rows, GRID_W, quarter))
        return jnp.concatenate(
            [sign * row_part, row_part, sign * col_part, col_part], axis=-1
        ).reshape(tok, width)

    tables = lax.optimization_barrier(
        (jnp.cos(row_angle), jnp.cos(col_angle), jnp.sin(row_angle), jnp.sin(col_angle))
    )
    return spread(tables[0], tables[1], 1.0), spread(tables[2], tables[3], -1.0)


def attention(mesh_sp, mesh_tp, queries, keys, values, query_gain, key_gain):
    tok, width = keys.shape
    group = queries.shape[1] // width
    planes = 4 if mesh_sp % 4 == 0 else 2
    per = mesh_sp // planes
    piece = tok // mesh_tp
    cosine, sine = angle_tables(tok, width)
    vmem = pl.BlockSpec(memory_space=pltpu.VMEM)
    return pl.pallas_call(
        functools.partial(attention_kernel, mesh_sp, mesh_tp, planes, group),
        out_shape=jax.ShapeDtypeStruct((piece, mesh_tp * group * width), jnp.bfloat16),
        in_specs=[vmem] * 7,
        out_specs=vmem,
        scratch_shapes=[
            pltpu.VMEM((mesh_sp, 2, tok, width), jnp.bfloat16),
            pltpu.VMEM((mesh_tp, group * piece, width), jnp.bfloat16),
            pltpu.VMEM((mesh_tp, group * piece, width), jnp.float32),
            pltpu.VMEM((mesh_tp, group * piece, width), jnp.float32),
            pltpu.VMEM((mesh_tp, group * piece, width), jnp.float32),
            pltpu.VMEM((mesh_tp, piece, group * width), jnp.bfloat16),
            pltpu.SemaphoreType.DMA((planes - 1,)),
            pltpu.SemaphoreType.DMA((planes, max(per - 1, 1))),
            pltpu.SemaphoreType.DMA((mesh_sp,)),
            pltpu.SemaphoreType.DMA((mesh_tp,)),
            pltpu.SemaphoreType.DMA((mesh_tp,)),
        ],
        compiler_params=pltpu.CompilerParams(
            collective_id=0, has_side_effects=True, vmem_limit_bytes=40 * 2**20
        ),
        name="attention",
    )(queries, keys, values, cosine, sine, query_gain.reshape(1, width), key_gain.reshape(1, width))


def expert_kernel(
    n_sp, n_tp, planes, cap, top_count, chunks,
    info_ref, normed_ref, hidden_ref, gate_ref, up_ref, down_ref,
    sgate_ref, sup_ref, sdown_ref, out_ref,
    info, gathered, sent, arrived, answers, returned, partial, sums,
    place, combine, acc, hid,
    s_info, r_info, s_z, r_z, s_in, r_in, s_back, r_back, s_sum, r_sum,
):
    per = n_sp // planes
    team = per * n_tp
    me_sp = lax.axis_index("sp")
    me_tp = lax.axis_index("tp")
    z, y = me_sp // per, me_sp % per
    me = y * n_tp + me_tp
    rows = normed_ref.shape[0]
    wide = normed_ref.shape[1] // chunks
    share = planes * cap
    slots = team * share
    tile = math.gcd(slots, 256)

    def in_plane(p):
        return {"sp": z * per + p // n_tp, "tp": p % n_tp}

    def at_plane(d):
        return {"sp": plane_peer(z, d, planes) * per + y}

    def block(p, size):
        return pl.ds(pl.multiple_of(p * size, size), size)

    def remote(src, dst, send, recv, target):
        return pltpu.make_async_remote_copy(
            src_ref=src, dst_ref=dst, send_sem=send, recv_sem=recv,
            device_id=target, device_id_type=MESH,
        )

    def cols(c):
        return pl.ds(c * wide, wide)

    barrier = pltpu.get_barrier_semaphore()

    @pl.loop(1, team)
    def _(d):
        pl.semaphore_signal(
            barrier, inc=1, device_id=in_plane(lax.rem(me + d, team)), device_id_type=MESH
        )

    for d in range(1, planes):
        pl.semaphore_signal(barrier, inc=1, device_id=at_plane(d), device_id_type=MESH)
    pl.semaphore_wait(barrier, team + planes - 2)

    def info_copy(d, source):
        return remote(info_ref, info.at[source], s_info.at[d], r_info.at[source], at_plane(d))

    def z_copy(c, d, source):
        return remote(
            normed_ref.at[:, cols(c)], gathered.at[c, block(source, rows)],
            s_z.at[c, d], r_z.at[c, source], at_plane(d),
        )

    def in_copy(c, p, source):
        return remote(
            sent.at[c, block(p, share)], arrived.at[c, block(source, share)],
            s_in.at[c, p], r_in.at[c, source], in_plane(p),
        )

    def back_copy(c, p, source):
        return remote(
            answers.at[c, block(p, share)], returned.at[c, block(source, share)],
            s_back.at[c, p], r_back.at[c, source], in_plane(p),
        )

    def sum_copy(c, d, source):
        return remote(
            partial.at[c, block(plane_peer(z, d, planes), rows)], sums.at[c, source],
            s_sum.at[c, d], r_sum.at[c, source], at_plane(d),
        )

    for d in range(1, planes):
        info_copy(d, z).start()
    for c in range(chunks):
        for d in range(1, planes):
            z_copy(c, d, z).start()
        gathered[c, block(z, rows)] = normed_ref[:, cols(c)]
    info[z] = info_ref[...]

    shared_gate = jnp.dot(normed_ref[...], sgate_ref[...], preferred_element_type=jnp.float32)
    shared_up = jnp.dot(normed_ref[...], sup_ref[...], preferred_element_type=jnp.float32)
    shared_hid = (jax.nn.silu(shared_gate) * shared_up).astype(jnp.bfloat16)
    for c in range(chunks):
        out_ref[:, cols(c)] = jnp.dot(
            shared_hid, sdown_ref[:, cols(c)], preferred_element_type=jnp.float32
        ) + hidden_ref[:, cols(c)].astype(jnp.float32)

    number = lax.broadcasted_iota(jnp.int32, (slots, rows), 0)
    owner = (number // cap) % planes
    slot = ((z * team + number // share) * cap + number % cap).astype(jnp.float32)
    for d in range(1, planes):
        info_copy(d, plane_peer(z, d, planes)).wait_recv()
    for plane in range(planes):
        wanted = jnp.where(owner == plane, slot, -1.0)
        ones = jnp.zeros((slots, rows), jnp.float32)
        shares = jnp.zeros((slots, rows), jnp.float32)
        for k in range(top_count):
            match = wanted == info[plane, k:k + 1, :]
            ones = jnp.where(match, 1.0, ones)
            shares = jnp.where(match, info[plane, top_count + k:top_count + k + 1, :], shares)
        place[:, pl.ds(plane * rows, rows)] = ones.astype(jnp.bfloat16)
        combine[pl.ds(plane * rows, rows), :] = shares.T.astype(jnp.bfloat16)

    for c in range(chunks):
        for d in range(1, planes):
            z_copy(c, d, plane_peer(z, d, planes)).wait_recv()

        @pl.loop(0, slots // tile)
        def _(i):
            sent[c, block(i, tile)] = jnp.dot(
                place[block(i, tile), :], gathered[c], preferred_element_type=jnp.float32
            ).astype(jnp.bfloat16)

        @pl.loop(1, team)
        def _(d):
            in_copy(c, lax.rem(me + d, team), me).start()

        arrived[c, block(me, share)] = sent[c, block(me, share)]

    inner = gate_ref.shape[2]
    for c in range(chunks):
        @pl.loop(1, team)
        def _(d):
            source = lax.rem(me + d, team)
            in_copy(c, source, source).wait_recv()

        @pl.loop(0, slots // tile)
        def _(i):
            part = arrived[c, block(i, tile)]
            gate = jnp.dot(part, gate_ref[0, cols(c), :], preferred_element_type=jnp.float32)
            up = jnp.dot(part, up_ref[0, cols(c), :], preferred_element_type=jnp.float32)
            if c > 0:
                gate = gate + acc[block(i, tile), pl.ds(0, inner)]
                up = up + acc[block(i, tile), pl.ds(inner, inner)]
            if c < chunks - 1:
                acc[block(i, tile), pl.ds(0, inner)] = gate
                acc[block(i, tile), pl.ds(inner, inner)] = up
            else:
                hid[block(i, tile), :] = (jax.nn.silu(gate) * up).astype(jnp.bfloat16)

    for c in range(chunks):
        @pl.loop(0, slots // tile)
        def _(i):
            answers[c, block(i, tile)] = jnp.dot(
                hid[block(i, tile), :], down_ref[0, :, cols(c)],
                preferred_element_type=jnp.float32,
            ).astype(jnp.bfloat16)

        @pl.loop(1, team)
        def _(d):
            back_copy(c, lax.rem(me + d, team), me).start()

        returned[c, block(me, share)] = answers[c, block(me, share)]

    for c in range(chunks):
        @pl.loop(1, team)
        def _(d):
            source = lax.rem(me + d, team)
            back_copy(c, source, source).wait_recv()

        @pl.loop(0, planes)
        def _(i):
            partial[c, block(i, rows)] = jnp.dot(
                combine[block(i, rows), :], returned[c], preferred_element_type=jnp.float32
            ).astype(jnp.bfloat16)

        for d in range(1, planes):
            sum_copy(c, d, z).start()
        sums[c, z] = partial[c, block(z, rows)]

    for c in range(chunks):
        for d in range(1, planes):
            sum_copy(c, d, plane_peer(z, d, planes)).wait_recv()
        result = out_ref[:, cols(c)]
        for plane in range(planes):
            result = result + sums[c, plane].astype(jnp.float32)
        out_ref[:, cols(c)] = result

    for d in range(1, planes):
        info_copy(d, z).wait_send()
    for c in range(chunks):
        for d in range(1, planes):
            z_copy(c, d, z).wait_send()
            sum_copy(c, d, z).wait_send()

        @pl.loop(1, team)
        def _(d):
            p = lax.rem(me + d, team)
            in_copy(c, p, me).wait_send()
            back_copy(c, p, me).wait_send()


def routed_experts(
    info, normed, hidden1, gate, up, down, shared_gate, shared_up, shared_down, cap
):
    n_sp, n_tp = lax.axis_size("sp"), lax.axis_size("tp")
    rows, model = normed.shape
    planes = 4 if n_sp % 4 == 0 else 2
    team = n_sp // planes * n_tp
    chunks = 8
    wide = model // chunks
    slots = team * planes * cap
    inner = gate.shape[2]
    top_count = info.shape[0] // 2
    vmem = pl.BlockSpec(memory_space=pltpu.VMEM)
    dma = pltpu.SemaphoreType.DMA
    return pl.pallas_call(
        functools.partial(expert_kernel, n_sp, n_tp, planes, cap, top_count, chunks),
        out_shape=jax.ShapeDtypeStruct((rows, model), jnp.float32),
        in_specs=[vmem] * 9,
        out_specs=vmem,
        scratch_shapes=[
            pltpu.VMEM((planes,) + info.shape, jnp.float32),
            pltpu.VMEM((chunks, planes * rows, wide), jnp.bfloat16),
            pltpu.VMEM((chunks, slots, wide), jnp.bfloat16),
            pltpu.VMEM((chunks, slots, wide), jnp.bfloat16),
            pltpu.VMEM((chunks, slots, wide), jnp.bfloat16),
            pltpu.VMEM((chunks, slots, wide), jnp.bfloat16),
            pltpu.VMEM((chunks, planes * rows, wide), jnp.bfloat16),
            pltpu.VMEM((chunks, planes, rows, wide), jnp.bfloat16),
            pltpu.VMEM((slots, planes * rows), jnp.bfloat16),
            pltpu.VMEM((planes * rows, slots), jnp.bfloat16),
            pltpu.VMEM((slots, 2 * inner), jnp.float32),
            pltpu.VMEM((slots, inner), jnp.bfloat16),
            dma((planes,)), dma((planes,)),
            dma((chunks, planes)), dma((chunks, planes)),
            dma((chunks, team)), dma((chunks, team)),
            dma((chunks, team)), dma((chunks, team)),
            dma((chunks, planes)), dma((chunks, planes)),
        ],
        compiler_params=pltpu.CompilerParams(
            collective_id=1, has_side_effects=True, vmem_limit_bytes=56 * 2**20
        ),
        name="experts",
    )(info, normed, hidden1, gate, up, down, shared_gate, shared_up, shared_down)


def layer_kernel(
    n_sp, n_tp, planes, cap, chunks,
    cos_rows, cos_cols, sin_rows, sin_cols, qg_ref, kg_ref, ng_ref, routes_ref, share_ref,
    q_any, k_any, v_any, residual_any, proj_any, *rest,
):
    own_any, shared_any, out_ref, rest = rest[:3], rest[3:6], rest[6], rest[7:]
    (
        q_ref, k_ref, residual, w_proj, w_gate, w_up, w_down,
        w_shared_gate, w_shared_up, w_shared_down,
        cos_ref, sin_ref, held, q_rot, top, total, accum, rows_out, heads, normed,
        info, gathered, sent, arrived, returned, partial, edge_in, mid_in,
        place, combine, acc, hid, base,
        s_load, s_kv, r_kv, s_o, r_o, s_trade, r_trade,
        s_info, r_info, s_z, r_z, s_in, r_in, s_back, r_back, s_sum, r_edge, r_mid,
    ) = rest
    answers = arrived
    me_sp = lax.axis_index("sp")
    me_tp = lax.axis_index("tp")
    z, y = me_sp // 2, lax.rem(me_sp, 2)
    x, k = me_tp // 2, lax.rem(me_tp, 2)
    middle = jnp.logical_or(z == 1, z == 2)
    edge = jnp.logical_or(z == 0, z == 3)
    tok, width = k_ref.shape
    group = q_ref.shape[1] // width
    rows = tok // n_tp
    lanes = group * width
    model = w_proj.shape[1]
    wide = model // chunks

    def flip(bit, by):
        return bit + by * (1 - 2 * bit)

    def device(yy, xx, kk):
        return {"sp": z * 2 + yy, "tp": xx * 2 + kk}

    def plane_of(r):
        return (z, flip(lax.rem(z, 2), 1) + z // 2 * 2, lax.rem(z + 2, 4), 3 - z)[r]

    def at_plane(r):
        return {"sp": plane_of(r) * 2 + y}

    def remote(src, dst, send, recv, target):
        return pltpu.make_async_remote_copy(
            src_ref=src, dst_ref=dst, send_sem=send, recv_sem=recv,
            device_id=target, device_id_type=MESH,
        )

    def cols(c):
        return pl.ds(c * wide, wide)

    pairs = [
        (k_any, k_ref), (v_any, held.at[0, 0, 1]), (q_any, q_ref), (residual_any, residual),
        (proj_any, w_proj),
        (shared_any[0], w_shared_gate), (shared_any[1], w_shared_up), (shared_any[2], w_shared_down),
        (own_any[0], w_gate.at[pl.ds(0, 1)]), (own_any[1], w_up.at[pl.ds(0, 1)]),
        (own_any[2], w_down.at[pl.ds(0, 1)]),
    ]
    loads = [pltpu.make_async_copy(src, dst, s_load.at[i]) for i, (src, dst) in enumerate(pairs)]
    for load in loads:
        load.start()

    partner = device(y, x, 1 - k)
    far_y = device(1 - y, x, 0)
    far_x = device(y, 1 - x, 1)
    sources = [device(flip(y, 1 - k), flip(x, k), core) for core in range(2)]
    across = {"sp": z * 2 + 1 - y}
    traded_to = device(flip(y, k), flip(x, 1 - k), k)
    barrier = pltpu.get_barrier_semaphore()
    for d in range(1, n_sp):
        pl.semaphore_signal(
            barrier, inc=1, device_id={"sp": lax.rem(me_sp + d, n_sp)}, device_id_type=MESH
        )
    for d in range(1, n_tp):
        pl.semaphore_signal(
            barrier, inc=1, device_id={"tp": lax.rem(me_tp + d, n_tp)}, device_id_type=MESH
        )
    pl.semaphore_signal(barrier, inc=1, device_id=device(1 - y, x, 1 - k), device_id_type=MESH)

    high = cos_cols.shape[0]
    for g in range(tok // high):
        cos_ref[pl.ds(g * high, high), :] = cos_rows[g:g + 1, :] + cos_cols[...]
        sin_ref[pl.ds(g * high, high), :] = sin_rows[g:g + 1, :] + sin_cols[...]
    loads[0].wait()
    held[0, 0, 0] = norm_rotate(
        k_ref[...].astype(jnp.float32), kg_ref[...], cos_ref[...], sin_ref[...]
    )
    info[0, pl.ds(0, routes_ref.shape[0]), :] = routes_ref[...].astype(jnp.float32)
    info[0, pl.ds(routes_ref.shape[0], routes_ref.shape[0]), :] = share_ref[...]
    loads[1].wait()
    pl.semaphore_wait(barrier, n_sp + n_tp - 1)

    def trade(i, quarter=None):
        ref = (w_gate, w_up, w_down)[i]
        src, dst = own_any[i], ref.at[pl.ds(1, 1)]
        if quarter is not None:
            size = src.shape[1] // 4
            src = src.at[:, pl.ds(quarter * size, size)]
            dst = ref.at[pl.ds(1, 1), pl.ds(quarter * size, size)]
        return remote(src, dst, s_trade.at[i], r_trade.at[i], traded_to)

    def trade_y(*parts):
        @pl.when(k == 1)
        def _():
            for i, quarter in parts:
                trade(i, quarter).start()

    def kv_plane(r):
        return remote(held.at[0, 0], held.at[r, 0], s_kv.at[0, r], r_kv.at[0, r], at_plane(r))

    def kv_pass():
        return remote(held.at[2, 0], held.at[3, 0], s_kv.at[0, 0], r_kv.at[0, 3], at_plane(1))

    def v_plane(r):
        return remote(
            held.at[0, 1, 1], held.at[r, 1, 1], s_kv.at[1, r], r_kv.at[1, r], at_plane(r)
        )

    def v_pass():
        return remote(
            held.at[2, 1, 1], held.at[3, 1, 1], s_kv.at[1, 0], r_kv.at[1, 3], at_plane(1)
        )

    def kv_across():
        return remote(held.at[0, 0], held.at[0, 1], s_kv.at[2, 0], r_kv.at[2, 0], across)

    def k_across(r):
        return remote(
            held.at[r, 0, 0], held.at[r, 1, 0], s_kv.at[2, r], r_kv.at[2, r], across
        )

    def info_copy(r):
        return remote(info.at[0], info.at[r], s_info.at[r], r_info.at[r], at_plane(r))

    kv_across().start()
    kv_plane(1).start()
    kv_plane(2).start()

    @pl.when(middle)
    def _():
        kv_plane(3).start()

    for r in range(1, planes):
        info_copy(r).start()

    @pl.when(k == 0)
    def _():
        trade(0).start()
        trade(1).start()

    loads[2].wait()
    for j in range(n_tp):
        part = pl.ds(j * rows, rows)
        for h in range(group):
            q_rot[j, pl.ds(h * rows, rows), :] = norm_rotate(
                q_ref[part, pl.ds(h * width, width)].astype(jnp.float32),
                qg_ref[...], cos_ref[part, :], sin_ref[part, :],
            )
    top[...] = jnp.full(top.shape, -1e30, jnp.float32)
    total[...] = jnp.zeros(total.shape, jnp.float32)
    accum[...] = jnp.zeros(accum.shape, jnp.float32)
    factor = math.log2(math.e) / math.sqrt(width)
    repeat = tok // width

    def attend(r, side, j):
        scores = lax.dot_general(
            q_rot[j], held[r, side, 0], (((1,), (1,)), ((), ())),
            preferred_element_type=jnp.float32,
        )
        old = top[j]
        new = jnp.maximum(old, jnp.max(scores, axis=1, keepdims=True))
        weights = jnp.exp2((scores - jnp.concatenate([new] * repeat, axis=1)) * factor)
        alpha = jnp.exp2((old - new) * factor)
        part = weights[:, :width]
        for i in range(1, repeat):
            part = part + weights[:, i * width:(i + 1) * width]
        summed = total[j] * alpha + part
        added = jnp.dot(
            weights.astype(jnp.bfloat16), held[r, side, 1], preferred_element_type=jnp.float32
        )
        return new, summed, accum[j] * alpha + added

    def step(r, side):
        @pl.loop(0, n_tp)
        def _(j):
            new, summed, added = attend(r, side, j)
            top[j] = new
            total[j] = summed
            accum[j] = added

    def out_copy(j):
        return remote(
            rows_out.at[j], heads.at[me_tp], s_o.at[j], r_o.at[me_tp], {"tp": j}
        )

    trade_y((0, 0))
    step(0, 0)
    kv_across().wait_recv()
    v_plane(1).start()
    v_plane(2).start()

    @pl.when(middle)
    def _():
        v_plane(3).start()

    step(0, 1)
    kv_plane(1).wait_recv()
    k_across(1).start()
    trade_y((0, 1))
    step(1, 0)
    kv_plane(2).wait_recv()

    @pl.when(middle)
    def _():
        kv_pass().start()

    k_across(2).start()
    trade_y((0, 2))
    k_across(1).wait_recv()
    v_plane(1).wait_recv()
    step(1, 1)
    step(2, 0)
    kv_plane(3).wait_recv()
    k_across(3).start()
    trade_y((0, 3), (1, 0), (1, 1), (1, 2), (1, 3), (2, 0), (2, 1), (2, 2), (2, 3))
    v_plane(2).wait_recv()

    @pl.when(middle)
    def _():
        v_pass().start()

    k_across(2).wait_recv()
    step(2, 1)
    step(3, 0)
    k_across(3).wait_recv()
    v_plane(3).wait_recv()
    for d in range(n_tp):
        j = lax.rem(me_tp + (2, 3, 1, 0)[d], n_tp)
        new, summed, added = attend(3, 1, j)
        result = added / jnp.sum(summed, axis=1, keepdims=True)
        result = result.astype(jnp.bfloat16)
        for h in range(group):
            piece = result[h * rows:(h + 1) * rows]
            if d < n_tp - 1:
                rows_out[j, :, pl.ds(h * width, width)] = piece
            else:
                heads[j, :, pl.ds(h * width, width)] = piece
        if d < n_tp - 1:
            out_copy(j).start()

    @pl.when(k == 0)
    def _():
        trade(2).start()

    before = (
        lax.broadcasted_iota(jnp.int32, (rows, rows), 0)
        < lax.broadcasted_iota(jnp.int32, (rows, rows), 1)
    ).astype(jnp.float32).astype(jnp.bfloat16)
    count = lax.broadcasted_iota(jnp.int32, (cap, rows), 0).astype(jnp.float32)
    top_count = routes_ref.shape[0]
    members = []
    for t in range(4):
        core = (k, 1 - k, 0, 1)[t]
        far = t // 2
        for e in range(2):
            yy = flip(y, far * (1 - core) + e * core)
            xx = flip(x, far * core + e * (1 - core))
            members.append((z * 2 + yy) * n_tp + xx * 2 + core)
    for r in range(1, planes):
        info_copy(r).wait_recv()
    for r in range(planes):
        hits, shares = [], []
        for member in members:
            wanted = jnp.full((1, rows), member, jnp.int32).astype(jnp.float32)
            hit = jnp.zeros((1, rows), jnp.float32)
            share = jnp.zeros((1, rows), jnp.float32)
            for j in range(top_count):
                match = info[r, j:j + 1, :] == wanted
                hit = jnp.where(match, 1.0, hit)
                share = jnp.where(match, info[r, top_count + j:top_count + j + 1, :], share)
            hits.append(hit)
            shares.append(share)
        stacked = jnp.concatenate(hits, axis=0)
        earlier = jnp.dot(stacked.astype(jnp.bfloat16), before, preferred_element_type=jnp.float32)
        earlier = jnp.where(stacked > 0.5, earlier, -1.0)
        spread = []
        for n in range(len(members)):
            ones = (earlier[n:n + 1, :] == count).astype(jnp.float32)
            place[r, pl.ds(n * cap, cap), :] = ones.astype(jnp.bfloat16)
            spread.append(ones * shares[n])
        combine[r] = jnp.concatenate(spread, axis=0).T.astype(jnp.bfloat16)

    loads[3].wait()
    loads[4].wait()
    base[...] = residual[...].astype(jnp.float32)
    for d in range(n_tp):
        source = lax.rem(me_tp + (0, 1, 3, 2)[d], n_tp)
        if d > 0:
            remote(
                rows_out.at[source], heads.at[source], s_o.at[source], r_o.at[source],
                {"tp": source},
            ).wait()
        for c in range(chunks // 2):
            two = pl.ds(c * 2 * wide, 2 * wide)
            base[:, two] = base[:, two] + jnp.dot(
                heads[source],
                w_proj[pl.ds(pl.multiple_of(source * lanes, lanes), lanes), two],
                preferred_element_type=jnp.float32,
            )
    squares = jnp.zeros((rows, 1), jnp.float32)
    for c in range(chunks):
        hidden = base[:, cols(c)].astype(jnp.bfloat16).astype(jnp.float32)
        base[:, cols(c)] = hidden
        squares = squares + jnp.sum(hidden * hidden, axis=1, keepdims=True)
    scale = lax.rsqrt(squares / model + EPS)

    def z_copy(n, c):
        src, dst, r = ((0, 1, 1), (0, 3, 3), (1, 2, 3), (3, 2, 1), (2, 3, 1))[n]
        return remote(
            gathered.at[src, c], gathered.at[dst, c], s_z.at[n, c], r_z.at[dst, c], at_plane(r)
        )

    def z_wait(r, c):
        remote(
            gathered.at[0, c], gathered.at[r, c], s_z.at[0, c], r_z.at[r, c], at_plane(1)
        ).wait_recv()

    def in_copy(r, c, t):
        place_there = 1 if t == 1 else 2 + k
        return remote(
            sent.at[r, c, t - 1], arrived.at[r, c, :, place_there],
            s_in.at[r, c, t], r_in.at[r, c, place_there], (None, partner, far_y, far_x)[t],
        )

    def back_copy(r, c, i):
        place_there = 1 if i == 1 else 2 + k
        return remote(
            answers.at[r, c, :, i], returned.at[r, c, place_there],
            s_back.at[r, c, i], r_back.at[r, c, place_there],
            partner if i == 1 else sources[i - 2],
        )

    def edge_sum(n, c):
        return remote(
            partial.at[n + 1, c], edge_in.at[n, c], s_sum.at[n, c], r_edge.at[n, c], at_plane(1)
        )

    def mid_sum(n, c):
        return remote(
            partial.at[3 - n, c], mid_in.at[n, c], s_sum.at[n + 1, c], r_mid.at[n, c], at_plane(3)
        )

    for c in range(chunks):
        part = (base[:, cols(c)] * scale * ng_ref[:, cols(c)]).astype(jnp.bfloat16)
        normed[:, cols(c)] = part
        gathered[0, c] = part
        z_copy(0, c).start()

        @pl.when(middle)
        def _():
            z_copy(1, c).start()

    inner = w_gate.shape[2]

    def dispatch(r, c):
        picked = jnp.dot(
            place[r], gathered[r, c], preferred_element_type=jnp.float32
        ).astype(jnp.bfloat16)
        for t in range(4):
            for e in range(2):
                part = picked[(2 * t + e) * cap:(2 * t + e + 1) * cap]
                if t == 0:
                    arrived[r, c, e, 0] = part
                else:
                    sent[r, c, t - 1, e] = part
        for t in (2, 3, 1):
            in_copy(r, c, t).start()

    def open_half(r, half):
        span = range(half * chunks // 2, (half + 1) * chunks // 2)
        for c in span:
            for i in (1, 2, 3):
                remote(
                    sent.at[r, c, 0], arrived.at[r, c, :, i], s_in.at[r, c, 1],
                    r_in.at[r, c, i], partner,
                ).wait_recv()
        for e in range(2):
            gate = up = None
            for c in span:
                part = arrived[r, c, e].reshape(4 * cap, wide)
                more_gate = jnp.dot(part, w_gate[e, cols(c), :], preferred_element_type=jnp.float32)
                more_up = jnp.dot(part, w_up[e, cols(c), :], preferred_element_type=jnp.float32)
                gate = more_gate if gate is None else gate + more_gate
                up = more_up if up is None else up + more_up
            if half == 0:
                acc[r, e, :, pl.ds(0, inner)] = gate
                acc[r, e, :, pl.ds(inner, inner)] = up
            else:
                gate = gate + acc[r, e, :, pl.ds(0, inner)]
                up = up + acc[r, e, :, pl.ds(inner, inner)]
                hid[r, e] = (jax.nn.silu(gate) * up).astype(jnp.bfloat16)

    def answer(r, *span):
        for c in span:
            for e in range(2):
                answers[r, c, e] = jnp.dot(
                    hid[r, e], w_down[e, :, cols(c)], preferred_element_type=jnp.float32
                ).astype(jnp.bfloat16).reshape(4, cap, wide)
        for c in span:
            for i in (2, 3, 1):
                back_copy(r, c, i).start()
        for c in span:
            for e in range(2):
                returned[r, c, 0, e] = answers[r, c, e, 0]

    def collect(r, *span):
        for c in span:
            for t in range(1, 4):
                remote(
                    answers.at[r, c, :, 1], returned.at[r, c, t], s_back.at[r, c, 1],
                    r_back.at[r, c, t], partner,
                ).wait_recv()
        for c in span:
            back = jnp.concatenate(
                [returned[r, c, t, e] for t in range(4) for e in range(2)], axis=0
            )
            partial[r, c] = jnp.dot(
                combine[r], back, preferred_element_type=jnp.float32
            ).astype(jnp.bfloat16)
        if r > 0:
            @pl.when(edge)
            def _():
                for c in span:
                    edge_sum(r - 1, c).start()

    def add_on(r, c, more):
        partial[r, c] = (
            partial[r, c].astype(jnp.float32) + more.astype(jnp.float32)
        ).astype(jnp.bfloat16)

    def relay(n, c):
        @pl.when(middle)
        def _():
            if n < 2:
                edge_sum(n + 1, c).wait_recv()
                add_on(3 - n, c, edge_in[n + 1, c])
                mid_sum(n, c).start()
            else:
                mid_sum(1, c).wait_recv()
                add_on(1, c, mid_in[1, c])
                edge_sum(0, c).start()

    for i in range(5, 8):
        loads[i].wait()
    shared_gate = jnp.dot(normed[...], w_shared_gate[...], preferred_element_type=jnp.float32)
    shared_up = jnp.dot(normed[...], w_shared_up[...], preferred_element_type=jnp.float32)
    shared_hid = (jax.nn.silu(shared_gate) * shared_up).astype(jnp.bfloat16)
    for c in range(chunks):
        base[:, cols(c)] = base[:, cols(c)] + jnp.dot(
            shared_hid, w_shared_down[:, cols(c)], preferred_element_type=jnp.float32
        )

    for c in range(chunks):
        z_wait(1, c)

        @pl.when(middle)
        def _():
            z_copy(2, c).start()
            z_wait(3, c)
            z_copy(3, c).start()

        dispatch(1, c)
    loads[8].wait()
    loads[9].wait()
    trade(0).wait_recv()
    trade(1).wait_recv()
    open_half(1, 0)
    open_half(1, 1)
    loads[10].wait()
    trade(2).wait_recv()
    for n in range(0, chunks, 2):
        answer(1, n, n + 1)
    for c in range(chunks):
        z_wait(2, c)

        @pl.when(middle)
        def _():
            z_copy(4, c).start()

        dispatch(2, c)
    for n in range(0, chunks, 2):
        collect(1, n, n + 1)
    for c in range(chunks):
        @pl.when(edge)
        def _():
            z_wait(3, c)

        dispatch(3, c)
    open_half(2, 0)
    open_half(2, 1)
    for n in range(0, chunks, 2):
        answer(2, n, n + 1)
    open_half(3, 0)
    open_half(3, 1)
    for n in range(0, chunks, 2):
        answer(3, n, n + 1)
    for n in range(0, chunks, 2):
        collect(2, n, n + 1)
    for c in range(chunks):
        dispatch(0, c)
    for c in range(0, chunks, 2):
        collect(3, c, c + 1)
        relay(0, c)
        relay(0, c + 1)
    for c in range(chunks + 2):
        if c < chunks:
            relay(1, c)
        if c >= 2:
            relay(2, c - 2)
        if c == 2:
            open_half(0, 0)
            open_half(0, 1)
            for n in range(0, chunks, 2):
                answer(0, n, n + 1)
        if c >= 6:
            collect(0, 2 * (c - 6), 2 * (c - 6) + 1)

    for c in range(chunks):
        edge_sum(0, c).wait_recv()
        base[:, cols(c)] = base[:, cols(c)] + (
            partial[0, c].astype(jnp.float32) + edge_in[0, c].astype(jnp.float32)
        )

        @pl.when(middle)
        def _():
            mid_sum(0, c).wait_recv()
            base[:, cols(c)] = base[:, cols(c)] + mid_in[0, c].astype(jnp.float32)

        out_ref[:, cols(c)] = base[:, cols(c)].astype(jnp.bfloat16)

    for i in range(3):
        trade(i).wait_send()
    for r in range(1, planes):
        info_copy(r).wait_send()
        k_across(r).wait_send()
    kv_across().wait_send()
    for r in (1, 2):
        kv_plane(r).wait_send()
        v_plane(r).wait_send()

    @pl.when(middle)
    def _():
        kv_plane(3).wait_send()
        v_plane(3).wait_send()
        kv_pass().wait_send()
        v_pass().wait_send()

    for c in range(chunks):
        z_copy(0, c).wait_send()
        for n in range(3):
            edge_sum(n, c).wait_send()
        for r in range(planes):
            for n in (1, 2, 3):
                in_copy(r, c, n).wait_send()
                back_copy(r, c, n).wait_send()

        @pl.when(middle)
        def _():
            for n in range(1, 5):
                z_copy(n, c).wait_send()


def small_tables(tok, width):
    quarter = width // 4
    inverse = jnp.power(THETA, -4.0 * jnp.arange(quarter, dtype=jnp.float32) / width)
    grid_rows = tok // GRID_W
    start = lax.axis_index("sp") * grid_rows
    row_angle = (start + jnp.arange(grid_rows)).astype(jnp.float32)[:, None] * inverse
    col_angle = jnp.arange(GRID_W).astype(jnp.float32)[:, None] * inverse
    none_row, none_col = jnp.zeros_like(row_angle), jnp.zeros_like(col_angle)
    cos_row, cos_col, sin_row, sin_col = lax.optimization_barrier(
        (jnp.cos(row_angle), jnp.cos(col_angle), jnp.sin(row_angle), jnp.sin(col_angle))
    )
    return (
        jnp.concatenate([cos_row, cos_row, none_row, none_row], axis=1),
        jnp.concatenate([none_col, none_col, cos_col, cos_col], axis=1),
        jnp.concatenate([-sin_row, sin_row, none_row, none_row], axis=1),
        jnp.concatenate([none_col, none_col, -sin_col, sin_col], axis=1),
    )


def whole_layer(
    queries, keys, values, residual, out_proj, query_gain, key_gain, norm_gain,
    routes, route_weight, gate, up, down, shared_gate, shared_up, shared_down, cap,
):
    n_sp, n_tp = lax.axis_size("sp"), lax.axis_size("tp")
    tok, width = keys.shape
    lanes = queries.shape[1]
    group = lanes // width
    rows, model = residual.shape
    planes, chunks = 4, 8
    wide = model // chunks
    inner = gate.shape[2]
    tables = small_tables(tok, width)
    vmem = pl.BlockSpec(memory_space=pltpu.VMEM)
    anywhere = pl.BlockSpec(memory_space=pl.ANY)
    dma = pltpu.SemaphoreType.DMA
    low, full = jnp.bfloat16, jnp.float32
    return pl.pallas_call(
        functools.partial(layer_kernel, n_sp, n_tp, planes, cap, chunks),
        out_shape=jax.ShapeDtypeStruct((rows, model), low),
        in_specs=[vmem] * 9 + [anywhere] * 11,
        out_specs=vmem,
        scratch_shapes=[
            pltpu.VMEM(queries.shape, low),
            pltpu.VMEM(keys.shape, low),
            pltpu.VMEM(residual.shape, low),
            pltpu.VMEM(out_proj.shape, low),
            pltpu.VMEM((2,) + gate.shape[1:], low),
            pltpu.VMEM((2,) + up.shape[1:], low),
            pltpu.VMEM((2,) + down.shape[1:], low),
            pltpu.VMEM(shared_gate.shape, low),
            pltpu.VMEM(shared_up.shape, low),
            pltpu.VMEM(shared_down.shape, low),
            pltpu.VMEM((tok, width), full),
            pltpu.VMEM((tok, width), full),
            pltpu.VMEM((planes, 2, 2, tok, width), low),
            pltpu.VMEM((n_tp, group * rows, width), low),
            pltpu.VMEM((n_tp, group * rows, width), full),
            pltpu.VMEM((n_tp, group * rows, width), full),
            pltpu.VMEM((n_tp, group * rows, width), full),
            pltpu.VMEM((n_tp, rows, lanes), low),
            pltpu.VMEM((n_tp, rows, lanes), low),
            pltpu.VMEM((rows, model), low),
            pltpu.VMEM((planes, 2 * routes.shape[1], rows), full),
            pltpu.VMEM((planes, chunks, rows, wide), low),
            pltpu.VMEM((planes, chunks, 3, 2, cap, wide), low),
            pltpu.VMEM((planes, chunks, 2, 4, cap, wide), low),
            pltpu.VMEM((planes, chunks, 4, 2, cap, wide), low),
            pltpu.VMEM((planes, chunks, rows, wide), low),
            pltpu.VMEM((3, chunks, rows, wide), low),
            pltpu.VMEM((2, chunks, rows, wide), low),
            pltpu.VMEM((planes, 8 * cap, rows), low),
            pltpu.VMEM((planes, rows, 8 * cap), low),
            pltpu.VMEM((planes, 2, 4 * cap, 2 * inner), full),
            pltpu.VMEM((planes, 2, 4 * cap, inner), low),
            pltpu.VMEM((rows, model), full),
            dma((11,)), dma((3, planes)), dma((3, planes)),
            dma((n_tp,)), dma((n_tp,)), dma((3,)), dma((3,)),
            dma((planes,)), dma((planes,)),
            dma((5, chunks)), dma((planes, chunks)),
            dma((planes, chunks, 4)), dma((planes, chunks, 4)),
            dma((planes, chunks, 4)), dma((planes, chunks, 4)),
            dma((3, chunks)), dma((3, chunks)), dma((2, chunks)),
        ],
        compiler_params=pltpu.CompilerParams(
            collective_id=2, has_side_effects=True, vmem_limit_bytes=61 * 2**20
        ),
        name="layer",
    )(
        *tables, query_gain.reshape(1, width), key_gain.reshape(1, width),
        norm_gain.reshape(1, model), routes.T, route_weight.T,
        queries, keys, values, residual, out_proj,
        gate, up, down, shared_gate, shared_up, shared_down,
    )


def body(
    queries,
    keys,
    values,
    residual,
    out_proj,
    query_gain,
    key_gain,
    norm_gain,
    routes,
    route_weight,
    expert_gate,
    expert_up,
    expert_down,
    shared_gate,
    shared_up,
    shared_down,
):
    n_sp, n_tp = lax.axis_size("sp"), lax.axis_size("tp")
    rows_local, top_count = routes.shape
    expert_total = expert_gate.shape[0] * n_sp * n_tp
    capacity = max(2, 2 * rows_local * top_count // expert_total)
    if n_sp == 8 and n_tp == 4 and expert_gate.shape[0] == 1 and capacity % 16 == 0:
        return whole_layer(
            queries, keys, values, residual, out_proj, query_gain, key_gain, norm_gain,
            routes, route_weight, expert_gate, expert_up, expert_down,
            shared_gate, shared_up, shared_down, capacity,
        )
    all_heads = attention(n_sp, n_tp, queries, keys, values, query_gain, key_gain)
    projected = jnp.dot(all_heads, out_proj, preferred_element_type=jnp.float32)
    hidden1 = (residual.astype(jnp.float32) + projected).astype(jnp.bfloat16)
    hidden_f = hidden1.astype(jnp.float32)
    normed = (
        hidden_f
        * lax.rsqrt(jnp.mean(hidden_f * hidden_f, axis=-1, keepdims=True) + EPS)
        * norm_gain
    ).astype(jnp.bfloat16)
    pair_count = rows_local * top_count
    flat_routes = routes.reshape(pair_count)
    one_hot = (flat_routes[:, None] == jnp.arange(expert_total, dtype=jnp.int32)[None, :]).astype(
        jnp.float32
    )
    lower = (jnp.arange(pair_count)[:, None] >= jnp.arange(pair_count)[None, :]).astype(jnp.float32)
    running_count = jnp.dot(lower, one_hot, precision=lax.Precision.HIGHEST)
    slot_place = (jnp.sum(running_count * one_hot, axis=1) - 1.0).astype(jnp.int32)
    slot_index = flat_routes * capacity + slot_place
    slots = slot_index.reshape(rows_local, top_count).astype(jnp.float32)
    info = jnp.concatenate([slots.T, route_weight.T], axis=0)
    layer_out = routed_experts(
        info, normed, hidden1, expert_gate, expert_up, expert_down,
        shared_gate, shared_up, shared_down, capacity,
    )
    return layer_out.astype(jnp.bfloat16)


def solution(mesh):
    placed = (
        P("sp", "tp"),
        P("sp", "tp"),
        P("sp", "tp"),
        P(("sp", "tp"), None),
        P(),
        P(),
        P(),
        P(),
        P(("sp", "tp"), None),
        P(("sp", "tp"), None),
        P(("sp", "tp"), None, None),
        P(("sp", "tp"), None, None),
        P(("sp", "tp"), None, None),
        P(),
        P(),
        P(),
    )
    return jax.shard_map(
        body, mesh=mesh, in_specs=placed, out_specs=P(("sp", "tp"), None), check_vma=False
    )
```

```python
import functools
import math

import jax
import jax.numpy as jnp
from jax import lax
from jax.experimental import pallas as pl
from jax.experimental.pallas import tpu as pltpu
from jax.sharding import PartitionSpec as P

GRID_W = 64
MESH = pl.DeviceIdType.MESH


EPS = 1e-06
THETA = 10000.0


def norm_rotate(block, gain, cosine, sine):
    mean = jnp.mean(block * block, axis=-1, keepdims=True)
    block = block * lax.rsqrt(mean + EPS) * gain
    quarter = block.shape[-1] // 4
    lane = lax.broadcasted_iota(jnp.int32, block.shape, 1)
    after = pltpu.roll(block, 3 * quarter, 1)
    before = pltpu.roll(block, quarter, 1)
    partner = jnp.where((lane // quarter) % 2 == 0, after, before)
    return (block * cosine + partner * sine).astype(jnp.bfloat16)


def plane_peer(z, d, planes):
    if planes == 4:
        return (z + 1 - 2 * (z % 2), z + 2 - 4 * (z // 2), 3 - z)[d - 1]
    return planes - 1 - z


def attention_kernel(
    n_sp, n_tp, planes, group,
    q_ref, k_ref, v_ref, cos_ref, sin_ref, qg_ref, kg_ref, out_ref,
    held, q_rot, top, total, accum, rows_out,
    send_z, send_y, recv_kv, send_o, recv_o,
):
    per = n_sp // planes
    me_sp = lax.axis_index("sp")
    me_tp = lax.axis_index("tp")
    z, y = me_sp // per, me_sp % per
    tok, width = k_ref.shape
    piece = tok // n_tp
    lanes = group * width
    held[me_sp, 0] = norm_rotate(
        k_ref[...].astype(jnp.float32), kg_ref[...], cos_ref[...], sin_ref[...]
    )
    held[me_sp, 1] = v_ref[...]
    barrier = pltpu.get_barrier_semaphore()
    for d in range(1, n_sp):
        pl.semaphore_signal(
            barrier, inc=1, device_id={"sp": lax.rem(me_sp + d, n_sp)}, device_id_type=MESH
        )
    for d in range(1, n_tp):
        pl.semaphore_signal(
            barrier, inc=1, device_id={"tp": lax.rem(me_tp + d, n_tp)}, device_id_type=MESH
        )
    pl.semaphore_wait(barrier, n_sp + n_tp - 2)

    def block_copy(block, target, sem):
        return pltpu.make_async_remote_copy(
            src_ref=held.at[block], dst_ref=held.at[block],
            send_sem=sem, recv_sem=recv_kv.at[block],
            device_id={"sp": target}, device_id_type=MESH,
        )

    def to_plane(slot, block):
        for d in range(1, per):
            block_copy(block, z * per + lax.rem(y + d, per), send_y.at[slot, d - 1]).start()

    for d in range(1, planes):
        if d == 1:
            block_copy(me_sp, plane_peer(z, d, planes) * per + y, send_z.at[d - 1]).start()
            to_plane(0, me_sp)
        else:
            block_copy(me_sp, plane_peer(z, d, planes) * per + y, send_z.at[d - 1]).start()
    for j in range(n_tp):
        rows = pl.ds(j * piece, piece)
        for h in range(group):
            q_rot[j, pl.ds(h * piece, piece), :] = norm_rotate(
                q_ref[rows, pl.ds(h * width, width)].astype(jnp.float32),
                qg_ref[...], cos_ref[rows, :], sin_ref[rows, :],
            )
    top[...] = jnp.full(top.shape, -1e30, jnp.float32)
    total[...] = jnp.zeros(total.shape, jnp.float32)
    accum[...] = jnp.zeros(accum.shape, jnp.float32)
    factor = math.log2(math.e) / math.sqrt(width)
    repeat = tok // width

    def attend(block, j):
        scores = lax.dot_general(
            q_rot[j], held[block, 0], (((1,), (1,)), ((), ())),
            preferred_element_type=jnp.float32,
        )
        old = top[j]
        new = jnp.maximum(old, jnp.max(scores, axis=1, keepdims=True))
        weights = jnp.exp2((scores - jnp.concatenate([new] * repeat, axis=1)) * factor)
        alpha = jnp.exp2((old - new) * factor)
        part = weights[:, :width]
        for r in range(1, repeat):
            part = part + weights[:, r * width:(r + 1) * width]
        summed = total[j] * alpha + part
        added = jnp.dot(
            weights.astype(jnp.bfloat16), held[block, 1], preferred_element_type=jnp.float32
        )
        return new, summed, accum[j] * alpha + added

    def out_copy(j):
        return pltpu.make_async_remote_copy(
            src_ref=rows_out.at[j],
            dst_ref=out_ref.at[:, pl.ds(pl.multiple_of(me_tp * lanes, 128), lanes)],
            send_sem=send_o.at[j], recv_sem=recv_o.at[me_tp],
            device_id={"tp": j}, device_id_type=MESH,
        )

    def step(block):
        @pl.loop(0, n_tp)
        def _(j):
            new, summed, acc = attend(block, j)
            top[j] = new
            total[j] = summed
            accum[j] = acc

    def arrive(block):
        block_copy(block, me_sp, send_z.at[0]).wait_recv()

    def others(plane, finish=False):
        for d in range(1, per):
            block = plane * per + lax.rem(y + d, per)
            arrive(block)
            step(block)

    step(me_sp)
    previous = z
    for d in range(1, planes):
        plane = plane_peer(z, d, planes)
        block = plane * per + y
        arrive(block)
        to_plane(d, block)
        others(previous)
        step(block)
        previous = plane
    others(previous)

    for d in range(n_tp):
        j = lax.rem(me_tp + 1 + d, n_tp)
        result = accum[j] / jnp.sum(total[j], axis=1, keepdims=True)
        result = result.astype(jnp.bfloat16)
        for h in range(group):
            rows_out[j, :, pl.ds(h * width, width)] = result[h * piece:(h + 1) * piece]
        if d < n_tp - 1:
            out_copy(j).start()
        else:
            for h in range(group):
                out_ref[:, pl.ds(pl.multiple_of(me_tp * lanes + h * width, 128), width)] = result[
                    h * piece:(h + 1) * piece
                ]
    for d in range(1, n_tp):
        source = lax.rem(me_tp + d, n_tp)
        pltpu.make_async_remote_copy(
            src_ref=rows_out.at[source],
            dst_ref=out_ref.at[:, pl.ds(pl.multiple_of(source * lanes, 128), lanes)],
            send_sem=send_o.at[source], recv_sem=recv_o.at[source],
            device_id={"tp": source}, device_id_type=MESH,
        ).wait()
    for d in range(1, planes):
        block_copy(me_sp, me_sp, send_z.at[d - 1]).wait_send()
    for slot in range(planes):
        for d in range(1, per):
            block_copy(me_sp, me_sp, send_y.at[slot, d - 1]).wait_send()


def angle_tables(tok, width):
    quarter = width // 4
    inverse = jnp.power(THETA, -4.0 * jnp.arange(quarter, dtype=jnp.float32) / width)
    start = lax.axis_index("sp") * tok
    grid_rows = tok // GRID_W
    row_angle = (start // GRID_W + jnp.arange(grid_rows)).astype(jnp.float32)[:, None] * inverse
    col_angle = jnp.arange(GRID_W).astype(jnp.float32)[:, None] * inverse

    def spread(row_part, col_part, sign):
        row_part = jnp.broadcast_to(row_part[:, None, :], (grid_rows, GRID_W, quarter))
        col_part = jnp.broadcast_to(col_part[None, :, :], (grid_rows, GRID_W, quarter))
        return jnp.concatenate(
            [sign * row_part, row_part, sign * col_part, col_part], axis=-1
        ).reshape(tok, width)

    tables = lax.optimization_barrier(
        (jnp.cos(row_angle), jnp.cos(col_angle), jnp.sin(row_angle), jnp.sin(col_angle))
    )
    return spread(tables[0], tables[1], 1.0), spread(tables[2], tables[3], -1.0)


def attention(mesh_sp, mesh_tp, queries, keys, values, query_gain, key_gain):
    tok, width = keys.shape
    group = queries.shape[1] // width
    planes = 4 if mesh_sp % 4 == 0 else 2
    per = mesh_sp // planes
    piece = tok // mesh_tp
    cosine, sine = angle_tables(tok, width)
    vmem = pl.BlockSpec(memory_space=pltpu.VMEM)
    return pl.pallas_call(
        functools.partial(attention_kernel, mesh_sp, mesh_tp, planes, group),
        out_shape=jax.ShapeDtypeStruct((piece, mesh_tp * group * width), jnp.bfloat16),
        in_specs=[vmem] * 7,
        out_specs=vmem,
        scratch_shapes=[
            pltpu.VMEM((mesh_sp, 2, tok, width), jnp.bfloat16),
            pltpu.VMEM((mesh_tp, group * piece, width), jnp.bfloat16),
            pltpu.VMEM((mesh_tp, group * piece, width), jnp.float32),
            pltpu.VMEM((mesh_tp, group * piece, width), jnp.float32),
            pltpu.VMEM((mesh_tp, group * piece, width), jnp.float32),
            pltpu.VMEM((mesh_tp, piece, group * width), jnp.bfloat16),
            pltpu.SemaphoreType.DMA((planes - 1,)),
            pltpu.SemaphoreType.DMA((planes, max(per - 1, 1))),
            pltpu.SemaphoreType.DMA((mesh_sp,)),
            pltpu.SemaphoreType.DMA((mesh_tp,)),
            pltpu.SemaphoreType.DMA((mesh_tp,)),
        ],
        compiler_params=pltpu.CompilerParams(
            collective_id=0, has_side_effects=True, vmem_limit_bytes=40 * 2**20
        ),
        name="attention",
    )(queries, keys, values, cosine, sine, query_gain.reshape(1, width), key_gain.reshape(1, width))


def expert_kernel(
    n_sp, n_tp, planes, cap, top_count, chunks,
    info_ref, normed_ref, hidden_ref, gate_ref, up_ref, down_ref,
    sgate_ref, sup_ref, sdown_ref, out_ref,
    info, gathered, sent, arrived, answers, returned, partial, sums,
    place, combine, acc, hid,
    s_info, r_info, s_z, r_z, s_in, r_in, s_back, r_back, s_sum, r_sum,
):
    per = n_sp // planes
    team = per * n_tp
    me_sp = lax.axis_index("sp")
    me_tp = lax.axis_index("tp")
    z, y = me_sp // per, me_sp % per
    me = y * n_tp + me_tp
    rows = normed_ref.shape[0]
    wide = normed_ref.shape[1] // chunks
    share = planes * cap
    slots = team * share
    tile = math.gcd(slots, 256)

    def in_plane(p):
        return {"sp": z * per + p // n_tp, "tp": p % n_tp}

    def at_plane(d):
        return {"sp": plane_peer(z, d, planes) * per + y}

    def block(p, size):
        return pl.ds(pl.multiple_of(p * size, size), size)

    def remote(src, dst, send, recv, target):
        return pltpu.make_async_remote_copy(
            src_ref=src, dst_ref=dst, send_sem=send, recv_sem=recv,
            device_id=target, device_id_type=MESH,
        )

    def cols(c):
        return pl.ds(c * wide, wide)

    barrier = pltpu.get_barrier_semaphore()

    @pl.loop(1, team)
    def _(d):
        pl.semaphore_signal(
            barrier, inc=1, device_id=in_plane(lax.rem(me + d, team)), device_id_type=MESH
        )

    for d in range(1, planes):
        pl.semaphore_signal(barrier, inc=1, device_id=at_plane(d), device_id_type=MESH)
    pl.semaphore_wait(barrier, team + planes - 2)

    def info_copy(d, source):
        return remote(info_ref, info.at[source], s_info.at[d], r_info.at[source], at_plane(d))

    def z_copy(c, d, source):
        return remote(
            normed_ref.at[:, cols(c)], gathered.at[c, block(source, rows)],
            s_z.at[c, d], r_z.at[c, source], at_plane(d),
        )

    def in_copy(c, p, source):
        return remote(
            sent.at[c, block(p, share)], arrived.at[c, block(source, share)],
            s_in.at[c, p], r_in.at[c, source], in_plane(p),
        )

    def back_copy(c, p, source):
        return remote(
            answers.at[c, block(p, share)], returned.at[c, block(source, share)],
            s_back.at[c, p], r_back.at[c, source], in_plane(p),
        )

    def sum_copy(c, d, source):
        return remote(
            partial.at[c, block(plane_peer(z, d, planes), rows)], sums.at[c, source],
            s_sum.at[c, d], r_sum.at[c, source], at_plane(d),
        )

    for d in range(1, planes):
        info_copy(d, z).start()
    for c in range(chunks):
        for d in range(1, planes):
            z_copy(c, d, z).start()
        gathered[c, block(z, rows)] = normed_ref[:, cols(c)]
    info[z] = info_ref[...]

    shared_gate = jnp.dot(normed_ref[...], sgate_ref[...], preferred_element_type=jnp.float32)
    shared_up = jnp.dot(normed_ref[...], sup_ref[...], preferred_element_type=jnp.float32)
    shared_hid = (jax.nn.silu(shared_gate) * shared_up).astype(jnp.bfloat16)
    for c in range(chunks):
        out_ref[:, cols(c)] = jnp.dot(
            shared_hid, sdown_ref[:, cols(c)], preferred_element_type=jnp.float32
        ) + hidden_ref[:, cols(c)].astype(jnp.float32)

    number = lax.broadcasted_iota(jnp.int32, (slots, rows), 0)
    owner = (number // cap) % planes
    slot = ((z * team + number // share) * cap + number % cap).astype(jnp.float32)
    for d in range(1, planes):
        info_copy(d, plane_peer(z, d, planes)).wait_recv()
    for plane in range(planes):
        wanted = jnp.where(owner == plane, slot, -1.0)
        ones = jnp.zeros((slots, rows), jnp.float32)
        shares = jnp.zeros((slots, rows), jnp.float32)
        for k in range(top_count):
            match = wanted == info[plane, k:k + 1, :]
            ones = jnp.where(match, 1.0, ones)
            shares = jnp.where(match, info[plane, top_count + k:top_count + k + 1, :], shares)
        place[:, pl.ds(plane * rows, rows)] = ones.astype(jnp.bfloat16)
        combine[pl.ds(plane * rows, rows), :] = shares.T.astype(jnp.bfloat16)

    for c in range(chunks):
        for d in range(1, planes):
            z_copy(c, d, plane_peer(z, d, planes)).wait_recv()

        @pl.loop(0, slots // tile)
        def _(i):
            sent[c, block(i, tile)] = jnp.dot(
                place[block(i, tile), :], gathered[c], preferred_element_type=jnp.float32
            ).astype(jnp.bfloat16)

        @pl.loop(1, team)
        def _(d):
            in_copy(c, lax.rem(me + d, team), me).start()

        arrived[c, block(me, share)] = sent[c, block(me, share)]

    inner = gate_ref.shape[2]
    for c in range(chunks):
        @pl.loop(1, team)
        def _(d):
            source = lax.rem(me + d, team)
            in_copy(c, source, source).wait_recv()

        @pl.loop(0, slots // tile)
        def _(i):
            part = arrived[c, block(i, tile)]
            gate = jnp.dot(part, gate_ref[0, cols(c), :], preferred_element_type=jnp.float32)
            up = jnp.dot(part, up_ref[0, cols(c), :], preferred_element_type=jnp.float32)
            if c > 0:
                gate = gate + acc[block(i, tile), pl.ds(0, inner)]
                up = up + acc[block(i, tile), pl.ds(inner, inner)]
            if c < chunks - 1:
                acc[block(i, tile), pl.ds(0, inner)] = gate
                acc[block(i, tile), pl.ds(inner, inner)] = up
            else:
                hid[block(i, tile), :] = (jax.nn.silu(gate) * up).astype(jnp.bfloat16)

    for c in range(chunks):
        @pl.loop(0, slots // tile)
        def _(i):
            answers[c, block(i, tile)] = jnp.dot(
                hid[block(i, tile), :], down_ref[0, :, cols(c)],
                preferred_element_type=jnp.float32,
            ).astype(jnp.bfloat16)

        @pl.loop(1, team)
        def _(d):
            back_copy(c, lax.rem(me + d, team), me).start()

        returned[c, block(me, share)] = answers[c, block(me, share)]

    for c in range(chunks):
        @pl.loop(1, team)
        def _(d):
            source = lax.rem(me + d, team)
            back_copy(c, source, source).wait_recv()

        @pl.loop(0, planes)
        def _(i):
            partial[c, block(i, rows)] = jnp.dot(
                combine[block(i, rows), :], returned[c], preferred_element_type=jnp.float32
            ).astype(jnp.bfloat16)

        for d in range(1, planes):
            sum_copy(c, d, z).start()
        sums[c, z] = partial[c, block(z, rows)]

    for c in range(chunks):
        for d in range(1, planes):
            sum_copy(c, d, plane_peer(z, d, planes)).wait_recv()
        result = out_ref[:, cols(c)]
        for plane in range(planes):
            result = result + sums[c, plane].astype(jnp.float32)
        out_ref[:, cols(c)] = result

    for d in range(1, planes):
        info_copy(d, z).wait_send()
    for c in range(chunks):
        for d in range(1, planes):
            z_copy(c, d, z).wait_send()
            sum_copy(c, d, z).wait_send()

        @pl.loop(1, team)
        def _(d):
            p = lax.rem(me + d, team)
            in_copy(c, p, me).wait_send()
            back_copy(c, p, me).wait_send()


def routed_experts(
    info, normed, hidden1, gate, up, down, shared_gate, shared_up, shared_down, cap
):
    n_sp, n_tp = lax.axis_size("sp"), lax.axis_size("tp")
    rows, model = normed.shape
    planes = 4 if n_sp % 4 == 0 else 2
    team = n_sp // planes * n_tp
    chunks = 8
    wide = model // chunks
    slots = team * planes * cap
    inner = gate.shape[2]
    top_count = info.shape[0] // 2
    vmem = pl.BlockSpec(memory_space=pltpu.VMEM)
    dma = pltpu.SemaphoreType.DMA
    return pl.pallas_call(
        functools.partial(expert_kernel, n_sp, n_tp, planes, cap, top_count, chunks),
        out_shape=jax.ShapeDtypeStruct((rows, model), jnp.float32),
        in_specs=[vmem] * 9,
        out_specs=vmem,
        scratch_shapes=[
            pltpu.VMEM((planes,) + info.shape, jnp.float32),
            pltpu.VMEM((chunks, planes * rows, wide), jnp.bfloat16),
            pltpu.VMEM((chunks, slots, wide), jnp.bfloat16),
            pltpu.VMEM((chunks, slots, wide), jnp.bfloat16),
            pltpu.VMEM((chunks, slots, wide), jnp.bfloat16),
            pltpu.VMEM((chunks, slots, wide), jnp.bfloat16),
            pltpu.VMEM((chunks, planes * rows, wide), jnp.bfloat16),
            pltpu.VMEM((chunks, planes, rows, wide), jnp.bfloat16),
            pltpu.VMEM((slots, planes * rows), jnp.bfloat16),
            pltpu.VMEM((planes * rows, slots), jnp.bfloat16),
            pltpu.VMEM((slots, 2 * inner), jnp.float32),
            pltpu.VMEM((slots, inner), jnp.bfloat16),
            dma((planes,)), dma((planes,)),
            dma((chunks, planes)), dma((chunks, planes)),
            dma((chunks, team)), dma((chunks, team)),
            dma((chunks, team)), dma((chunks, team)),
            dma((chunks, planes)), dma((chunks, planes)),
        ],
        compiler_params=pltpu.CompilerParams(
            collective_id=1, has_side_effects=True, vmem_limit_bytes=56 * 2**20
        ),
        name="experts",
    )(info, normed, hidden1, gate, up, down, shared_gate, shared_up, shared_down)


def layer_kernel(
    n_sp, n_tp, planes, cap, chunks,
    cos_rows, cos_cols, sin_rows, sin_cols, qg_ref, kg_ref, ng_ref, routes_ref, share_ref,
    q_any, k_any, v_any, residual_any, proj_any, *rest,
):
    own_any, shared_any, out_ref, rest = rest[:3], rest[3:6], rest[6], rest[7:]
    (
        q_ref, k_ref, residual, w_proj, w_gate, w_up, w_down,
        w_shared_gate, w_shared_up, w_shared_down,
        cos_ref, sin_ref, held, q_rot, top, total, accum, rows_out, heads, normed,
        info, gathered, sent, arrived, returned, partial, edge_in, mid_in,
        place, combine, acc, hid, base,
        s_load, s_kv, r_kv, s_o, r_o, s_trade, r_trade,
        s_info, r_info, s_z, r_z, s_in, r_in, s_back, r_back, s_sum, r_edge, r_mid,
    ) = rest
    answers = arrived
    me_sp = lax.axis_index("sp")
    me_tp = lax.axis_index("tp")
    z, y = me_sp // 2, lax.rem(me_sp, 2)
    x, k = me_tp // 2, lax.rem(me_tp, 2)
    middle = jnp.logical_or(z == 1, z == 2)
    edge = jnp.logical_or(z == 0, z == 3)
    tok, width = k_ref.shape
    group = q_ref.shape[1] // width
    rows = tok // n_tp
    lanes = group * width
    model = w_proj.shape[1]
    wide = model // chunks

    def flip(bit, by):
        return bit + by * (1 - 2 * bit)

    def device(yy, xx, kk):
        return {"sp": z * 2 + yy, "tp": xx * 2 + kk}

    def plane_of(r):
        return (z, flip(lax.rem(z, 2), 1) + z // 2 * 2, lax.rem(z + 2, 4), 3 - z)[r]

    def at_plane(r):
        return {"sp": plane_of(r) * 2 + y}

    def remote(src, dst, send, recv, target):
        return pltpu.make_async_remote_copy(
            src_ref=src, dst_ref=dst, send_sem=send, recv_sem=recv,
            device_id=target, device_id_type=MESH,
        )

    def cols(c):
        return pl.ds(c * wide, wide)

    pairs = [
        (k_any, k_ref), (v_any, held.at[0, 0, 1]), (q_any, q_ref), (residual_any, residual),
        (proj_any, w_proj),
        (shared_any[0], w_shared_gate), (shared_any[1], w_shared_up), (shared_any[2], w_shared_down),
        (own_any[0], w_gate.at[pl.ds(0, 1)]), (own_any[1], w_up.at[pl.ds(0, 1)]),
        (own_any[2], w_down.at[pl.ds(0, 1)]),
    ]
    loads = [pltpu.make_async_copy(src, dst, s_load.at[i]) for i, (src, dst) in enumerate(pairs)]
    for load in loads:
        load.start()

    partner = device(y, x, 1 - k)
    far_y = device(1 - y, x, 0)
    far_x = device(y, 1 - x, 1)
    sources = [device(flip(y, 1 - k), flip(x, k), core) for core in range(2)]
    across = {"sp": z * 2 + 1 - y}
    traded_to = device(flip(y, k), flip(x, 1 - k), k)
    barrier = pltpu.get_barrier_semaphore()
    for d in range(1, n_sp):
        pl.semaphore_signal(
            barrier, inc=1, device_id={"sp": lax.rem(me_sp + d, n_sp)}, device_id_type=MESH
        )
    for d in range(1, n_tp):
        pl.semaphore_signal(
            barrier, inc=1, device_id={"tp": lax.rem(me_tp + d, n_tp)}, device_id_type=MESH
        )
    pl.semaphore_signal(barrier, inc=1, device_id=device(1 - y, x, 1 - k), device_id_type=MESH)

    high = cos_cols.shape[0]
    for g in range(tok // high):
        cos_ref[pl.ds(g * high, high), :] = cos_rows[g:g + 1, :] + cos_cols[...]
        sin_ref[pl.ds(g * high, high), :] = sin_rows[g:g + 1, :] + sin_cols[...]
    loads[0].wait()
    held[0, 0, 0] = norm_rotate(
        k_ref[...].astype(jnp.float32), kg_ref[...], cos_ref[...], sin_ref[...]
    )
    info[0, pl.ds(0, routes_ref.shape[0]), :] = routes_ref[...].astype(jnp.float32)
    info[0, pl.ds(routes_ref.shape[0], routes_ref.shape[0]), :] = share_ref[...]
    loads[1].wait()
    pl.semaphore_wait(barrier, n_sp + n_tp - 1)

    def trade(i, quarter=None):
        ref = (w_gate, w_up, w_down)[i]
        src, dst = own_any[i], ref.at[pl.ds(1, 1)]
        if quarter is not None:
            size = src.shape[1] // 4
            src = src.at[:, pl.ds(quarter * size, size)]
            dst = ref.at[pl.ds(1, 1), pl.ds(quarter * size, size)]
        return remote(src, dst, s_trade.at[i], r_trade.at[i], traded_to)

    def trade_y(*parts):
        @pl.when(k == 1)
        def _():
            for i, quarter in parts:
                trade(i, quarter).start()

    def kv_plane(r):
        return remote(held.at[0, 0], held.at[r, 0], s_kv.at[0, r], r_kv.at[0, r], at_plane(r))

    def kv_pass():
        return remote(held.at[2, 0], held.at[3, 0], s_kv.at[0, 0], r_kv.at[0, 3], at_plane(1))

    def v_plane(r):
        return remote(
            held.at[0, 1, 1], held.at[r, 1, 1], s_kv.at[1, r], r_kv.at[1, r], at_plane(r)
        )

    def v_pass():
        return remote(
            held.at[2, 1, 1], held.at[3, 1, 1], s_kv.at[1, 0], r_kv.at[1, 3], at_plane(1)
        )

    def kv_across():
        return remote(held.at[0, 0], held.at[0, 1], s_kv.at[2, 0], r_kv.at[2, 0], across)

    def k_across(r):
        return remote(
            held.at[r, 0, 0], held.at[r, 1, 0], s_kv.at[2, r], r_kv.at[2, r], across
        )

    def info_copy(r):
        return remote(info.at[0], info.at[r], s_info.at[r], r_info.at[r], at_plane(r))

    kv_across().start()
    kv_plane(1).start()
    kv_plane(2).start()

    @pl.when(middle)
    def _():
        kv_plane(3).start()

    for r in range(1, planes):
        info_copy(r).start()

    @pl.when(k == 0)
    def _():
        trade(0).start()
        trade(1).start()
    loads[2].wait()
    for j in range(n_tp):
        part = pl.ds(j * rows, rows)
        for h in range(group):
            q_rot[j, pl.ds(h * rows, rows), :] = norm_rotate(
                q_ref[part, pl.ds(h * width, width)].astype(jnp.float32),
                qg_ref[...], cos_ref[part, :], sin_ref[part, :],
            )
    top[...] = jnp.full(top.shape, -1e30, jnp.float32)
    total[...] = jnp.zeros(total.shape, jnp.float32)
    accum[...] = jnp.zeros(accum.shape, jnp.float32)
    factor = math.log2(math.e) / math.sqrt(width)
    repeat = tok // width

    def attend(r, side, j):
        scores = lax.dot_general(
            q_rot[j], held[r, side, 0], (((1,), (1,)), ((), ())),
            preferred_element_type=jnp.float32,
        )
        old = top[j]
        new = jnp.maximum(old, jnp.max(scores, axis=1, keepdims=True))
        weights = jnp.exp2((scores - jnp.concatenate([new] * repeat, axis=1)) * factor)
        alpha = jnp.exp2((old - new) * factor)
        part = weights[:, :width]
        for i in range(1, repeat):
            part = part + weights[:, i * width:(i + 1) * width]
        summed = total[j] * alpha + part
        added = jnp.dot(
            weights.astype(jnp.bfloat16), held[r, side, 1], preferred_element_type=jnp.float32
        )
        return new, summed, accum[j] * alpha + added

    def step(r, side):
        @pl.loop(0, n_tp)
        def _(j):
            new, summed, added = attend(r, side, j)
            top[j] = new
            total[j] = summed
            accum[j] = added

    def out_copy(j):
        return remote(
            rows_out.at[j], heads.at[me_tp], s_o.at[j], r_o.at[me_tp], {"tp": j}
        )

    trade_y((0, 0), (0, 1))
    step(0, 0)
    kv_across().wait_recv()
    v_plane(1).start()
    v_plane(2).start()

    @pl.when(middle)
    def _():
        v_plane(3).start()

    step(0, 1)
    kv_plane(1).wait_recv()
    k_across(1).start()
    trade_y((0, 2))
    step(1, 0)
    kv_plane(2).wait_recv()

    @pl.when(middle)
    def _():
        kv_pass().start()

    k_across(2).start()
    trade_y((0, 3))
    k_across(1).wait_recv()
    v_plane(1).wait_recv()
    step(1, 1)
    step(2, 0)
    kv_plane(3).wait_recv()
    k_across(3).start()
    trade_y((1, 0), (1, 1), (1, 2), (1, 3), (2, 0), (2, 1), (2, 2), (2, 3))
    v_plane(2).wait_recv()

    @pl.when(middle)
    def _():
        v_pass().start()

    k_across(2).wait_recv()
    step(2, 1)
    step(3, 0)
    k_across(3).wait_recv()
    v_plane(3).wait_recv()
    for d in range(n_tp):
        j = lax.rem(me_tp + (2, 3, 1, 0)[d], n_tp)
        new, summed, added = attend(3, 1, j)
        result = added / jnp.sum(summed, axis=1, keepdims=True)
        result = result.astype(jnp.bfloat16)
        for h in range(group):
            piece = result[h * rows:(h + 1) * rows]
            if d < n_tp - 1:
                rows_out[j, :, pl.ds(h * width, width)] = piece
            else:
                heads[j, :, pl.ds(h * width, width)] = piece
        if d < n_tp - 1:
            out_copy(j).start()

    @pl.when(k == 0)
    def _():
        trade(2).start()

    before = (
        lax.broadcasted_iota(jnp.int32, (rows, rows), 0)
        < lax.broadcasted_iota(jnp.int32, (rows, rows), 1)
    ).astype(jnp.float32).astype(jnp.bfloat16)
    count = lax.broadcasted_iota(jnp.int32, (cap, rows), 0).astype(jnp.float32)
    top_count = routes_ref.shape[0]
    members = []
    for t in range(4):
        core = (k, 1 - k, 0, 1)[t]
        far = t // 2
        for e in range(2):
            yy = flip(y, far * (1 - core) + e * core)
            xx = flip(x, far * core + e * (1 - core))
            members.append((z * 2 + yy) * n_tp + xx * 2 + core)
    for r in range(1, planes):
        info_copy(r).wait_recv()
    for r in range(planes):
        hits, shares = [], []
        for member in members:
            wanted = jnp.full((1, rows), member, jnp.int32).astype(jnp.float32)
            hit = jnp.zeros((1, rows), jnp.float32)
            share = jnp.zeros((1, rows), jnp.float32)
            for j in range(top_count):
                match = info[r, j:j + 1, :] == wanted
                hit = jnp.where(match, 1.0, hit)
                share = jnp.where(match, info[r, top_count + j:top_count + j + 1, :], share)
            hits.append(hit)
            shares.append(share)
        stacked = jnp.concatenate(hits, axis=0)
        earlier = jnp.dot(stacked.astype(jnp.bfloat16), before, preferred_element_type=jnp.float32)
        earlier = jnp.where(stacked > 0.5, earlier, -1.0)
        spread = []
        for n in range(len(members)):
            ones = (earlier[n:n + 1, :] == count).astype(jnp.float32)
            place[r, pl.ds(n * cap, cap), :] = ones.astype(jnp.bfloat16)
            spread.append(ones * shares[n])
        combine[r] = jnp.concatenate(spread, axis=0).T.astype(jnp.bfloat16)

    loads[3].wait()
    loads[4].wait()
    base[...] = residual[...].astype(jnp.float32)
    for d in range(n_tp):
        source = lax.rem(me_tp + (0, 1, 3, 2)[d], n_tp)
        if d > 0:
            remote(
                rows_out.at[source], heads.at[source], s_o.at[source], r_o.at[source],
                {"tp": source},
            ).wait()
        for c in range(chunks // 2):
            two = pl.ds(c * 2 * wide, 2 * wide)
            base[:, two] = base[:, two] + jnp.dot(
                heads[source],
                w_proj[pl.ds(pl.multiple_of(source * lanes, lanes), lanes), two],
                preferred_element_type=jnp.float32,
            )
    squares = jnp.zeros((rows, 1), jnp.float32)
    for c in range(chunks):
        hidden = base[:, cols(c)].astype(jnp.bfloat16).astype(jnp.float32)
        base[:, cols(c)] = hidden
        squares = squares + jnp.sum(hidden * hidden, axis=1, keepdims=True)
    scale = lax.rsqrt(squares / model + EPS)

    def z_copy(n, c):
        src, dst, r = ((0, 1, 1), (0, 3, 3), (1, 2, 3), (3, 2, 1), (2, 3, 1))[n]
        return remote(
            gathered.at[src, c], gathered.at[dst, c], s_z.at[n, c], r_z.at[dst, c], at_plane(r)
        )

    def z_wait(r, c):
        remote(
            gathered.at[0, c], gathered.at[r, c], s_z.at[0, c], r_z.at[r, c], at_plane(1)
        ).wait_recv()

    def in_copy(r, c, t):
        place_there = 1 if t == 1 else 2 + k
        return remote(
            sent.at[r, c, t - 1], arrived.at[r, c, :, place_there],
            s_in.at[r, c, t], r_in.at[r, c, place_there], (None, partner, far_y, far_x)[t],
        )

    def back_copy(r, c, i):
        place_there = 1 if i == 1 else 2 + k
        return remote(
            answers.at[r, c, :, i], returned.at[r, c, place_there],
            s_back.at[r, c, i], r_back.at[r, c, place_there],
            partner if i == 1 else sources[i - 2],
        )

    def edge_sum(n, c):
        return remote(
            partial.at[n + 1, c], edge_in.at[n, c], s_sum.at[n, c], r_edge.at[n, c], at_plane(1)
        )

    def mid_sum(n, c):
        return remote(
            partial.at[3 - n, c], mid_in.at[n, c], s_sum.at[n + 1, c], r_mid.at[n, c],
            at_plane(3 - n),
        )

    for c in range(chunks):
        part = (base[:, cols(c)] * scale * ng_ref[:, cols(c)]).astype(jnp.bfloat16)
        normed[:, cols(c)] = part
        gathered[0, c] = part
        z_copy(0, c).start()

        @pl.when(middle)
        def _():
            z_copy(1, c).start()

    inner = w_gate.shape[2]

    def dispatch(r, *span):
        for c in span:
            picked = jnp.dot(
                place[r], gathered[r, c], preferred_element_type=jnp.float32
            ).astype(jnp.bfloat16)
            for t in range(4):
                for e in range(2):
                    part = picked[(2 * t + e) * cap:(2 * t + e + 1) * cap]
                    if t == 0:
                        arrived[r, c, e, 0] = part
                    else:
                        sent[r, c, t - 1, e] = part
        for c in span:
            for t in (2, 3, 1):
                in_copy(r, c, t).start()

    def open_half(r, half):
        span = range(half * chunks // 2, (half + 1) * chunks // 2)
        for c in span:
            for i in (1, 2, 3):
                remote(
                    sent.at[r, c, 0], arrived.at[r, c, :, i], s_in.at[r, c, 1],
                    r_in.at[r, c, i], partner,
                ).wait_recv()
        for e in range(2):
            gate = up = None
            for c in span:
                part = arrived[r, c, e].reshape(4 * cap, wide)
                more_gate = jnp.dot(part, w_gate[e, cols(c), :], preferred_element_type=jnp.float32)
                more_up = jnp.dot(part, w_up[e, cols(c), :], preferred_element_type=jnp.float32)
                gate = more_gate if gate is None else gate + more_gate
                up = more_up if up is None else up + more_up
            if half == 0:
                acc[r, e, :, pl.ds(0, inner)] = gate
                acc[r, e, :, pl.ds(inner, inner)] = up
            else:
                gate = gate + acc[r, e, :, pl.ds(0, inner)]
                up = up + acc[r, e, :, pl.ds(inner, inner)]
                hid[r, e] = (jax.nn.silu(gate) * up).astype(jnp.bfloat16)

    def answer(r, *span):
        for c in span:
            for e in range(2):
                answers[r, c, e] = jnp.dot(
                    hid[r, e], w_down[e, :, cols(c)], preferred_element_type=jnp.float32
                ).astype(jnp.bfloat16).reshape(4, cap, wide)
        for c in span:
            for i in (2, 3, 1):
                back_copy(r, c, i).start()
        for c in span:
            for e in range(2):
                returned[r, c, 0, e] = answers[r, c, e, 0]

    def collect(r, *span):
        for c in span:
            for t in range(1, 4):
                remote(
                    answers.at[r, c, :, 1], returned.at[r, c, t], s_back.at[r, c, 1],
                    r_back.at[r, c, t], partner,
                ).wait_recv()
        for c in span:
            back = jnp.concatenate(
                [returned[r, c, t, e] for t in range(4) for e in range(2)], axis=0
            )
            partial[r, c] = jnp.dot(
                combine[r], back, preferred_element_type=jnp.float32
            ).astype(jnp.bfloat16)
        if r == 1:
            for c in span:
                edge_sum(0, c).start()
        if r > 1:
            @pl.when(edge)
            def _():
                for c in span:
                    edge_sum(r - 1, c).start()

    def add_on(r, c, more):
        partial[r, c] = (
            partial[r, c].astype(jnp.float32) + more.astype(jnp.float32)
        ).astype(jnp.bfloat16)

    def relay(n, c):
        @pl.when(middle)
        def _():
            edge_sum(n + 1, c).wait_recv()
            add_on(3 - n, c, edge_in[n + 1, c])
            mid_sum(n, c).start()

    for i in range(5, 8):
        loads[i].wait()
    shared_gate = jnp.dot(normed[...], w_shared_gate[...], preferred_element_type=jnp.float32)
    shared_up = jnp.dot(normed[...], w_shared_up[...], preferred_element_type=jnp.float32)
    shared_hid = (jax.nn.silu(shared_gate) * shared_up).astype(jnp.bfloat16)
    for c in range(chunks):
        base[:, cols(c)] = base[:, cols(c)] + jnp.dot(
            shared_hid, w_shared_down[:, cols(c)], preferred_element_type=jnp.float32
        )

    for c in range(chunks):
        z_wait(1, c)

        @pl.when(middle)
        def _():
            z_copy(2, c).start()
            z_wait(3, c)
            z_copy(3, c).start()

        dispatch(1, c)
    loads[8].wait()
    loads[9].wait()
    trade(0).wait_recv()
    trade(1).wait_recv()
    open_half(1, 0)
    open_half(1, 1)
    loads[10].wait()
    trade(2).wait_recv()
    for n in range(0, chunks, 2):
        answer(1, n, n + 1)
    for c in range(0, chunks, 2):
        z_wait(2, c)
        z_wait(2, c + 1)

        @pl.when(middle)
        def _():
            z_copy(4, c).start()
            z_copy(4, c + 1).start()

        dispatch(2, c, c + 1)
    for n in range(0, chunks, 2):
        collect(1, n, n + 1)
    for c in range(0, chunks, 2):
        @pl.when(edge)
        def _():
            z_wait(3, c)
            z_wait(3, c + 1)

        dispatch(3, c, c + 1)
    open_half(2, 0)
    open_half(2, 1)
    for n in range(0, chunks, 2):
        answer(2, n, n + 1)
    open_half(3, 0)
    open_half(3, 1)
    for n in range(0, chunks, 2):
        answer(3, n, n + 1)
    for n in range(0, chunks, 2):
        collect(2, n, n + 1)
        if n == 2:
            for c in range(0, chunks, 2):
                dispatch(0, c, c + 1)
    for c in range(0, chunks, 2):
        collect(3, c, c + 1)
        relay(0, c)
        relay(0, c + 1)
    open_half(0, 0)
    open_half(0, 1)
    for n in range(0, chunks, 2):
        answer(0, n, n + 1)
    for c in range(chunks):
        relay(1, c)
    for n in range(0, chunks, 2):
        collect(0, n, n + 1)
    for c in range(chunks):
        edge_sum(0, c).wait_recv()
        base[:, cols(c)] = base[:, cols(c)] + (
            partial[0, c].astype(jnp.float32) + edge_in[0, c].astype(jnp.float32)
        )

        @pl.when(middle)
        def _():
            mid_sum(0, c).wait_recv()
            out_ref[:, cols(c)] = (
                base[:, cols(c)] + mid_in[0, c].astype(jnp.float32)
            ).astype(jnp.bfloat16)

    for c in range(chunks):
        @pl.when(edge)
        def _():
            mid_sum(1, c).wait_recv()
            out_ref[:, cols(c)] = (
                base[:, cols(c)] + mid_in[1, c].astype(jnp.float32)
            ).astype(jnp.bfloat16)

    for i in range(3):
        trade(i).wait_send()
    for r in range(1, planes):
        info_copy(r).wait_send()
        k_across(r).wait_send()
    kv_across().wait_send()
    for r in (1, 2):
        kv_plane(r).wait_send()
        v_plane(r).wait_send()

    @pl.when(middle)
    def _():
        kv_plane(3).wait_send()
        v_plane(3).wait_send()
        kv_pass().wait_send()
        v_pass().wait_send()

    for c in range(chunks):
        z_copy(0, c).wait_send()
        for n in range(3):
            edge_sum(n, c).wait_send()
        for r in range(planes):
            for n in (1, 2, 3):
                in_copy(r, c, n).wait_send()
                back_copy(r, c, n).wait_send()

        @pl.when(middle)
        def _():
            for n in range(1, 5):
                z_copy(n, c).wait_send()


def small_tables(tok, width):
    quarter = width // 4
    lane = jnp.arange(width)
    inverse = jnp.power(THETA, -4.0 * (lane % quarter).astype(jnp.float32) / width)
    sign = jnp.where(lane // quarter % 2 == 0, -1.0, 1.0)
    by_row = (lane < width // 2)[None, :]
    grid_rows = tok // GRID_W
    start = lax.axis_index("sp") * grid_rows
    row_angle = (start + jnp.arange(grid_rows)).astype(jnp.float32)[:, None] * inverse
    col_angle = jnp.arange(GRID_W).astype(jnp.float32)[:, None] * inverse
    return (
        jnp.where(by_row, jnp.cos(row_angle), 0.0),
        jnp.where(by_row, 0.0, jnp.cos(col_angle)),
        jnp.where(by_row, jnp.sin(row_angle) * sign, 0.0),
        jnp.where(by_row, 0.0, jnp.sin(col_angle) * sign),
    )


def whole_layer(
    queries, keys, values, residual, out_proj, query_gain, key_gain, norm_gain,
    routes, route_weight, gate, up, down, shared_gate, shared_up, shared_down, cap,
):
    n_sp, n_tp = lax.axis_size("sp"), lax.axis_size("tp")
    tok, width = keys.shape
    lanes = queries.shape[1]
    group = lanes // width
    rows, model = residual.shape
    planes, chunks = 4, 8
    wide = model // chunks
    inner = gate.shape[2]
    tables = small_tables(tok, width)
    vmem = pl.BlockSpec(memory_space=pltpu.VMEM)
    anywhere = pl.BlockSpec(memory_space=pl.ANY)
    dma = pltpu.SemaphoreType.DMA
    low, full = jnp.bfloat16, jnp.float32
    return pl.pallas_call(
        functools.partial(layer_kernel, n_sp, n_tp, planes, cap, chunks),
        out_shape=jax.ShapeDtypeStruct((rows, model), low),
        in_specs=[vmem] * 9 + [anywhere] * 11,
        out_specs=vmem,
        scratch_shapes=[
            pltpu.VMEM(queries.shape, low),
            pltpu.VMEM(keys.shape, low),
            pltpu.VMEM(residual.shape, low),
            pltpu.VMEM(out_proj.shape, low),
            pltpu.VMEM((2,) + gate.shape[1:], low),
            pltpu.VMEM((2,) + up.shape[1:], low),
            pltpu.VMEM((2,) + down.shape[1:], low),
            pltpu.VMEM(shared_gate.shape, low),
            pltpu.VMEM(shared_up.shape, low),
            pltpu.VMEM(shared_down.shape, low),
            pltpu.VMEM((tok, width), full),
            pltpu.VMEM((tok, width), full),
            pltpu.VMEM((planes, 2, 2, tok, width), low),
            pltpu.VMEM((n_tp, group * rows, width), low),
            pltpu.VMEM((n_tp, group * rows, width), full),
            pltpu.VMEM((n_tp, group * rows, width), full),
            pltpu.VMEM((n_tp, group * rows, width), full),
            pltpu.VMEM((n_tp, rows, lanes), low),
            pltpu.VMEM((n_tp, rows, lanes), low),
            pltpu.VMEM((rows, model), low),
            pltpu.VMEM((planes, 2 * routes.shape[1], rows), full),
            pltpu.VMEM((planes, chunks, rows, wide), low),
            pltpu.VMEM((planes, chunks, 3, 2, cap, wide), low),
            pltpu.VMEM((planes, chunks, 2, 4, cap, wide), low),
            pltpu.VMEM((planes, chunks, 4, 2, cap, wide), low),
            pltpu.VMEM((planes, chunks, rows, wide), low),
            pltpu.VMEM((3, chunks, rows, wide), low),
            pltpu.VMEM((2, chunks, rows, wide), low),
            pltpu.VMEM((planes, 8 * cap, rows), low),
            pltpu.VMEM((planes, rows, 8 * cap), low),
            pltpu.VMEM((planes, 2, 4 * cap, 2 * inner), full),
            pltpu.VMEM((planes, 2, 4 * cap, inner), low),
            pltpu.VMEM((rows, model), full),
            dma((11,)), dma((3, planes)), dma((3, planes)),
            dma((n_tp,)), dma((n_tp,)), dma((3,)), dma((3,)),
            dma((planes,)), dma((planes,)),
            dma((5, chunks)), dma((planes, chunks)),
            dma((planes, chunks, 4)), dma((planes, chunks, 4)),
            dma((planes, chunks, 4)), dma((planes, chunks, 4)),
            dma((3, chunks)), dma((3, chunks)), dma((2, chunks)),
        ],
        compiler_params=pltpu.CompilerParams(
            collective_id=2, has_side_effects=True, vmem_limit_bytes=61 * 2**20
        ),
        name="layer",
    )(
        *tables, query_gain.reshape(1, width), key_gain.reshape(1, width),
        norm_gain.reshape(1, model), routes.T, route_weight.T,
        queries, keys, values, residual, out_proj,
        gate, up, down, shared_gate, shared_up, shared_down,
    )


def body(
    queries,
    keys,
    values,
    residual,
    out_proj,
    query_gain,
    key_gain,
    norm_gain,
    routes,
    route_weight,
    expert_gate,
    expert_up,
    expert_down,
    shared_gate,
    shared_up,
    shared_down,
):
    n_sp, n_tp = lax.axis_size("sp"), lax.axis_size("tp")
    rows_local, top_count = routes.shape
    expert_total = expert_gate.shape[0] * n_sp * n_tp
    capacity = max(2, 2 * rows_local * top_count // expert_total)
    if n_sp == 8 and n_tp == 4 and expert_gate.shape[0] == 1 and capacity % 16 == 0:
        return whole_layer(
            queries, keys, values, residual, out_proj, query_gain, key_gain, norm_gain,
            routes, route_weight, expert_gate, expert_up, expert_down,
            shared_gate, shared_up, shared_down, capacity,
        )
    all_heads = attention(n_sp, n_tp, queries, keys, values, query_gain, key_gain)
    projected = jnp.dot(all_heads, out_proj, preferred_element_type=jnp.float32)
    hidden1 = (residual.astype(jnp.float32) + projected).astype(jnp.bfloat16)
    hidden_f = hidden1.astype(jnp.float32)
    normed = (
        hidden_f
        * lax.rsqrt(jnp.mean(hidden_f * hidden_f, axis=-1, keepdims=True) + EPS)
        * norm_gain
    ).astype(jnp.bfloat16)
    pair_count = rows_local * top_count
    flat_routes = routes.reshape(pair_count)
    one_hot = (flat_routes[:, None] == jnp.arange(expert_total, dtype=jnp.int32)[None, :]).astype(
        jnp.float32
    )
    lower = (jnp.arange(pair_count)[:, None] >= jnp.arange(pair_count)[None, :]).astype(jnp.float32)
    running_count = jnp.dot(lower, one_hot, precision=lax.Precision.HIGHEST)
    slot_place = (jnp.sum(running_count * one_hot, axis=1) - 1.0).astype(jnp.int32)
    slot_index = flat_routes * capacity + slot_place
    slots = slot_index.reshape(rows_local, top_count).astype(jnp.float32)
    info = jnp.concatenate([slots.T, route_weight.T], axis=0)
    layer_out = routed_experts(
        info, normed, hidden1, expert_gate, expert_up, expert_down,
        shared_gate, shared_up, shared_down, capacity,
    )
    return layer_out.astype(jnp.bfloat16)


def solution(mesh):
    placed = (
        P("sp", "tp"),
        P("sp", "tp"),
        P("sp", "tp"),
        P(("sp", "tp"), None),
        P(),
        P(),
        P(),
        P(),
        P(("sp", "tp"), None),
        P(("sp", "tp"), None),
        P(("sp", "tp"), None, None),
        P(("sp", "tp"), None, None),
        P(("sp", "tp"), None, None),
        P(),
        P(),
        P(),
    )
    return jax.shard_map(
        body, mesh=mesh, in_specs=placed, out_specs=P(("sp", "tp"), None), check_vma=False
    )
```

```python
import functools
import math

import jax
import jax.numpy as jnp
from jax import lax
from jax.experimental import pallas as pl
from jax.experimental.pallas import tpu as pltpu
from jax.sharding import PartitionSpec as P

GRID_W = 64
MESH = pl.DeviceIdType.MESH


EPS = 1e-06
THETA = 10000.0


def norm_rotate(block, gain, cosine, sine):
    mean = jnp.mean(block * block, axis=-1, keepdims=True)
    block = block * lax.rsqrt(mean + EPS) * gain
    quarter = block.shape[-1] // 4
    lane = lax.broadcasted_iota(jnp.int32, block.shape, 1)
    after = pltpu.roll(block, 3 * quarter, 1)
    before = pltpu.roll(block, quarter, 1)
    partner = jnp.where((lane // quarter) % 2 == 0, after, before)
    return (block * cosine + partner * sine).astype(jnp.bfloat16)


def plane_peer(z, d, planes):
    if planes == 4:
        return (z + 1 - 2 * (z % 2), z + 2 - 4 * (z // 2), 3 - z)[d - 1]
    return planes - 1 - z


def attention_kernel(
    n_sp, n_tp, planes, group,
    q_ref, k_ref, v_ref, cos_ref, sin_ref, qg_ref, kg_ref, out_ref,
    held, q_rot, top, total, accum, rows_out,
    send_z, send_y, recv_kv, send_o, recv_o,
):
    per = n_sp // planes
    me_sp = lax.axis_index("sp")
    me_tp = lax.axis_index("tp")
    z, y = me_sp // per, me_sp % per
    tok, width = k_ref.shape
    piece = tok // n_tp
    lanes = group * width
    held[me_sp, 0] = norm_rotate(
        k_ref[...].astype(jnp.float32), kg_ref[...], cos_ref[...], sin_ref[...]
    )
    held[me_sp, 1] = v_ref[...]
    barrier = pltpu.get_barrier_semaphore()
    for d in range(1, n_sp):
        pl.semaphore_signal(
            barrier, inc=1, device_id={"sp": lax.rem(me_sp + d, n_sp)}, device_id_type=MESH
        )
    for d in range(1, n_tp):
        pl.semaphore_signal(
            barrier, inc=1, device_id={"tp": lax.rem(me_tp + d, n_tp)}, device_id_type=MESH
        )
    pl.semaphore_wait(barrier, n_sp + n_tp - 2)

    def block_copy(block, target, sem):
        return pltpu.make_async_remote_copy(
            src_ref=held.at[block], dst_ref=held.at[block],
            send_sem=sem, recv_sem=recv_kv.at[block],
            device_id={"sp": target}, device_id_type=MESH,
        )

    def to_plane(slot, block):
        for d in range(1, per):
            block_copy(block, z * per + lax.rem(y + d, per), send_y.at[slot, d - 1]).start()

    for d in range(1, planes):
        if d == 1:
            block_copy(me_sp, plane_peer(z, d, planes) * per + y, send_z.at[d - 1]).start()
            to_plane(0, me_sp)
        else:
            block_copy(me_sp, plane_peer(z, d, planes) * per + y, send_z.at[d - 1]).start()
    for j in range(n_tp):
        rows = pl.ds(j * piece, piece)
        for h in range(group):
            q_rot[j, pl.ds(h * piece, piece), :] = norm_rotate(
                q_ref[rows, pl.ds(h * width, width)].astype(jnp.float32),
                qg_ref[...], cos_ref[rows, :], sin_ref[rows, :],
            )
    top[...] = jnp.full(top.shape, -1e30, jnp.float32)
    total[...] = jnp.zeros(total.shape, jnp.float32)
    accum[...] = jnp.zeros(accum.shape, jnp.float32)
    factor = math.log2(math.e) / math.sqrt(width)
    repeat = tok // width

    def attend(block, j):
        scores = lax.dot_general(
            q_rot[j], held[block, 0], (((1,), (1,)), ((), ())),
            preferred_element_type=jnp.float32,
        )
        old = top[j]
        new = jnp.maximum(old, jnp.max(scores, axis=1, keepdims=True))
        weights = jnp.exp2((scores - jnp.concatenate([new] * repeat, axis=1)) * factor)
        alpha = jnp.exp2((old - new) * factor)
        part = weights[:, :width]
        for r in range(1, repeat):
            part = part + weights[:, r * width:(r + 1) * width]
        summed = total[j] * alpha + part
        added = jnp.dot(
            weights.astype(jnp.bfloat16), held[block, 1], preferred_element_type=jnp.float32
        )
        return new, summed, accum[j] * alpha + added

    def out_copy(j):
        return pltpu.make_async_remote_copy(
            src_ref=rows_out.at[j],
            dst_ref=out_ref.at[:, pl.ds(pl.multiple_of(me_tp * lanes, 128), lanes)],
            send_sem=send_o.at[j], recv_sem=recv_o.at[me_tp],
            device_id={"tp": j}, device_id_type=MESH,
        )

    def step(block):
        @pl.loop(0, n_tp)
        def _(j):
            new, summed, acc = attend(block, j)
            top[j] = new
            total[j] = summed
            accum[j] = acc

    def arrive(block):
        block_copy(block, me_sp, send_z.at[0]).wait_recv()

    def others(plane, finish=False):
        for d in range(1, per):
            block = plane * per + lax.rem(y + d, per)
            arrive(block)
            step(block)

    step(me_sp)
    previous = z
    for d in range(1, planes):
        plane = plane_peer(z, d, planes)
        block = plane * per + y
        arrive(block)
        to_plane(d, block)
        others(previous)
        step(block)
        previous = plane
    others(previous)

    for d in range(n_tp):
        j = lax.rem(me_tp + 1 + d, n_tp)
        result = accum[j] / jnp.sum(total[j], axis=1, keepdims=True)
        result = result.astype(jnp.bfloat16)
        for h in range(group):
            rows_out[j, :, pl.ds(h * width, width)] = result[h * piece:(h + 1) * piece]
        if d < n_tp - 1:
            out_copy(j).start()
        else:
            for h in range(group):
                out_ref[:, pl.ds(pl.multiple_of(me_tp * lanes + h * width, 128), width)] = result[
                    h * piece:(h + 1) * piece
                ]
    for d in range(1, n_tp):
        source = lax.rem(me_tp + d, n_tp)
        pltpu.make_async_remote_copy(
            src_ref=rows_out.at[source],
            dst_ref=out_ref.at[:, pl.ds(pl.multiple_of(source * lanes, 128), lanes)],
            send_sem=send_o.at[source], recv_sem=recv_o.at[source],
            device_id={"tp": source}, device_id_type=MESH,
        ).wait()
    for d in range(1, planes):
        block_copy(me_sp, me_sp, send_z.at[d - 1]).wait_send()
    for slot in range(planes):
        for d in range(1, per):
            block_copy(me_sp, me_sp, send_y.at[slot, d - 1]).wait_send()


def angle_tables(tok, width):
    quarter = width // 4
    inverse = jnp.power(THETA, -4.0 * jnp.arange(quarter, dtype=jnp.float32) / width)
    start = lax.axis_index("sp") * tok
    grid_rows = tok // GRID_W
    row_angle = (start // GRID_W + jnp.arange(grid_rows)).astype(jnp.float32)[:, None] * inverse
    col_angle = jnp.arange(GRID_W).astype(jnp.float32)[:, None] * inverse

    def spread(row_part, col_part, sign):
        row_part = jnp.broadcast_to(row_part[:, None, :], (grid_rows, GRID_W, quarter))
        col_part = jnp.broadcast_to(col_part[None, :, :], (grid_rows, GRID_W, quarter))
        return jnp.concatenate(
            [sign * row_part, row_part, sign * col_part, col_part], axis=-1
        ).reshape(tok, width)

    tables = lax.optimization_barrier(
        (jnp.cos(row_angle), jnp.cos(col_angle), jnp.sin(row_angle), jnp.sin(col_angle))
    )
    return spread(tables[0], tables[1], 1.0), spread(tables[2], tables[3], -1.0)


def attention(mesh_sp, mesh_tp, queries, keys, values, query_gain, key_gain):
    tok, width = keys.shape
    group = queries.shape[1] // width
    planes = 4 if mesh_sp % 4 == 0 else 2
    per = mesh_sp // planes
    piece = tok // mesh_tp
    cosine, sine = angle_tables(tok, width)
    vmem = pl.BlockSpec(memory_space=pltpu.VMEM)
    return pl.pallas_call(
        functools.partial(attention_kernel, mesh_sp, mesh_tp, planes, group),
        out_shape=jax.ShapeDtypeStruct((piece, mesh_tp * group * width), jnp.bfloat16),
        in_specs=[vmem] * 7,
        out_specs=vmem,
        scratch_shapes=[
            pltpu.VMEM((mesh_sp, 2, tok, width), jnp.bfloat16),
            pltpu.VMEM((mesh_tp, group * piece, width), jnp.bfloat16),
            pltpu.VMEM((mesh_tp, group * piece, width), jnp.float32),
            pltpu.VMEM((mesh_tp, group * piece, width), jnp.float32),
            pltpu.VMEM((mesh_tp, group * piece, width), jnp.float32),
            pltpu.VMEM((mesh_tp, piece, group * width), jnp.bfloat16),
            pltpu.SemaphoreType.DMA((planes - 1,)),
            pltpu.SemaphoreType.DMA((planes, max(per - 1, 1))),
            pltpu.SemaphoreType.DMA((mesh_sp,)),
            pltpu.SemaphoreType.DMA((mesh_tp,)),
            pltpu.SemaphoreType.DMA((mesh_tp,)),
        ],
        compiler_params=pltpu.CompilerParams(
            collective_id=0, has_side_effects=True, vmem_limit_bytes=40 * 2**20
        ),
        name="attention",
    )(queries, keys, values, cosine, sine, query_gain.reshape(1, width), key_gain.reshape(1, width))


def expert_kernel(
    n_sp, n_tp, planes, cap, top_count, chunks,
    info_ref, normed_ref, hidden_ref, gate_ref, up_ref, down_ref,
    sgate_ref, sup_ref, sdown_ref, out_ref,
    info, gathered, sent, arrived, answers, returned, partial, sums,
    place, combine, acc, hid,
    s_info, r_info, s_z, r_z, s_in, r_in, s_back, r_back, s_sum, r_sum,
):
    per = n_sp // planes
    team = per * n_tp
    me_sp = lax.axis_index("sp")
    me_tp = lax.axis_index("tp")
    z, y = me_sp // per, me_sp % per
    me = y * n_tp + me_tp
    rows = normed_ref.shape[0]
    wide = normed_ref.shape[1] // chunks
    share = planes * cap
    slots = team * share
    tile = math.gcd(slots, 256)

    def in_plane(p):
        return {"sp": z * per + p // n_tp, "tp": p % n_tp}

    def at_plane(d):
        return {"sp": plane_peer(z, d, planes) * per + y}

    def block(p, size):
        return pl.ds(pl.multiple_of(p * size, size), size)

    def remote(src, dst, send, recv, target):
        return pltpu.make_async_remote_copy(
            src_ref=src, dst_ref=dst, send_sem=send, recv_sem=recv,
            device_id=target, device_id_type=MESH,
        )

    def cols(c):
        return pl.ds(c * wide, wide)

    barrier = pltpu.get_barrier_semaphore()

    @pl.loop(1, team)
    def _(d):
        pl.semaphore_signal(
            barrier, inc=1, device_id=in_plane(lax.rem(me + d, team)), device_id_type=MESH
        )

    for d in range(1, planes):
        pl.semaphore_signal(barrier, inc=1, device_id=at_plane(d), device_id_type=MESH)
    pl.semaphore_wait(barrier, team + planes - 2)

    def info_copy(d, source):
        return remote(info_ref, info.at[source], s_info.at[d], r_info.at[source], at_plane(d))

    def z_copy(c, d, source):
        return remote(
            normed_ref.at[:, cols(c)], gathered.at[c, block(source, rows)],
            s_z.at[c, d], r_z.at[c, source], at_plane(d),
        )

    def in_copy(c, p, source):
        return remote(
            sent.at[c, block(p, share)], arrived.at[c, block(source, share)],
            s_in.at[c, p], r_in.at[c, source], in_plane(p),
        )

    def back_copy(c, p, source):
        return remote(
            answers.at[c, block(p, share)], returned.at[c, block(source, share)],
            s_back.at[c, p], r_back.at[c, source], in_plane(p),
        )

    def sum_copy(c, d, source):
        return remote(
            partial.at[c, block(plane_peer(z, d, planes), rows)], sums.at[c, source],
            s_sum.at[c, d], r_sum.at[c, source], at_plane(d),
        )

    for d in range(1, planes):
        info_copy(d, z).start()
    for c in range(chunks):
        for d in range(1, planes):
            z_copy(c, d, z).start()
        gathered[c, block(z, rows)] = normed_ref[:, cols(c)]
    info[z] = info_ref[...]

    shared_gate = jnp.dot(normed_ref[...], sgate_ref[...], preferred_element_type=jnp.float32)
    shared_up = jnp.dot(normed_ref[...], sup_ref[...], preferred_element_type=jnp.float32)
    shared_hid = (jax.nn.silu(shared_gate) * shared_up).astype(jnp.bfloat16)
    for c in range(chunks):
        out_ref[:, cols(c)] = jnp.dot(
            shared_hid, sdown_ref[:, cols(c)], preferred_element_type=jnp.float32
        ) + hidden_ref[:, cols(c)].astype(jnp.float32)

    number = lax.broadcasted_iota(jnp.int32, (slots, rows), 0)
    owner = (number // cap) % planes
    slot = ((z * team + number // share) * cap + number % cap).astype(jnp.float32)
    for d in range(1, planes):
        info_copy(d, plane_peer(z, d, planes)).wait_recv()
    for plane in range(planes):
        wanted = jnp.where(owner == plane, slot, -1.0)
        ones = jnp.zeros((slots, rows), jnp.float32)
        shares = jnp.zeros((slots, rows), jnp.float32)
        for k in range(top_count):
            match = wanted == info[plane, k:k + 1, :]
            ones = jnp.where(match, 1.0, ones)
            shares = jnp.where(match, info[plane, top_count + k:top_count + k + 1, :], shares)
        place[:, pl.ds(plane * rows, rows)] = ones.astype(jnp.bfloat16)
        combine[pl.ds(plane * rows, rows), :] = shares.T.astype(jnp.bfloat16)

    for c in range(chunks):
        for d in range(1, planes):
            z_copy(c, d, plane_peer(z, d, planes)).wait_recv()

        @pl.loop(0, slots // tile)
        def _(i):
            sent[c, block(i, tile)] = jnp.dot(
                place[block(i, tile), :], gathered[c], preferred_element_type=jnp.float32
            ).astype(jnp.bfloat16)

        @pl.loop(1, team)
        def _(d):
            in_copy(c, lax.rem(me + d, team), me).start()

        arrived[c, block(me, share)] = sent[c, block(me, share)]

    inner = gate_ref.shape[2]
    for c in range(chunks):
        @pl.loop(1, team)
        def _(d):
            source = lax.rem(me + d, team)
            in_copy(c, source, source).wait_recv()

        @pl.loop(0, slots // tile)
        def _(i):
            part = arrived[c, block(i, tile)]
            gate = jnp.dot(part, gate_ref[0, cols(c), :], preferred_element_type=jnp.float32)
            up = jnp.dot(part, up_ref[0, cols(c), :], preferred_element_type=jnp.float32)
            if c > 0:
                gate = gate + acc[block(i, tile), pl.ds(0, inner)]
                up = up + acc[block(i, tile), pl.ds(inner, inner)]
            if c < chunks - 1:
                acc[block(i, tile), pl.ds(0, inner)] = gate
                acc[block(i, tile), pl.ds(inner, inner)] = up
            else:
                hid[block(i, tile), :] = (jax.nn.silu(gate) * up).astype(jnp.bfloat16)

    for c in range(chunks):
        @pl.loop(0, slots // tile)
        def _(i):
            answers[c, block(i, tile)] = jnp.dot(
                hid[block(i, tile), :], down_ref[0, :, cols(c)],
                preferred_element_type=jnp.float32,
            ).astype(jnp.bfloat16)

        @pl.loop(1, team)
        def _(d):
            back_copy(c, lax.rem(me + d, team), me).start()

        returned[c, block(me, share)] = answers[c, block(me, share)]

    for c in range(chunks):
        @pl.loop(1, team)
        def _(d):
            source = lax.rem(me + d, team)
            back_copy(c, source, source).wait_recv()

        @pl.loop(0, planes)
        def _(i):
            partial[c, block(i, rows)] = jnp.dot(
                combine[block(i, rows), :], returned[c], preferred_element_type=jnp.float32
            ).astype(jnp.bfloat16)

        for d in range(1, planes):
            sum_copy(c, d, z).start()
        sums[c, z] = partial[c, block(z, rows)]

    for c in range(chunks):
        for d in range(1, planes):
            sum_copy(c, d, plane_peer(z, d, planes)).wait_recv()
        result = out_ref[:, cols(c)]
        for plane in range(planes):
            result = result + sums[c, plane].astype(jnp.float32)
        out_ref[:, cols(c)] = result

    for d in range(1, planes):
        info_copy(d, z).wait_send()
    for c in range(chunks):
        for d in range(1, planes):
            z_copy(c, d, z).wait_send()
            sum_copy(c, d, z).wait_send()

        @pl.loop(1, team)
        def _(d):
            p = lax.rem(me + d, team)
            in_copy(c, p, me).wait_send()
            back_copy(c, p, me).wait_send()


def routed_experts(
    info, normed, hidden1, gate, up, down, shared_gate, shared_up, shared_down, cap
):
    n_sp, n_tp = lax.axis_size("sp"), lax.axis_size("tp")
    rows, model = normed.shape
    planes = 4 if n_sp % 4 == 0 else 2
    team = n_sp // planes * n_tp
    chunks = 8
    wide = model // chunks
    slots = team * planes * cap
    inner = gate.shape[2]
    top_count = info.shape[0] // 2
    vmem = pl.BlockSpec(memory_space=pltpu.VMEM)
    dma = pltpu.SemaphoreType.DMA
    return pl.pallas_call(
        functools.partial(expert_kernel, n_sp, n_tp, planes, cap, top_count, chunks),
        out_shape=jax.ShapeDtypeStruct((rows, model), jnp.float32),
        in_specs=[vmem] * 9,
        out_specs=vmem,
        scratch_shapes=[
            pltpu.VMEM((planes,) + info.shape, jnp.float32),
            pltpu.VMEM((chunks, planes * rows, wide), jnp.bfloat16),
            pltpu.VMEM((chunks, slots, wide), jnp.bfloat16),
            pltpu.VMEM((chunks, slots, wide), jnp.bfloat16),
            pltpu.VMEM((chunks, slots, wide), jnp.bfloat16),
            pltpu.VMEM((chunks, slots, wide), jnp.bfloat16),
            pltpu.VMEM((chunks, planes * rows, wide), jnp.bfloat16),
            pltpu.VMEM((chunks, planes, rows, wide), jnp.bfloat16),
            pltpu.VMEM((slots, planes * rows), jnp.bfloat16),
            pltpu.VMEM((planes * rows, slots), jnp.bfloat16),
            pltpu.VMEM((slots, 2 * inner), jnp.float32),
            pltpu.VMEM((slots, inner), jnp.bfloat16),
            dma((planes,)), dma((planes,)),
            dma((chunks, planes)), dma((chunks, planes)),
            dma((chunks, team)), dma((chunks, team)),
            dma((chunks, team)), dma((chunks, team)),
            dma((chunks, planes)), dma((chunks, planes)),
        ],
        compiler_params=pltpu.CompilerParams(
            collective_id=1, has_side_effects=True, vmem_limit_bytes=56 * 2**20
        ),
        name="experts",
    )(info, normed, hidden1, gate, up, down, shared_gate, shared_up, shared_down)


def layer_kernel(
    n_sp, n_tp, planes, cap, chunks,
    *rest,
):
    small_any, rest = rest[:9], rest[9:]
    q_any, k_any, v_any, residual_any, proj_any, *rest = rest
    own_any, shared_any, out_any, rest = rest[:3], rest[3:6], rest[6], rest[7:]
    small_refs, rest = rest[:9], rest[9:]
    cos_rows, cos_cols, sin_rows, sin_cols, qg_ref, kg_ref, ng_ref, routes_ref, share_ref = small_refs
    (
        q_ref, k_ref, residual, w_proj, w_gate, w_up, w_down,
        w_shared_gate, w_shared_up, w_shared_down,
        cos_ref, sin_ref, held, q_rot, top, total, accum, rows_out, heads, normed,
        info, gathered, sent, arrived, returned, partial, edge_in, mid_in,
        place, combine, acc, hid, base,
        out_ref, s_load, s_small, s_out, s_kv, r_kv, s_o, r_o, s_trade, r_trade,
        s_info, r_info, s_z, r_z, s_in, r_in, s_back, r_back, s_sum, r_edge, r_mid,
    ) = rest
    answers = arrived
    me_sp = lax.axis_index("sp")
    me_tp = lax.axis_index("tp")
    z, y = me_sp // 2, lax.rem(me_sp, 2)
    x, k = me_tp // 2, lax.rem(me_tp, 2)
    middle = jnp.logical_or(z == 1, z == 2)
    edge = jnp.logical_or(z == 0, z == 3)
    tok, width = k_ref.shape
    group = q_ref.shape[1] // width
    rows = tok // n_tp
    lanes = group * width
    model = w_proj.shape[1]
    wide = model // chunks

    def flip(bit, by):
        return bit + by * (1 - 2 * bit)

    def device(yy, xx, kk):
        return {"sp": z * 2 + yy, "tp": xx * 2 + kk}

    def plane_of(r):
        return (z, flip(lax.rem(z, 2), 1) + z // 2 * 2, lax.rem(z + 2, 4), 3 - z)[r]

    def at_plane(r):
        return {"sp": plane_of(r) * 2 + y}

    def remote(src, dst, send, recv, target):
        return pltpu.make_async_remote_copy(
            src_ref=src, dst_ref=dst, send_sem=send, recv_sem=recv,
            device_id=target, device_id_type=MESH,
        )

    def cols(c):
        return pl.ds(c * wide, wide)

    partner = device(y, x, 1 - k)
    far_y = device(1 - y, x, 0)
    far_x = device(y, 1 - x, 1)
    sources = [device(flip(y, 1 - k), flip(x, k), core) for core in range(2)]
    across = {"sp": z * 2 + 1 - y}
    traded_to = device(flip(y, k), flip(x, 1 - k), k)
    barrier = pltpu.get_barrier_semaphore()
    for d in range(1, n_sp):
        pl.semaphore_signal(
            barrier, inc=1, device_id={"sp": lax.rem(me_sp + d, n_sp)}, device_id_type=MESH
        )
    for d in range(1, n_tp):
        pl.semaphore_signal(
            barrier, inc=1, device_id={"tp": lax.rem(me_tp + d, n_tp)}, device_id_type=MESH
        )
    pl.semaphore_signal(barrier, inc=1, device_id=device(1 - y, x, 1 - k), device_id_type=MESH)

    pairs = [
        (k_any, k_ref), (v_any, held.at[0, 0, 1]), (q_any, q_ref), (residual_any, residual),
        (proj_any, w_proj),
        (shared_any[0], w_shared_gate), (shared_any[1], w_shared_up), (shared_any[2], w_shared_down),
        (own_any[0], w_gate.at[pl.ds(0, 1)]), (own_any[1], w_up.at[pl.ds(0, 1)]),
        (own_any[2], w_down.at[pl.ds(0, 1)]),
    ]
    loads = [pltpu.make_async_copy(src, dst, s_load.at[i]) for i, (src, dst) in enumerate(pairs)]
    small_loads = [
        pltpu.make_async_copy(src, dst, s_small.at[i])
        for i, (src, dst) in enumerate(zip(small_any, small_refs))
    ]
    loads[1].start()
    loads[0].start()
    for load in small_loads:
        load.start()
    loads[2].start()

    def trade(i, quarter=None):
        ref = (w_gate, w_up, w_down)[i]
        src, dst = own_any[i], ref.at[pl.ds(1, 1)]
        if quarter is not None:
            size = src.shape[1] // 4
            src = src.at[:, pl.ds(quarter * size, size)]
            dst = ref.at[pl.ds(1, 1), pl.ds(quarter * size, size)]
        return remote(src, dst, s_trade.at[i], r_trade.at[i], traded_to)

    def trade_y(*parts):
        @pl.when(k == 1)
        def _():
            for i, quarter in parts:
                trade(i, quarter).start()

    def kv_plane(n, r):
        side, kind = n // 2, (0, 1, 1)[n]
        return remote(
            held.at[0, side, kind], held.at[r, side, kind], s_kv.at[n, r], r_kv.at[n, r],
            at_plane(r),
        )

    def kv_pass(n):
        side, kind = n // 2, (0, 1, 1)[n]
        return remote(
            held.at[2, side, kind], held.at[3, side, kind], s_kv.at[n, 0], r_kv.at[n, 3],
            at_plane(1),
        )

    def planes_start(n):
        kv_plane(n, 1).start()
        kv_plane(n, 2).start()

        @pl.when(middle)
        def _():
            kv_plane(n, 3).start()

    def pass_start(*kinds):
        @pl.when(middle)
        def _():
            for n in kinds:
                kv_pass(n).start()

    def v_across():
        return remote(held.at[0, 0, 1], held.at[0, 1, 1], s_kv.at[4, 0], r_kv.at[4, 0], across)

    def k_across(r):
        return remote(
            held.at[r, 0, 0], held.at[r, 1, 0], s_kv.at[3, r], r_kv.at[3, r], across
        )

    def info_copy(r):
        return remote(info.at[0], info.at[r], s_info.at[r], r_info.at[r], at_plane(r))

    loads[1].wait()
    pl.semaphore_wait(barrier, n_sp + n_tp - 1)
    v_across().start()
    planes_start(1)

    @pl.when(k == 0)
    def _():
        trade(0).start()
        trade(1).start()

    for load in small_loads:
        load.wait()
    high = cos_cols.shape[0]
    for g in range(tok // high):
        cos_ref[pl.ds(g * high, high), :] = cos_rows[g:g + 1, :] + cos_cols[...]
        sin_ref[pl.ds(g * high, high), :] = sin_rows[g:g + 1, :] + sin_cols[...]
    loads[0].wait()
    held[0, 0, 0] = norm_rotate(
        k_ref[...].astype(jnp.float32), kg_ref[...], cos_ref[...], sin_ref[...]
    )
    k_across(0).start()
    planes_start(0)
    for load in loads[3:]:
        load.start()
    trade_y((0, 0), (0, 1))
    info[0, pl.ds(0, routes_ref.shape[0]), :] = routes_ref[...].astype(jnp.float32)
    info[0, pl.ds(routes_ref.shape[0], routes_ref.shape[0]), :] = share_ref[...]
    for r in range(1, planes):
        info_copy(r).start()

    loads[2].wait()
    for j in range(n_tp):
        part = pl.ds(j * rows, rows)
        for h in range(group):
            q_rot[j, pl.ds(h * rows, rows), :] = norm_rotate(
                q_ref[part, pl.ds(h * width, width)].astype(jnp.float32),
                qg_ref[...], cos_ref[part, :], sin_ref[part, :],
            )
    top[...] = jnp.full(top.shape, -1e30, jnp.float32)
    total[...] = jnp.zeros(total.shape, jnp.float32)
    accum[...] = jnp.zeros(accum.shape, jnp.float32)
    factor = math.log2(math.e) / math.sqrt(width)
    repeat = tok // width

    def attend(r, side, j):
        scores = lax.dot_general(
            q_rot[j], held[r, side, 0], (((1,), (1,)), ((), ())),
            preferred_element_type=jnp.float32,
        )
        old = top[j]
        new = jnp.maximum(old, jnp.max(scores, axis=1, keepdims=True))
        weights = jnp.exp2((scores - jnp.concatenate([new] * repeat, axis=1)) * factor)
        alpha = jnp.exp2((old - new) * factor)
        part = weights[:, :width]
        for i in range(1, repeat):
            part = part + weights[:, i * width:(i + 1) * width]
        summed = total[j] * alpha + part
        added = jnp.dot(
            weights.astype(jnp.bfloat16), held[r, side, 1], preferred_element_type=jnp.float32
        )
        return new, summed, accum[j] * alpha + added

    def step(r, side):
        @pl.loop(0, n_tp // 2)
        def _(half):
            pair = [(2 * half + i, attend(r, side, 2 * half + i)) for i in range(2)]
            for j, (new, summed, added) in pair:
                top[j] = new
                total[j] = summed
                accum[j] = added

    def out_copy(j):
        return remote(
            rows_out.at[j], heads.at[me_tp], s_o.at[j], r_o.at[me_tp], {"tp": j}
        )

    step(0, 0)
    v_across().wait_recv()
    planes_start(2)
    k_across(0).wait_recv()
    step(0, 1)
    kv_plane(0, 1).wait_recv()
    k_across(1).start()
    trade_y((0, 2))
    kv_plane(1, 1).wait_recv()
    step(1, 0)
    kv_plane(0, 2).wait_recv()
    kv_plane(1, 2).wait_recv()
    pass_start(0, 1)
    k_across(2).start()
    trade_y((0, 3))
    k_across(1).wait_recv()
    kv_plane(2, 1).wait_recv()
    step(1, 1)
    kv_plane(0, 3).wait_recv()
    k_across(3).start()
    trade_y((1, 0), (1, 1), (1, 2), (1, 3), (2, 0), (2, 1), (2, 2), (2, 3))
    step(2, 0)
    kv_plane(2, 2).wait_recv()
    pass_start(2)
    k_across(2).wait_recv()
    step(2, 1)
    kv_plane(1, 3).wait_recv()
    step(3, 0)
    k_across(3).wait_recv()
    kv_plane(2, 3).wait_recv()
    for d in range(n_tp):
        j = lax.rem(me_tp + (2, 3, 1, 0)[d], n_tp)
        new, summed, added = attend(3, 1, j)
        result = added / jnp.sum(summed, axis=1, keepdims=True)
        result = result.astype(jnp.bfloat16)
        for h in range(group):
            piece = result[h * rows:(h + 1) * rows]
            if d < n_tp - 1:
                rows_out[j, :, pl.ds(h * width, width)] = piece
            else:
                heads[j, :, pl.ds(h * width, width)] = piece
        if d < n_tp - 1:
            out_copy(j).start()

    @pl.when(k == 0)
    def _():
        trade(2).start()

    before = (
        lax.broadcasted_iota(jnp.int32, (rows, rows), 0)
        < lax.broadcasted_iota(jnp.int32, (rows, rows), 1)
    ).astype(jnp.float32).astype(jnp.bfloat16)
    count = lax.broadcasted_iota(jnp.int32, (cap, rows), 0).astype(jnp.float32)
    top_count = routes_ref.shape[0]
    members = []
    for t in range(4):
        core = (k, 1 - k, 0, 1)[t]
        far = t // 2
        for e in range(2):
            yy = flip(y, far * (1 - core) + e * core)
            xx = flip(x, far * core + e * (1 - core))
            members.append((z * 2 + yy) * n_tp + xx * 2 + core)
    for r in range(1, planes):
        info_copy(r).wait_recv()
    for r in range(planes):
        hits, shares = [], []
        for member in members:
            wanted = jnp.full((1, rows), member, jnp.int32).astype(jnp.float32)
            hit = jnp.zeros((1, rows), jnp.float32)
            share = jnp.zeros((1, rows), jnp.float32)
            for j in range(top_count):
                match = info[r, j:j + 1, :] == wanted
                hit = jnp.where(match, 1.0, hit)
                share = jnp.where(match, info[r, top_count + j:top_count + j + 1, :], share)
            hits.append(hit)
            shares.append(share)
        stacked = jnp.concatenate(hits, axis=0)
        earlier = jnp.dot(stacked.astype(jnp.bfloat16), before, preferred_element_type=jnp.float32)
        earlier = jnp.where(stacked > 0.5, earlier, -1.0)
        spread = []
        for n in range(len(members)):
            ones = (earlier[n:n + 1, :] == count).astype(jnp.float32)
            place[r, pl.ds(n * cap, cap), :] = ones.astype(jnp.bfloat16)
            spread.append(ones * shares[n])
        combine[r] = jnp.concatenate(spread, axis=0).T.astype(jnp.bfloat16)

    loads[3].wait()
    loads[4].wait()
    base[...] = residual[...].astype(jnp.float32)
    for d in range(n_tp):
        source = lax.rem(me_tp + (0, 1, 3, 2)[d], n_tp)
        if d > 0:
            remote(
                rows_out.at[source], heads.at[source], s_o.at[source], r_o.at[source],
                {"tp": source},
            ).wait()
        for c in range(chunks // 2):
            two = pl.ds(c * 2 * wide, 2 * wide)
            base[:, two] = base[:, two] + jnp.dot(
                heads[source],
                w_proj[pl.ds(pl.multiple_of(source * lanes, lanes), lanes), two],
                preferred_element_type=jnp.float32,
            )
    squares = jnp.zeros((rows, 1), jnp.float32)
    for c in range(chunks):
        hidden = base[:, cols(c)].astype(jnp.bfloat16).astype(jnp.float32)
        base[:, cols(c)] = hidden
        squares = squares + jnp.sum(hidden * hidden, axis=1, keepdims=True)
    scale = lax.rsqrt(squares / model + EPS)

    def z_copy(n, c):
        src, dst, r = ((0, 1, 1), (0, 3, 3), (1, 2, 3), (3, 2, 1), (2, 3, 1))[n]
        return remote(
            gathered.at[src, c], gathered.at[dst, c], s_z.at[n, c], r_z.at[dst, c], at_plane(r)
        )

    def z_wait(r, c):
        remote(
            gathered.at[0, c], gathered.at[r, c], s_z.at[0, c], r_z.at[r, c], at_plane(1)
        ).wait_recv()

    def in_copy(r, c, t):
        place_there = 1 if t == 1 else 2 + k
        return remote(
            sent.at[r, c, t - 1], arrived.at[r, c, :, place_there],
            s_in.at[r, c, t], r_in.at[r, c, place_there], (None, partner, far_y, far_x)[t],
        )

    def back_copy(r, c, i):
        place_there = 1 if i == 1 else 2 + k
        return remote(
            answers.at[r, c, :, i], returned.at[r, c, place_there],
            s_back.at[r, c, i], r_back.at[r, c, place_there],
            partner if i == 1 else sources[i - 2],
        )

    def edge_sum(n, c):
        return remote(
            partial.at[n + 1, c], edge_in.at[n, c], s_sum.at[n, c], r_edge.at[n, c], at_plane(1)
        )

    def mid_sum(n, c):
        return remote(
            partial.at[3 - n, c], mid_in.at[n, c], s_sum.at[n + 1, c], r_mid.at[n, c],
            at_plane(3 - n),
        )

    for c in range(chunks):
        part = (base[:, cols(c)] * scale * ng_ref[:, cols(c)]).astype(jnp.bfloat16)
        normed[:, cols(c)] = part
        gathered[0, c] = part
        z_copy(0, c).start()

        @pl.when(middle)
        def _():
            z_copy(1, c).start()

    inner = w_gate.shape[2]

    def dispatch(r, *span):
        for c in span:
            picked = jnp.dot(
                place[r], gathered[r, c], preferred_element_type=jnp.float32
            ).astype(jnp.bfloat16)
            for t in range(4):
                for e in range(2):
                    part = picked[(2 * t + e) * cap:(2 * t + e + 1) * cap]
                    if t == 0:
                        arrived[r, c, e, 0] = part
                    else:
                        sent[r, c, t - 1, e] = part
        for c in span:
            for t in (2, 3, 1):
                in_copy(r, c, t).start()

    def open_half(r, half):
        span = range(half * chunks // 2, (half + 1) * chunks // 2)
        for c in span:
            for i in (1, 2, 3):
                remote(
                    sent.at[r, c, 0], arrived.at[r, c, :, i], s_in.at[r, c, 1],
                    r_in.at[r, c, i], partner,
                ).wait_recv()
        for e in range(2):
            gate = up = None
            for c in span:
                part = arrived[r, c, e].reshape(4 * cap, wide)
                more_gate = jnp.dot(part, w_gate[e, cols(c), :], preferred_element_type=jnp.float32)
                more_up = jnp.dot(part, w_up[e, cols(c), :], preferred_element_type=jnp.float32)
                gate = more_gate if gate is None else gate + more_gate
                up = more_up if up is None else up + more_up
            if half == 0:
                acc[r, e, :, pl.ds(0, inner)] = gate
                acc[r, e, :, pl.ds(inner, inner)] = up
            else:
                gate = gate + acc[r, e, :, pl.ds(0, inner)]
                up = up + acc[r, e, :, pl.ds(inner, inner)]
                hid[r, e] = (jax.nn.silu(gate) * up).astype(jnp.bfloat16)

    def answer(r, *span):
        for c in span:
            for e in range(2):
                answers[r, c, e] = jnp.dot(
                    hid[r, e], w_down[e, :, cols(c)], preferred_element_type=jnp.float32
                ).astype(jnp.bfloat16).reshape(4, cap, wide)
        for c in span:
            for i in (2, 3, 1):
                back_copy(r, c, i).start()
        for c in span:
            for e in range(2):
                returned[r, c, 0, e] = answers[r, c, e, 0]

    def collect(r, *span):
        for c in span:
            for t in range(1, 4):
                remote(
                    answers.at[r, c, :, 1], returned.at[r, c, t], s_back.at[r, c, 1],
                    r_back.at[r, c, t], partner,
                ).wait_recv()
        for c in span:
            back = jnp.concatenate(
                [returned[r, c, t, e] for t in range(4) for e in range(2)], axis=0
            )
            partial[r, c] = jnp.dot(
                combine[r], back, preferred_element_type=jnp.float32
            ).astype(jnp.bfloat16)
        if r == 1:
            for c in span:
                edge_sum(0, c).start()
        if r > 1:
            @pl.when(edge)
            def _():
                for c in span:
                    edge_sum(r - 1, c).start()

    def add_on(r, c, more):
        partial[r, c] = (
            partial[r, c].astype(jnp.float32) + more.astype(jnp.float32)
        ).astype(jnp.bfloat16)

    def relay(n, c):
        @pl.when(middle)
        def _():
            edge_sum(n + 1, c).wait_recv()
            add_on(3 - n, c, edge_in[n + 1, c])
            mid_sum(n, c).start()

    for i in range(5, 8):
        loads[i].wait()
    shared_gate = jnp.dot(normed[...], w_shared_gate[...], preferred_element_type=jnp.float32)
    shared_up = jnp.dot(normed[...], w_shared_up[...], preferred_element_type=jnp.float32)
    shared_hid = (jax.nn.silu(shared_gate) * shared_up).astype(jnp.bfloat16)
    for c in range(chunks):
        base[:, cols(c)] = base[:, cols(c)] + jnp.dot(
            shared_hid, w_shared_down[:, cols(c)], preferred_element_type=jnp.float32
        )

    for c in range(chunks):
        z_wait(1, c)

        @pl.when(middle)
        def _():
            z_copy(2, c).start()
            z_wait(3, c)
            z_copy(3, c).start()

        dispatch(1, c)
    loads[8].wait()
    loads[9].wait()
    trade(0).wait_recv()
    trade(1).wait_recv()
    open_half(1, 0)
    open_half(1, 1)
    loads[10].wait()
    trade(2).wait_recv()
    for n in range(0, chunks, 2):
        answer(1, n, n + 1)
    for c in range(0, chunks, 2):
        z_wait(2, c)
        z_wait(2, c + 1)

        @pl.when(middle)
        def _():
            z_copy(4, c).start()
            z_copy(4, c + 1).start()

        dispatch(2, c, c + 1)
    for n in range(0, chunks, 2):
        collect(1, n, n + 1)
    for c in range(0, chunks, 2):
        @pl.when(edge)
        def _():
            z_wait(3, c)
            z_wait(3, c + 1)

        dispatch(3, c, c + 1)
    open_half(2, 0)
    open_half(2, 1)
    for n in range(0, chunks, 2):
        answer(2, n, n + 1)
    open_half(3, 0)
    open_half(3, 1)
    for n in range(0, chunks, 2):
        answer(3, n, n + 1)
    for n in range(0, chunks, 2):
        collect(2, n, n + 1)
        if n == 2:
            for c in range(0, chunks, 2):
                dispatch(0, c, c + 1)
    for c in range(0, chunks, 2):
        collect(3, c, c + 1)
        relay(0, c)
        relay(0, c + 1)
    open_half(0, 0)
    open_half(0, 1)
    for n in range(0, chunks, 2):
        answer(0, n, n + 1)
    for c in range(chunks):
        relay(1, c)
    for n in range(0, chunks, 2):
        collect(0, n, n + 1)
    def out_write(c):
        return pltpu.make_async_copy(out_ref.at[:, cols(c)], out_any.at[:, cols(c)], s_out.at[c])

    for c in range(chunks):
        edge_sum(0, c).wait_recv()
        base[:, cols(c)] = base[:, cols(c)] + (
            partial[0, c].astype(jnp.float32) + edge_in[0, c].astype(jnp.float32)
        )

        @pl.when(middle)
        def _():
            mid_sum(0, c).wait_recv()
            out_ref[:, cols(c)] = (
                base[:, cols(c)] + mid_in[0, c].astype(jnp.float32)
            ).astype(jnp.bfloat16)
            out_write(c).start()

    for c in range(chunks):
        @pl.when(edge)
        def _():
            mid_sum(1, c).wait_recv()
            out_ref[:, cols(c)] = (
                base[:, cols(c)] + mid_in[1, c].astype(jnp.float32)
            ).astype(jnp.bfloat16)
            out_write(c).start()

    for c in range(chunks):
        out_write(c).wait()
    for i in range(3):
        trade(i).wait_send()
    for r in range(1, planes):
        info_copy(r).wait_send()
    v_across().wait_send()
    for r in range(planes):
        k_across(r).wait_send()
    for n in range(3):
        kv_plane(n, 1).wait_send()
        kv_plane(n, 2).wait_send()

    @pl.when(middle)
    def _():
        for n in range(3):
            kv_plane(n, 3).wait_send()
            kv_pass(n).wait_send()

    for c in range(chunks):
        z_copy(0, c).wait_send()
        for n in range(3):
            edge_sum(n, c).wait_send()
        for r in range(planes):
            for n in (1, 2, 3):
                in_copy(r, c, n).wait_send()
                back_copy(r, c, n).wait_send()

        @pl.when(middle)
        def _():
            for n in range(1, 5):
                z_copy(n, c).wait_send()


def small_tables(tok, width):
    quarter = width // 4
    lane = jnp.arange(width)
    inverse = jnp.power(THETA, -4.0 * (lane % quarter).astype(jnp.float32) / width)
    sign = jnp.where(lane // quarter % 2 == 0, -1.0, 1.0)
    by_row = (lane < width // 2)[None, :]
    grid_rows = tok // GRID_W
    start = lax.axis_index("sp") * grid_rows
    row_angle = (start + jnp.arange(grid_rows)).astype(jnp.float32)[:, None] * inverse
    col_angle = jnp.arange(GRID_W).astype(jnp.float32)[:, None] * inverse
    return (
        jnp.where(by_row, jnp.cos(row_angle), 0.0),
        jnp.where(by_row, 0.0, jnp.cos(col_angle)),
        jnp.where(by_row, jnp.sin(row_angle) * sign, 0.0),
        jnp.where(by_row, 0.0, jnp.sin(col_angle) * sign),
    )


def whole_layer(
    queries, keys, values, residual, out_proj, query_gain, key_gain, norm_gain,
    routes, route_weight, gate, up, down, shared_gate, shared_up, shared_down, cap,
):
    n_sp, n_tp = lax.axis_size("sp"), lax.axis_size("tp")
    tok, width = keys.shape
    lanes = queries.shape[1]
    group = lanes // width
    rows, model = residual.shape
    planes, chunks = 4, 8
    wide = model // chunks
    inner = gate.shape[2]
    tables = small_tables(tok, width)
    anywhere = pl.BlockSpec(memory_space=pl.ANY)
    dma = pltpu.SemaphoreType.DMA
    low, full = jnp.bfloat16, jnp.float32
    small = (
        *tables, query_gain.reshape(1, width), key_gain.reshape(1, width),
        norm_gain.reshape(1, model), routes.T, route_weight.T,
    )
    return pl.pallas_call(
        functools.partial(layer_kernel, n_sp, n_tp, planes, cap, chunks),
        out_shape=jax.ShapeDtypeStruct((rows, model), low),
        in_specs=[anywhere] * 20,
        out_specs=anywhere,
        scratch_shapes=[pltpu.VMEM(a.shape, a.dtype) for a in small] + [
            pltpu.VMEM(queries.shape, low),
            pltpu.VMEM(keys.shape, low),
            pltpu.VMEM(residual.shape, low),
            pltpu.VMEM(out_proj.shape, low),
            pltpu.VMEM((2,) + gate.shape[1:], low),
            pltpu.VMEM((2,) + up.shape[1:], low),
            pltpu.VMEM((2,) + down.shape[1:], low),
            pltpu.VMEM(shared_gate.shape, low),
            pltpu.VMEM(shared_up.shape, low),
            pltpu.VMEM(shared_down.shape, low),
            pltpu.VMEM((tok, width), full),
            pltpu.VMEM((tok, width), full),
            pltpu.VMEM((planes, 2, 2, tok, width), low),
            pltpu.VMEM((n_tp, group * rows, width), low),
            pltpu.VMEM((n_tp, group * rows, width), full),
            pltpu.VMEM((n_tp, group * rows, width), full),
            pltpu.VMEM((n_tp, group * rows, width), full),
            pltpu.VMEM((n_tp, rows, lanes), low),
            pltpu.VMEM((n_tp, rows, lanes), low),
            pltpu.VMEM((rows, model), low),
            pltpu.VMEM((planes, 2 * routes.shape[1], rows), full),
            pltpu.VMEM((planes, chunks, rows, wide), low),
            pltpu.VMEM((planes, chunks, 3, 2, cap, wide), low),
            pltpu.VMEM((planes, chunks, 2, 4, cap, wide), low),
            pltpu.VMEM((planes, chunks, 4, 2, cap, wide), low),
            pltpu.VMEM((planes, chunks, rows, wide), low),
            pltpu.VMEM((3, chunks, rows, wide), low),
            pltpu.VMEM((2, chunks, rows, wide), low),
            pltpu.VMEM((planes, 8 * cap, rows), low),
            pltpu.VMEM((planes, rows, 8 * cap), low),
            pltpu.VMEM((planes, 2, 4 * cap, 2 * inner), full),
            pltpu.VMEM((planes, 2, 4 * cap, inner), low),
            pltpu.VMEM((rows, model), full),
            pltpu.VMEM((rows, model), low),
            dma((11,)), dma((9,)), dma((chunks,)), dma((5, planes)), dma((5, planes)),
            dma((n_tp,)), dma((n_tp,)), dma((3,)), dma((3,)),
            dma((planes,)), dma((planes,)),
            dma((5, chunks)), dma((planes, chunks)),
            dma((planes, chunks, 4)), dma((planes, chunks, 4)),
            dma((planes, chunks, 4)), dma((planes, chunks, 4)),
            dma((3, chunks)), dma((3, chunks)), dma((2, chunks)),
        ],
        compiler_params=pltpu.CompilerParams(
            collective_id=2, has_side_effects=True, vmem_limit_bytes=61 * 2**20
        ),
        name="layer",
    )(
        *small,
        queries, keys, values, residual, out_proj,
        gate, up, down, shared_gate, shared_up, shared_down,
    )


def body(
    queries,
    keys,
    values,
    residual,
    out_proj,
    query_gain,
    key_gain,
    norm_gain,
    routes,
    route_weight,
    expert_gate,
    expert_up,
    expert_down,
    shared_gate,
    shared_up,
    shared_down,
):
    n_sp, n_tp = lax.axis_size("sp"), lax.axis_size("tp")
    rows_local, top_count = routes.shape
    expert_total = expert_gate.shape[0] * n_sp * n_tp
    capacity = max(2, 2 * rows_local * top_count // expert_total)
    if n_sp == 8 and n_tp == 4 and expert_gate.shape[0] == 1 and capacity % 16 == 0:
        return whole_layer(
            queries, keys, values, residual, out_proj, query_gain, key_gain, norm_gain,
            routes, route_weight, expert_gate, expert_up, expert_down,
            shared_gate, shared_up, shared_down, capacity,
        )
    all_heads = attention(n_sp, n_tp, queries, keys, values, query_gain, key_gain)
    projected = jnp.dot(all_heads, out_proj, preferred_element_type=jnp.float32)
    hidden1 = (residual.astype(jnp.float32) + projected).astype(jnp.bfloat16)
    hidden_f = hidden1.astype(jnp.float32)
    normed = (
        hidden_f
        * lax.rsqrt(jnp.mean(hidden_f * hidden_f, axis=-1, keepdims=True) + EPS)
        * norm_gain
    ).astype(jnp.bfloat16)
    pair_count = rows_local * top_count
    flat_routes = routes.reshape(pair_count)
    one_hot = (flat_routes[:, None] == jnp.arange(expert_total, dtype=jnp.int32)[None, :]).astype(
        jnp.float32
    )
    lower = (jnp.arange(pair_count)[:, None] >= jnp.arange(pair_count)[None, :]).astype(jnp.float32)
    running_count = jnp.dot(lower, one_hot, precision=lax.Precision.HIGHEST)
    slot_place = (jnp.sum(running_count * one_hot, axis=1) - 1.0).astype(jnp.int32)
    slot_index = flat_routes * capacity + slot_place
    slots = slot_index.reshape(rows_local, top_count).astype(jnp.float32)
    info = jnp.concatenate([slots.T, route_weight.T], axis=0)
    layer_out = routed_experts(
        info, normed, hidden1, expert_gate, expert_up, expert_down,
        shared_gate, shared_up, shared_down, capacity,
    )
    return layer_out.astype(jnp.bfloat16)


def solution(mesh):
    placed = (
        P("sp", "tp"),
        P("sp", "tp"),
        P("sp", "tp"),
        P(("sp", "tp"), None),
        P(),
        P(),
        P(),
        P(),
        P(("sp", "tp"), None),
        P(("sp", "tp"), None),
        P(("sp", "tp"), None, None),
        P(("sp", "tp"), None, None),
        P(("sp", "tp"), None, None),
        P(),
        P(),
        P(),
    )
    return jax.shard_map(
        body, mesh=mesh, in_specs=placed, out_specs=P(("sp", "tp"), None), check_vma=False
    )
```

```python
import functools
import math

import jax
import jax.numpy as jnp
from jax import lax
from jax.experimental import pallas as pl
from jax.experimental.pallas import tpu as pltpu
from jax.sharding import PartitionSpec as P

GRID_W = 64
MESH = pl.DeviceIdType.MESH


EPS = 1e-06
THETA = 10000.0


def norm_rotate(block, gain, cosine, sine):
    mean = jnp.mean(block * block, axis=-1, keepdims=True)
    block = block * lax.rsqrt(mean + EPS) * gain
    quarter = block.shape[-1] // 4
    lane = lax.broadcasted_iota(jnp.int32, block.shape, 1)
    after = pltpu.roll(block, 3 * quarter, 1)
    before = pltpu.roll(block, quarter, 1)
    partner = jnp.where((lane // quarter) % 2 == 0, after, before)
    return (block * cosine + partner * sine).astype(jnp.bfloat16)


def plane_peer(z, d, planes):
    if planes == 4:
        return (z + 1 - 2 * (z % 2), z + 2 - 4 * (z // 2), 3 - z)[d - 1]
    return planes - 1 - z


def attention_kernel(
    n_sp, n_tp, planes, group,
    q_ref, k_ref, v_ref, cos_ref, sin_ref, qg_ref, kg_ref, out_ref,
    held, q_rot, top, total, accum, rows_out,
    send_z, send_y, recv_kv, send_o, recv_o,
):
    per = n_sp // planes
    me_sp = lax.axis_index("sp")
    me_tp = lax.axis_index("tp")
    z, y = me_sp // per, me_sp % per
    tok, width = k_ref.shape
    piece = tok // n_tp
    lanes = group * width
    held[me_sp, 0] = norm_rotate(
        k_ref[...].astype(jnp.float32), kg_ref[...], cos_ref[...], sin_ref[...]
    )
    held[me_sp, 1] = v_ref[...]
    barrier = pltpu.get_barrier_semaphore()
    for d in range(1, n_sp):
        pl.semaphore_signal(
            barrier, inc=1, device_id={"sp": lax.rem(me_sp + d, n_sp)}, device_id_type=MESH
        )
    for d in range(1, n_tp):
        pl.semaphore_signal(
            barrier, inc=1, device_id={"tp": lax.rem(me_tp + d, n_tp)}, device_id_type=MESH
        )
    pl.semaphore_wait(barrier, n_sp + n_tp - 2)

    def block_copy(block, target, sem):
        return pltpu.make_async_remote_copy(
            src_ref=held.at[block], dst_ref=held.at[block],
            send_sem=sem, recv_sem=recv_kv.at[block],
            device_id={"sp": target}, device_id_type=MESH,
        )

    def to_plane(slot, block):
        for d in range(1, per):
            block_copy(block, z * per + lax.rem(y + d, per), send_y.at[slot, d - 1]).start()

    for d in range(1, planes):
        if d == 1:
            block_copy(me_sp, plane_peer(z, d, planes) * per + y, send_z.at[d - 1]).start()
            to_plane(0, me_sp)
        else:
            block_copy(me_sp, plane_peer(z, d, planes) * per + y, send_z.at[d - 1]).start()
    for j in range(n_tp):
        rows = pl.ds(j * piece, piece)
        for h in range(group):
            q_rot[j, pl.ds(h * piece, piece), :] = norm_rotate(
                q_ref[rows, pl.ds(h * width, width)].astype(jnp.float32),
                qg_ref[...], cos_ref[rows, :], sin_ref[rows, :],
            )
    top[...] = jnp.full(top.shape, -1e30, jnp.float32)
    total[...] = jnp.zeros(total.shape, jnp.float32)
    accum[...] = jnp.zeros(accum.shape, jnp.float32)
    factor = math.log2(math.e) / math.sqrt(width)
    repeat = tok // width

    def attend(block, j):
        scores = lax.dot_general(
            q_rot[j], held[block, 0], (((1,), (1,)), ((), ())),
            preferred_element_type=jnp.float32,
        )
        old = top[j]
        new = jnp.maximum(old, jnp.max(scores, axis=1, keepdims=True))
        weights = jnp.exp2((scores - jnp.concatenate([new] * repeat, axis=1)) * factor)
        alpha = jnp.exp2((old - new) * factor)
        part = weights[:, :width]
        for r in range(1, repeat):
            part = part + weights[:, r * width:(r + 1) * width]
        summed = total[j] * alpha + part
        added = jnp.dot(
            weights.astype(jnp.bfloat16), held[block, 1], preferred_element_type=jnp.float32
        )
        return new, summed, accum[j] * alpha + added

    def out_copy(j):
        return pltpu.make_async_remote_copy(
            src_ref=rows_out.at[j],
            dst_ref=out_ref.at[:, pl.ds(pl.multiple_of(me_tp * lanes, 128), lanes)],
            send_sem=send_o.at[j], recv_sem=recv_o.at[me_tp],
            device_id={"tp": j}, device_id_type=MESH,
        )

    def step(block):
        @pl.loop(0, n_tp)
        def _(j):
            new, summed, acc = attend(block, j)
            top[j] = new
            total[j] = summed
            accum[j] = acc

    def arrive(block):
        block_copy(block, me_sp, send_z.at[0]).wait_recv()

    def others(plane, finish=False):
        for d in range(1, per):
            block = plane * per + lax.rem(y + d, per)
            arrive(block)
            step(block)

    step(me_sp)
    previous = z
    for d in range(1, planes):
        plane = plane_peer(z, d, planes)
        block = plane * per + y
        arrive(block)
        to_plane(d, block)
        others(previous)
        step(block)
        previous = plane
    others(previous)

    for d in range(n_tp):
        j = lax.rem(me_tp + 1 + d, n_tp)
        result = accum[j] / jnp.sum(total[j], axis=1, keepdims=True)
        result = result.astype(jnp.bfloat16)
        for h in range(group):
            rows_out[j, :, pl.ds(h * width, width)] = result[h * piece:(h + 1) * piece]
        if d < n_tp - 1:
            out_copy(j).start()
        else:
            for h in range(group):
                out_ref[:, pl.ds(pl.multiple_of(me_tp * lanes + h * width, 128), width)] = result[
                    h * piece:(h + 1) * piece
                ]
    for d in range(1, n_tp):
        source = lax.rem(me_tp + d, n_tp)
        pltpu.make_async_remote_copy(
            src_ref=rows_out.at[source],
            dst_ref=out_ref.at[:, pl.ds(pl.multiple_of(source * lanes, 128), lanes)],
            send_sem=send_o.at[source], recv_sem=recv_o.at[source],
            device_id={"tp": source}, device_id_type=MESH,
        ).wait()
    for d in range(1, planes):
        block_copy(me_sp, me_sp, send_z.at[d - 1]).wait_send()
    for slot in range(planes):
        for d in range(1, per):
            block_copy(me_sp, me_sp, send_y.at[slot, d - 1]).wait_send()


def angle_tables(tok, width):
    quarter = width // 4
    inverse = jnp.power(THETA, -4.0 * jnp.arange(quarter, dtype=jnp.float32) / width)
    start = lax.axis_index("sp") * tok
    grid_rows = tok // GRID_W
    row_angle = (start // GRID_W + jnp.arange(grid_rows)).astype(jnp.float32)[:, None] * inverse
    col_angle = jnp.arange(GRID_W).astype(jnp.float32)[:, None] * inverse

    def spread(row_part, col_part, sign):
        row_part = jnp.broadcast_to(row_part[:, None, :], (grid_rows, GRID_W, quarter))
        col_part = jnp.broadcast_to(col_part[None, :, :], (grid_rows, GRID_W, quarter))
        return jnp.concatenate(
            [sign * row_part, row_part, sign * col_part, col_part], axis=-1
        ).reshape(tok, width)

    tables = lax.optimization_barrier(
        (jnp.cos(row_angle), jnp.cos(col_angle), jnp.sin(row_angle), jnp.sin(col_angle))
    )
    return spread(tables[0], tables[1], 1.0), spread(tables[2], tables[3], -1.0)


def attention(mesh_sp, mesh_tp, queries, keys, values, query_gain, key_gain):
    tok, width = keys.shape
    group = queries.shape[1] // width
    planes = 4 if mesh_sp % 4 == 0 else 2
    per = mesh_sp // planes
    piece = tok // mesh_tp
    cosine, sine = angle_tables(tok, width)
    vmem = pl.BlockSpec(memory_space=pltpu.VMEM)
    return pl.pallas_call(
        functools.partial(attention_kernel, mesh_sp, mesh_tp, planes, group),
        out_shape=jax.ShapeDtypeStruct((piece, mesh_tp * group * width), jnp.bfloat16),
        in_specs=[vmem] * 7,
        out_specs=vmem,
        scratch_shapes=[
            pltpu.VMEM((mesh_sp, 2, tok, width), jnp.bfloat16),
            pltpu.VMEM((mesh_tp, group * piece, width), jnp.bfloat16),
            pltpu.VMEM((mesh_tp, group * piece, width), jnp.float32),
            pltpu.VMEM((mesh_tp, group * piece, width), jnp.float32),
            pltpu.VMEM((mesh_tp, group * piece, width), jnp.float32),
            pltpu.VMEM((mesh_tp, piece, group * width), jnp.bfloat16),
            pltpu.SemaphoreType.DMA((planes - 1,)),
            pltpu.SemaphoreType.DMA((planes, max(per - 1, 1))),
            pltpu.SemaphoreType.DMA((mesh_sp,)),
            pltpu.SemaphoreType.DMA((mesh_tp,)),
            pltpu.SemaphoreType.DMA((mesh_tp,)),
        ],
        compiler_params=pltpu.CompilerParams(
            collective_id=0, has_side_effects=True, vmem_limit_bytes=40 * 2**20
        ),
        name="attention",
    )(queries, keys, values, cosine, sine, query_gain.reshape(1, width), key_gain.reshape(1, width))


def expert_kernel(
    n_sp, n_tp, planes, cap, top_count, chunks,
    info_ref, normed_ref, hidden_ref, gate_ref, up_ref, down_ref,
    sgate_ref, sup_ref, sdown_ref, out_ref,
    info, gathered, sent, arrived, answers, returned, partial, sums,
    place, combine, acc, hid,
    s_info, r_info, s_z, r_z, s_in, r_in, s_back, r_back, s_sum, r_sum,
):
    per = n_sp // planes
    team = per * n_tp
    me_sp = lax.axis_index("sp")
    me_tp = lax.axis_index("tp")
    z, y = me_sp // per, me_sp % per
    me = y * n_tp + me_tp
    rows = normed_ref.shape[0]
    wide = normed_ref.shape[1] // chunks
    share = planes * cap
    slots = team * share
    tile = math.gcd(slots, 256)

    def in_plane(p):
        return {"sp": z * per + p // n_tp, "tp": p % n_tp}

    def at_plane(d):
        return {"sp": plane_peer(z, d, planes) * per + y}

    def block(p, size):
        return pl.ds(pl.multiple_of(p * size, size), size)

    def remote(src, dst, send, recv, target):
        return pltpu.make_async_remote_copy(
            src_ref=src, dst_ref=dst, send_sem=send, recv_sem=recv,
            device_id=target, device_id_type=MESH,
        )

    def cols(c):
        return pl.ds(c * wide, wide)

    barrier = pltpu.get_barrier_semaphore()

    @pl.loop(1, team)
    def _(d):
        pl.semaphore_signal(
            barrier, inc=1, device_id=in_plane(lax.rem(me + d, team)), device_id_type=MESH
        )

    for d in range(1, planes):
        pl.semaphore_signal(barrier, inc=1, device_id=at_plane(d), device_id_type=MESH)
    pl.semaphore_wait(barrier, team + planes - 2)

    def info_copy(d, source):
        return remote(info_ref, info.at[source], s_info.at[d], r_info.at[source], at_plane(d))

    def z_copy(c, d, source):
        return remote(
            normed_ref.at[:, cols(c)], gathered.at[c, block(source, rows)],
            s_z.at[c, d], r_z.at[c, source], at_plane(d),
        )

    def in_copy(c, p, source):
        return remote(
            sent.at[c, block(p, share)], arrived.at[c, block(source, share)],
            s_in.at[c, p], r_in.at[c, source], in_plane(p),
        )

    def back_copy(c, p, source):
        return remote(
            answers.at[c, block(p, share)], returned.at[c, block(source, share)],
            s_back.at[c, p], r_back.at[c, source], in_plane(p),
        )

    def sum_copy(c, d, source):
        return remote(
            partial.at[c, block(plane_peer(z, d, planes), rows)], sums.at[c, source],
            s_sum.at[c, d], r_sum.at[c, source], at_plane(d),
        )

    for d in range(1, planes):
        info_copy(d, z).start()
    for c in range(chunks):
        for d in range(1, planes):
            z_copy(c, d, z).start()
        gathered[c, block(z, rows)] = normed_ref[:, cols(c)]
    info[z] = info_ref[...]

    shared_gate = jnp.dot(normed_ref[...], sgate_ref[...], preferred_element_type=jnp.float32)
    shared_up = jnp.dot(normed_ref[...], sup_ref[...], preferred_element_type=jnp.float32)
    shared_hid = (jax.nn.silu(shared_gate) * shared_up).astype(jnp.bfloat16)
    for c in range(chunks):
        out_ref[:, cols(c)] = jnp.dot(
            shared_hid, sdown_ref[:, cols(c)], preferred_element_type=jnp.float32
        ) + hidden_ref[:, cols(c)].astype(jnp.float32)

    number = lax.broadcasted_iota(jnp.int32, (slots, rows), 0)
    owner = (number // cap) % planes
    slot = ((z * team + number // share) * cap + number % cap).astype(jnp.float32)
    for d in range(1, planes):
        info_copy(d, plane_peer(z, d, planes)).wait_recv()
    for plane in range(planes):
        wanted = jnp.where(owner == plane, slot, -1.0)
        ones = jnp.zeros((slots, rows), jnp.float32)
        shares = jnp.zeros((slots, rows), jnp.float32)
        for k in range(top_count):
            match = wanted == info[plane, k:k + 1, :]
            ones = jnp.where(match, 1.0, ones)
            shares = jnp.where(match, info[plane, top_count + k:top_count + k + 1, :], shares)
        place[:, pl.ds(plane * rows, rows)] = ones.astype(jnp.bfloat16)
        combine[pl.ds(plane * rows, rows), :] = shares.T.astype(jnp.bfloat16)

    for c in range(chunks):
        for d in range(1, planes):
            z_copy(c, d, plane_peer(z, d, planes)).wait_recv()

        @pl.loop(0, slots // tile)
        def _(i):
            sent[c, block(i, tile)] = jnp.dot(
                place[block(i, tile), :], gathered[c], preferred_element_type=jnp.float32
            ).astype(jnp.bfloat16)

        @pl.loop(1, team)
        def _(d):
            in_copy(c, lax.rem(me + d, team), me).start()

        arrived[c, block(me, share)] = sent[c, block(me, share)]

    inner = gate_ref.shape[2]
    for c in range(chunks):
        @pl.loop(1, team)
        def _(d):
            source = lax.rem(me + d, team)
            in_copy(c, source, source).wait_recv()

        @pl.loop(0, slots // tile)
        def _(i):
            part = arrived[c, block(i, tile)]
            gate = jnp.dot(part, gate_ref[0, cols(c), :], preferred_element_type=jnp.float32)
            up = jnp.dot(part, up_ref[0, cols(c), :], preferred_element_type=jnp.float32)
            if c > 0:
                gate = gate + acc[block(i, tile), pl.ds(0, inner)]
                up = up + acc[block(i, tile), pl.ds(inner, inner)]
            if c < chunks - 1:
                acc[block(i, tile), pl.ds(0, inner)] = gate
                acc[block(i, tile), pl.ds(inner, inner)] = up
            else:
                hid[block(i, tile), :] = (jax.nn.silu(gate) * up).astype(jnp.bfloat16)

    for c in range(chunks):
        @pl.loop(0, slots // tile)
        def _(i):
            answers[c, block(i, tile)] = jnp.dot(
                hid[block(i, tile), :], down_ref[0, :, cols(c)],
                preferred_element_type=jnp.float32,
            ).astype(jnp.bfloat16)

        @pl.loop(1, team)
        def _(d):
            back_copy(c, lax.rem(me + d, team), me).start()

        returned[c, block(me, share)] = answers[c, block(me, share)]

    for c in range(chunks):
        @pl.loop(1, team)
        def _(d):
            source = lax.rem(me + d, team)
            back_copy(c, source, source).wait_recv()

        @pl.loop(0, planes)
        def _(i):
            partial[c, block(i, rows)] = jnp.dot(
                combine[block(i, rows), :], returned[c], preferred_element_type=jnp.float32
            ).astype(jnp.bfloat16)

        for d in range(1, planes):
            sum_copy(c, d, z).start()
        sums[c, z] = partial[c, block(z, rows)]

    for c in range(chunks):
        for d in range(1, planes):
            sum_copy(c, d, plane_peer(z, d, planes)).wait_recv()
        result = out_ref[:, cols(c)]
        for plane in range(planes):
            result = result + sums[c, plane].astype(jnp.float32)
        out_ref[:, cols(c)] = result

    for d in range(1, planes):
        info_copy(d, z).wait_send()
    for c in range(chunks):
        for d in range(1, planes):
            z_copy(c, d, z).wait_send()
            sum_copy(c, d, z).wait_send()

        @pl.loop(1, team)
        def _(d):
            p = lax.rem(me + d, team)
            in_copy(c, p, me).wait_send()
            back_copy(c, p, me).wait_send()


def routed_experts(
    info, normed, hidden1, gate, up, down, shared_gate, shared_up, shared_down, cap
):
    n_sp, n_tp = lax.axis_size("sp"), lax.axis_size("tp")
    rows, model = normed.shape
    planes = 4 if n_sp % 4 == 0 else 2
    team = n_sp // planes * n_tp
    chunks = 8
    wide = model // chunks
    slots = team * planes * cap
    inner = gate.shape[2]
    top_count = info.shape[0] // 2
    vmem = pl.BlockSpec(memory_space=pltpu.VMEM)
    dma = pltpu.SemaphoreType.DMA
    return pl.pallas_call(
        functools.partial(expert_kernel, n_sp, n_tp, planes, cap, top_count, chunks),
        out_shape=jax.ShapeDtypeStruct((rows, model), jnp.float32),
        in_specs=[vmem] * 9,
        out_specs=vmem,
        scratch_shapes=[
            pltpu.VMEM((planes,) + info.shape, jnp.float32),
            pltpu.VMEM((chunks, planes * rows, wide), jnp.bfloat16),
            pltpu.VMEM((chunks, slots, wide), jnp.bfloat16),
            pltpu.VMEM((chunks, slots, wide), jnp.bfloat16),
            pltpu.VMEM((chunks, slots, wide), jnp.bfloat16),
            pltpu.VMEM((chunks, slots, wide), jnp.bfloat16),
            pltpu.VMEM((chunks, planes * rows, wide), jnp.bfloat16),
            pltpu.VMEM((chunks, planes, rows, wide), jnp.bfloat16),
            pltpu.VMEM((slots, planes * rows), jnp.bfloat16),
            pltpu.VMEM((planes * rows, slots), jnp.bfloat16),
            pltpu.VMEM((slots, 2 * inner), jnp.float32),
            pltpu.VMEM((slots, inner), jnp.bfloat16),
            dma((planes,)), dma((planes,)),
            dma((chunks, planes)), dma((chunks, planes)),
            dma((chunks, team)), dma((chunks, team)),
            dma((chunks, team)), dma((chunks, team)),
            dma((chunks, planes)), dma((chunks, planes)),
        ],
        compiler_params=pltpu.CompilerParams(
            collective_id=1, has_side_effects=True, vmem_limit_bytes=56 * 2**20
        ),
        name="experts",
    )(info, normed, hidden1, gate, up, down, shared_gate, shared_up, shared_down)


def layer_kernel(
    n_sp, n_tp, planes, cap, chunks,
    *rest,
):
    small_any, rest = rest[:9], rest[9:]
    q_any, k_any, v_any, residual_any, proj_any, *rest = rest
    own_any, shared_any, out_any, rest = rest[:3], rest[3:6], rest[6], rest[7:]
    small_refs, rest = rest[:9], rest[9:]
    cos_rows, cos_cols, sin_rows, sin_cols, qg_ref, kg_ref, ng_ref, routes_ref, share_ref = small_refs
    (
        q_ref, k_ref, residual, w_proj, w_gate, w_up, w_down,
        w_shared_gate, w_shared_up, w_shared_down,
        cos_ref, sin_ref, held, q_rot, top, total, accum, rows_out, heads, normed,
        info, gathered, sent, arrived, returned, partial, edge_in, mid_in,
        place, combine, acc, hid, base,
        out_ref, s_load, s_small, s_out, s_kv, r_kv, s_o, r_o, s_trade, r_trade,
        s_info, r_info, s_z, r_z, s_in, r_in, s_back, r_back, s_sum, r_edge, r_mid,
    ) = rest
    answers = arrived
    me_sp = lax.axis_index("sp")
    me_tp = lax.axis_index("tp")
    z, y = me_sp // 2, lax.rem(me_sp, 2)
    x, k = me_tp // 2, lax.rem(me_tp, 2)
    middle = jnp.logical_or(z == 1, z == 2)
    edge = jnp.logical_or(z == 0, z == 3)
    tok, width = k_ref.shape
    group = q_ref.shape[1] // width
    rows = tok // n_tp
    lanes = group * width
    model = w_proj.shape[1]
    wide = model // chunks

    def flip(bit, by):
        return bit + by * (1 - 2 * bit)

    def device(yy, xx, kk):
        return {"sp": z * 2 + yy, "tp": xx * 2 + kk}

    def plane_of(r):
        return (z, flip(lax.rem(z, 2), 1) + z // 2 * 2, lax.rem(z + 2, 4), 3 - z)[r]

    def at_plane(r):
        return {"sp": plane_of(r) * 2 + y}

    def remote(src, dst, send, recv, target):
        return pltpu.make_async_remote_copy(
            src_ref=src, dst_ref=dst, send_sem=send, recv_sem=recv,
            device_id=target, device_id_type=MESH,
        )

    def cols(c):
        return pl.ds(c * wide, wide)

    partner = device(y, x, 1 - k)
    far_y = device(1 - y, x, 0)
    far_x = device(y, 1 - x, 1)
    sources = [device(flip(y, 1 - k), flip(x, k), core) for core in range(2)]
    across = {"sp": z * 2 + 1 - y}
    traded_to = device(flip(y, k), flip(x, 1 - k), k)
    barrier = pltpu.get_barrier_semaphore()
    for d in range(1, n_sp):
        pl.semaphore_signal(
            barrier, inc=1, device_id={"sp": lax.rem(me_sp + d, n_sp)}, device_id_type=MESH
        )
    for d in range(1, n_tp):
        pl.semaphore_signal(
            barrier, inc=1, device_id={"tp": lax.rem(me_tp + d, n_tp)}, device_id_type=MESH
        )
    pl.semaphore_signal(barrier, inc=1, device_id=device(1 - y, x, 1 - k), device_id_type=MESH)

    pairs = [
        (k_any, k_ref), (v_any, held.at[0, 0, 1]), (q_any, q_ref), (residual_any, residual),
        (proj_any, w_proj),
        (shared_any[0], w_shared_gate), (shared_any[1], w_shared_up), (shared_any[2], w_shared_down),
        (own_any[0], w_gate.at[pl.ds(0, 1)]), (own_any[1], w_up.at[pl.ds(0, 1)]),
        (own_any[2], w_down.at[pl.ds(0, 1)]),
    ]
    loads = [pltpu.make_async_copy(src, dst, s_load.at[i]) for i, (src, dst) in enumerate(pairs)]
    small_loads = [
        pltpu.make_async_copy(src, dst, s_small.at[i])
        for i, (src, dst) in enumerate(zip(small_any, small_refs))
    ]
    loads[1].start()
    loads[0].start()
    for load in small_loads:
        load.start()
    loads[2].start()

    def trade(i, quarter=None):
        ref = (w_gate, w_up, w_down)[i]
        src, dst = own_any[i], ref.at[pl.ds(1, 1)]
        if quarter is not None:
            size = src.shape[1] // 4
            src = src.at[:, pl.ds(quarter * size, size)]
            dst = ref.at[pl.ds(1, 1), pl.ds(quarter * size, size)]
        return remote(src, dst, s_trade.at[i], r_trade.at[i], traded_to)

    def trade_y(*parts):
        @pl.when(k == 1)
        def _():
            for i, quarter in parts:
                trade(i, quarter).start()

    def kv_plane(n, r):
        side, kind = n // 2, (0, 1, 1)[n]
        return remote(
            held.at[0, side, kind], held.at[r, side, kind], s_kv.at[n, r], r_kv.at[n, r],
            at_plane(r),
        )

    def kv_pass(n):
        side, kind = n // 2, (0, 1, 1)[n]
        return remote(
            held.at[2, side, kind], held.at[3, side, kind], s_kv.at[n, 0], r_kv.at[n, 3],
            at_plane(1),
        )

    def planes_start(n):
        kv_plane(n, 1).start()
        kv_plane(n, 2).start()

        @pl.when(middle)
        def _():
            kv_plane(n, 3).start()

    def pass_start(*kinds):
        @pl.when(middle)
        def _():
            for n in kinds:
                kv_pass(n).start()

    def v_across():
        return remote(held.at[0, 0, 1], held.at[0, 1, 1], s_kv.at[4, 0], r_kv.at[4, 0], across)

    def k_across(r):
        return remote(
            held.at[r, 0, 0], held.at[r, 1, 0], s_kv.at[3, r], r_kv.at[3, r], across
        )

    def info_copy(r):
        return remote(info.at[0], info.at[r], s_info.at[r], r_info.at[r], at_plane(r))

    loads[1].wait()
    pl.semaphore_wait(barrier, n_sp + n_tp - 1)
    v_across().start()
    planes_start(1)

    @pl.when(k == 0)
    def _():
        trade(0).start()
        trade(1).start()

    for load in small_loads:
        load.wait()
    high = cos_cols.shape[0]
    for g in range(tok // high):
        cos_ref[pl.ds(g * high, high), :] = cos_rows[g:g + 1, :] + cos_cols[...]
        sin_ref[pl.ds(g * high, high), :] = sin_rows[g:g + 1, :] + sin_cols[...]
    loads[0].wait()
    held[0, 0, 0] = norm_rotate(
        k_ref[...].astype(jnp.float32), kg_ref[...], cos_ref[...], sin_ref[...]
    )
    k_across(0).start()
    planes_start(0)
    for load in loads[3:]:
        load.start()
    trade_y((0, 0), (0, 1))
    info[0, pl.ds(0, routes_ref.shape[0]), :] = routes_ref[...].astype(jnp.float32)
    info[0, pl.ds(routes_ref.shape[0], routes_ref.shape[0]), :] = share_ref[...]
    for r in range(1, planes):
        info_copy(r).start()

    loads[2].wait()
    for j in range(n_tp):
        part = pl.ds(j * rows, rows)
        for h in range(group):
            q_rot[j, pl.ds(h * rows, rows), :] = norm_rotate(
                q_ref[part, pl.ds(h * width, width)].astype(jnp.float32),
                qg_ref[...], cos_ref[part, :], sin_ref[part, :],
            )
    top[...] = jnp.full(top.shape, -1e30, jnp.float32)
    total[...] = jnp.zeros(total.shape, jnp.float32)
    accum[...] = jnp.zeros(accum.shape, jnp.float32)
    factor = math.log2(math.e) / math.sqrt(width)
    repeat = tok // width

    def attend(r, side, j):
        scores = lax.dot_general(
            q_rot[j], held[r, side, 0], (((1,), (1,)), ((), ())),
            preferred_element_type=jnp.float32,
        )
        old = top[j]
        new = jnp.maximum(old, jnp.max(scores, axis=1, keepdims=True))
        weights = jnp.exp2((scores - jnp.concatenate([new] * repeat, axis=1)) * factor)
        alpha = jnp.exp2((old - new) * factor)
        part = weights[:, :width]
        for i in range(1, repeat):
            part = part + weights[:, i * width:(i + 1) * width]
        summed = total[j] * alpha + part
        added = jnp.dot(
            weights.astype(jnp.bfloat16), held[r, side, 1], preferred_element_type=jnp.float32
        )
        return new, summed, accum[j] * alpha + added

    def step(r, side):
        @pl.loop(0, n_tp // 2)
        def _(half):
            pair = [(2 * half + i, attend(r, side, 2 * half + i)) for i in range(2)]
            for j, (new, summed, added) in pair:
                top[j] = new
                total[j] = summed
                accum[j] = added

    def out_copy(j):
        return remote(
            rows_out.at[j], heads.at[me_tp], s_o.at[j], r_o.at[me_tp], {"tp": j}
        )

    step(0, 0)
    v_across().wait_recv()
    planes_start(2)
    k_across(0).wait_recv()
    step(0, 1)
    kv_plane(0, 1).wait_recv()
    k_across(1).start()
    trade_y((0, 2))
    kv_plane(1, 1).wait_recv()
    step(1, 0)
    kv_plane(0, 2).wait_recv()
    kv_plane(1, 2).wait_recv()
    pass_start(0, 1)
    k_across(2).start()
    trade_y((0, 3))
    k_across(1).wait_recv()
    kv_plane(2, 1).wait_recv()
    step(1, 1)
    kv_plane(0, 3).wait_recv()
    k_across(3).start()
    trade_y((1, 0), (1, 1), (1, 2), (1, 3), (2, 0), (2, 1), (2, 2), (2, 3))
    step(2, 0)
    kv_plane(2, 2).wait_recv()
    pass_start(2)
    k_across(2).wait_recv()
    step(2, 1)
    kv_plane(1, 3).wait_recv()
    step(3, 0)
    k_across(3).wait_recv()
    kv_plane(2, 3).wait_recv()
    for d in range(n_tp):
        j = lax.rem(me_tp + (2, 3, 1, 0)[d], n_tp)
        new, summed, added = attend(3, 1, j)
        result = added / jnp.sum(summed, axis=1, keepdims=True)
        result = result.astype(jnp.bfloat16)
        for h in range(group):
            piece = result[h * rows:(h + 1) * rows]
            if d < n_tp - 1:
                rows_out[j, :, pl.ds(h * width, width)] = piece
            else:
                heads[j, :, pl.ds(h * width, width)] = piece
        if d < n_tp - 1:
            out_copy(j).start()

    @pl.when(k == 0)
    def _():
        trade(2).start()

    before = (
        lax.broadcasted_iota(jnp.int32, (rows, rows), 0)
        < lax.broadcasted_iota(jnp.int32, (rows, rows), 1)
    ).astype(jnp.float32).astype(jnp.bfloat16)
    count = lax.broadcasted_iota(jnp.int32, (cap, rows), 0).astype(jnp.float32)
    top_count = routes_ref.shape[0]
    members = []
    for t in range(4):
        core = (k, 1 - k, 0, 1)[t]
        far = t // 2
        for e in range(2):
            yy = flip(y, far * (1 - core) + e * core)
            xx = flip(x, far * core + e * (1 - core))
            members.append((z * 2 + yy) * n_tp + xx * 2 + core)
    for r in range(1, planes):
        info_copy(r).wait_recv()
    for r in range(planes):
        hits, shares = [], []
        for member in members:
            wanted = jnp.full((1, rows), member, jnp.int32).astype(jnp.float32)
            hit = jnp.zeros((1, rows), jnp.float32)
            share = jnp.zeros((1, rows), jnp.float32)
            for j in range(top_count):
                match = info[r, j:j + 1, :] == wanted
                hit = jnp.where(match, 1.0, hit)
                share = jnp.where(match, info[r, top_count + j:top_count + j + 1, :], share)
            hits.append(hit)
            shares.append(share)
        stacked = jnp.concatenate(hits, axis=0)
        earlier = jnp.dot(stacked.astype(jnp.bfloat16), before, preferred_element_type=jnp.float32)
        earlier = jnp.where(stacked > 0.5, earlier, -1.0)
        spread = []
        for n in range(len(members)):
            ones = (earlier[n:n + 1, :] == count).astype(jnp.float32)
            place[r, pl.ds(n * cap, cap), :] = ones.astype(jnp.bfloat16)
            spread.append(ones * shares[n])
        combine[r] = jnp.concatenate(spread, axis=0).T.astype(jnp.bfloat16)

    loads[3].wait()
    loads[4].wait()
    base[...] = residual[...].astype(jnp.float32)
    for d in range(n_tp):
        source = lax.rem(me_tp + (0, 1, 3, 2)[d], n_tp)
        if d > 0:
            remote(
                rows_out.at[source], heads.at[source], s_o.at[source], r_o.at[source],
                {"tp": source},
            ).wait()
        for c in range(chunks // 2):
            two = pl.ds(c * 2 * wide, 2 * wide)
            base[:, two] = base[:, two] + jnp.dot(
                heads[source],
                w_proj[pl.ds(pl.multiple_of(source * lanes, lanes), lanes), two],
                preferred_element_type=jnp.float32,
            )
    squares = jnp.zeros((rows, 1), jnp.float32)
    for c in range(chunks):
        hidden = base[:, cols(c)].astype(jnp.bfloat16).astype(jnp.float32)
        base[:, cols(c)] = hidden
        squares = squares + jnp.sum(hidden * hidden, axis=1, keepdims=True)
    scale = lax.rsqrt(squares / model + EPS)

    def z_copy(n, c):
        src, dst, r = ((0, 1, 1), (0, 3, 3), (1, 2, 3), (3, 2, 1), (2, 3, 1))[n]
        return remote(
            gathered.at[src, c], gathered.at[dst, c], s_z.at[n, c], r_z.at[dst, c], at_plane(r)
        )

    def z_wait(r, c):
        remote(
            gathered.at[0, c], gathered.at[r, c], s_z.at[0, c], r_z.at[r, c], at_plane(1)
        ).wait_recv()

    def in_copy(r, c, t):
        place_there = 1 if t == 1 else 2 + k
        return remote(
            sent.at[r, c, t - 1], arrived.at[r, c, :, place_there],
            s_in.at[r, c, t], r_in.at[r, c, place_there], (None, partner, far_y, far_x)[t],
        )

    def back_copy(r, c, i):
        place_there = 1 if i == 1 else 2 + k
        return remote(
            answers.at[r, c, :, i], returned.at[r, c, place_there],
            s_back.at[r, c, i], r_back.at[r, c, place_there],
            partner if i == 1 else sources[i - 2],
        )

    def edge_sum(n, c):
        return remote(
            partial.at[n + 1, c], edge_in.at[n, c], s_sum.at[n, c], r_edge.at[n, c], at_plane(1)
        )

    def mid_sum(n, c):
        return remote(
            partial.at[3 - n, c], mid_in.at[n, c], s_sum.at[n + 1, c], r_mid.at[n, c],
            at_plane(3 - n),
        )

    for c in range(chunks):
        part = (base[:, cols(c)] * scale * ng_ref[:, cols(c)]).astype(jnp.bfloat16)
        normed[:, cols(c)] = part
        gathered[0, c] = part
        z_copy(0, c).start()

        @pl.when(middle)
        def _():
            z_copy(1, c).start()

    inner = w_gate.shape[2]

    def dispatch(r, *span):
        for c in span:
            picked = jnp.dot(
                place[r], gathered[r, c], preferred_element_type=jnp.float32
            ).astype(jnp.bfloat16)
            for t in range(4):
                for e in range(2):
                    part = picked[(2 * t + e) * cap:(2 * t + e + 1) * cap]
                    if t == 0:
                        arrived[r, c, e, 0] = part
                    else:
                        sent[r, c, t - 1, e] = part
        for c in span:
            for t in (2, 3, 1):
                in_copy(r, c, t).start()

    def open_half(r, half):
        span = range(half * chunks // 2, (half + 1) * chunks // 2)
        for c in span:
            for i in (1, 2, 3):
                remote(
                    sent.at[r, c, 0], arrived.at[r, c, :, i], s_in.at[r, c, 1],
                    r_in.at[r, c, i], partner,
                ).wait_recv()
        for e in range(2):
            gate = up = None
            for c in span:
                part = arrived[r, c, e].reshape(4 * cap, wide)
                more_gate = jnp.dot(part, w_gate[e, cols(c), :], preferred_element_type=jnp.float32)
                more_up = jnp.dot(part, w_up[e, cols(c), :], preferred_element_type=jnp.float32)
                gate = more_gate if gate is None else gate + more_gate
                up = more_up if up is None else up + more_up
            if half == 0:
                acc[r, e, :, pl.ds(0, inner)] = gate
                acc[r, e, :, pl.ds(inner, inner)] = up
            else:
                gate = gate + acc[r, e, :, pl.ds(0, inner)]
                up = up + acc[r, e, :, pl.ds(inner, inner)]
                hid[r, e] = (jax.nn.silu(gate) * up).astype(jnp.bfloat16)

    def answer(r, *span):
        for c in span:
            for e in range(2):
                answers[r, c, e] = jnp.dot(
                    hid[r, e], w_down[e, :, cols(c)], preferred_element_type=jnp.float32
                ).astype(jnp.bfloat16).reshape(4, cap, wide)
        for c in span:
            for i in (2, 3, 1):
                back_copy(r, c, i).start()
        for c in span:
            for e in range(2):
                returned[r, c, 0, e] = answers[r, c, e, 0]

    def collect(r, *span):
        for c in span:
            for t in range(1, 4):
                remote(
                    answers.at[r, c, :, 1], returned.at[r, c, t], s_back.at[r, c, 1],
                    r_back.at[r, c, t], partner,
                ).wait_recv()
        for c in span:
            back = jnp.concatenate(
                [returned[r, c, t, e] for t in range(4) for e in range(2)], axis=0
            )
            partial[r, c] = jnp.dot(
                combine[r], back, preferred_element_type=jnp.float32
            ).astype(jnp.bfloat16)
        if r == 1:
            for c in span:
                edge_sum(0, c).start()
        if r > 1:
            @pl.when(edge)
            def _():
                for c in span:
                    edge_sum(r - 1, c).start()

    def add_on(r, c, more):
        partial[r, c] = (
            partial[r, c].astype(jnp.float32) + more.astype(jnp.float32)
        ).astype(jnp.bfloat16)

    def relay(n, c):
        @pl.when(middle)
        def _():
            edge_sum(n + 1, c).wait_recv()
            add_on(3 - n, c, edge_in[n + 1, c])
            mid_sum(n, c).start()

    for i in range(5, 8):
        loads[i].wait()
    shared_gate = jnp.dot(normed[...], w_shared_gate[...], preferred_element_type=jnp.float32)
    shared_up = jnp.dot(normed[...], w_shared_up[...], preferred_element_type=jnp.float32)
    shared_hid = (jax.nn.silu(shared_gate) * shared_up).astype(jnp.bfloat16)
    for c in range(chunks):
        base[:, cols(c)] = base[:, cols(c)] + jnp.dot(
            shared_hid, w_shared_down[:, cols(c)], preferred_element_type=jnp.float32
        )

    for c in range(chunks):
        z_wait(1, c)

        @pl.when(middle)
        def _():
            z_copy(2, c).start()
            z_wait(3, c)
            z_copy(3, c).start()

        dispatch(1, c)
    loads[8].wait()
    loads[9].wait()
    trade(0).wait_recv()
    trade(1).wait_recv()
    open_half(1, 0)
    open_half(1, 1)
    loads[10].wait()
    trade(2).wait_recv()
    for n in range(0, chunks, 2):
        answer(1, n, n + 1)
    for c in range(0, chunks, 2):
        z_wait(2, c)
        z_wait(2, c + 1)

        @pl.when(middle)
        def _():
            z_copy(4, c).start()
            z_copy(4, c + 1).start()

        dispatch(2, c, c + 1)
    for n in range(0, chunks, 2):
        collect(1, n, n + 1)
    for c in range(0, chunks, 2):
        @pl.when(edge)
        def _():
            z_wait(3, c)
            z_wait(3, c + 1)

        dispatch(3, c, c + 1)
    open_half(2, 0)
    open_half(2, 1)
    for n in range(0, chunks, 2):
        answer(2, n, n + 1)
    open_half(3, 0)
    open_half(3, 1)
    for n in range(0, chunks, 2):
        answer(3, n, n + 1)
    for n in range(0, chunks, 2):
        collect(2, n, n + 1)
        if n == 2:
            for c in range(0, chunks, 2):
                dispatch(0, c, c + 1)
    for c in range(0, chunks, 2):
        collect(3, c, c + 1)
        relay(0, c)
        relay(0, c + 1)
    open_half(0, 0)
    open_half(0, 1)
    for n in range(0, chunks, 2):
        answer(0, n, n + 1)
    for c in range(chunks):
        relay(1, c)
    for n in range(0, chunks, 2):
        collect(0, n, n + 1)
    def out_write(c):
        return pltpu.make_async_copy(out_ref.at[:, cols(c)], out_any.at[:, cols(c)], s_out.at[c])

    for c in range(chunks):
        edge_sum(0, c).wait_recv()
        base[:, cols(c)] = base[:, cols(c)] + (
            partial[0, c].astype(jnp.float32) + edge_in[0, c].astype(jnp.float32)
        )

        @pl.when(middle)
        def _():
            mid_sum(0, c).wait_recv()
            out_ref[:, cols(c)] = (
                base[:, cols(c)] + mid_in[0, c].astype(jnp.float32)
            ).astype(jnp.bfloat16)
            out_write(c).start()

    for c in range(chunks):
        @pl.when(edge)
        def _():
            mid_sum(1, c).wait_recv()
            out_ref[:, cols(c)] = (
                base[:, cols(c)] + mid_in[1, c].astype(jnp.float32)
            ).astype(jnp.bfloat16)
            out_write(c).start()

    for c in range(chunks):
        out_write(c).wait()
    for i in range(3):
        trade(i).wait_send()
    for r in range(1, planes):
        info_copy(r).wait_send()
    v_across().wait_send()
    for r in range(planes):
        k_across(r).wait_send()
    for n in range(3):
        kv_plane(n, 1).wait_send()
        kv_plane(n, 2).wait_send()

    @pl.when(middle)
    def _():
        for n in range(3):
            kv_plane(n, 3).wait_send()
            kv_pass(n).wait_send()

    for c in range(chunks):
        z_copy(0, c).wait_send()
        for n in range(3):
            edge_sum(n, c).wait_send()
        for r in range(planes):
            for n in (1, 2, 3):
                in_copy(r, c, n).wait_send()
                back_copy(r, c, n).wait_send()

        @pl.when(middle)
        def _():
            for n in range(1, 5):
                z_copy(n, c).wait_send()


def small_tables(tok, width):
    quarter = width // 4
    lane = jnp.arange(width)
    inverse = jnp.power(THETA, -4.0 * (lane % quarter).astype(jnp.float32) / width)
    sign = jnp.where(lane // quarter % 2 == 0, -1.0, 1.0)
    by_row = (lane < width // 2)[None, :]
    grid_rows = tok // GRID_W
    start = lax.axis_index("sp") * grid_rows
    row_angle = (start + jnp.arange(grid_rows)).astype(jnp.float32)[:, None] * inverse
    col_angle = jnp.arange(GRID_W).astype(jnp.float32)[:, None] * inverse
    return (
        jnp.where(by_row, jnp.cos(row_angle), 0.0),
        jnp.where(by_row, 0.0, jnp.cos(col_angle)),
        jnp.where(by_row, jnp.sin(row_angle) * sign, 0.0),
        jnp.where(by_row, 0.0, jnp.sin(col_angle) * sign),
    )


def whole_layer(
    queries, keys, values, residual, out_proj, query_gain, key_gain, norm_gain,
    routes, route_weight, gate, up, down, shared_gate, shared_up, shared_down, cap,
):
    n_sp, n_tp = lax.axis_size("sp"), lax.axis_size("tp")
    tok, width = keys.shape
    lanes = queries.shape[1]
    group = lanes // width
    rows, model = residual.shape
    planes, chunks = 4, 4
    wide = model // chunks
    inner = gate.shape[2]
    tables = small_tables(tok, width)
    anywhere = pl.BlockSpec(memory_space=pl.ANY)
    dma = pltpu.SemaphoreType.DMA
    low, full = jnp.bfloat16, jnp.float32
    small = (
        *tables, query_gain.reshape(1, width), key_gain.reshape(1, width),
        norm_gain.reshape(1, model), routes.T, route_weight.T,
    )
    return pl.pallas_call(
        functools.partial(layer_kernel, n_sp, n_tp, planes, cap, chunks),
        out_shape=jax.ShapeDtypeStruct((rows, model), low),
        in_specs=[anywhere] * 20,
        out_specs=anywhere,
        scratch_shapes=[pltpu.VMEM(a.shape, a.dtype) for a in small] + [
            pltpu.VMEM(queries.shape, low),
            pltpu.VMEM(keys.shape, low),
            pltpu.VMEM(residual.shape, low),
            pltpu.VMEM(out_proj.shape, low),
            pltpu.VMEM((2,) + gate.shape[1:], low),
            pltpu.VMEM((2,) + up.shape[1:], low),
            pltpu.VMEM((2,) + down.shape[1:], low),
            pltpu.VMEM(shared_gate.shape, low),
            pltpu.VMEM(shared_up.shape, low),
            pltpu.VMEM(shared_down.shape, low),
            pltpu.VMEM((tok, width), full),
            pltpu.VMEM((tok, width), full),
            pltpu.VMEM((planes, 2, 2, tok, width), low),
            pltpu.VMEM((n_tp, group * rows, width), low),
            pltpu.VMEM((n_tp, group * rows, width), full),
            pltpu.VMEM((n_tp, group * rows, width), full),
            pltpu.VMEM((n_tp, group * rows, width), full),
            pltpu.VMEM((n_tp, rows, lanes), low),
            pltpu.VMEM((n_tp, rows, lanes), low),
            pltpu.VMEM((rows, model), low),
            pltpu.VMEM((planes, 2 * routes.shape[1], rows), full),
            pltpu.VMEM((planes, chunks, rows, wide), low),
            pltpu.VMEM((planes, chunks, 3, 2, cap, wide), low),
            pltpu.VMEM((planes, chunks, 2, 4, cap, wide), low),
            pltpu.VMEM((planes, chunks, 4, 2, cap, wide), low),
            pltpu.VMEM((planes, chunks, rows, wide), low),
            pltpu.VMEM((3, chunks, rows, wide), low),
            pltpu.VMEM((2, chunks, rows, wide), low),
            pltpu.VMEM((planes, 8 * cap, rows), low),
            pltpu.VMEM((planes, rows, 8 * cap), low),
            pltpu.VMEM((planes, 2, 4 * cap, 2 * inner), full),
            pltpu.VMEM((planes, 2, 4 * cap, inner), low),
            pltpu.VMEM((rows, model), full),
            pltpu.VMEM((rows, model), low),
            dma((11,)), dma((9,)), dma((chunks,)), dma((5, planes)), dma((5, planes)),
            dma((n_tp,)), dma((n_tp,)), dma((3,)), dma((3,)),
            dma((planes,)), dma((planes,)),
            dma((5, chunks)), dma((planes, chunks)),
            dma((planes, chunks, 4)), dma((planes, chunks, 4)),
            dma((planes, chunks, 4)), dma((planes, chunks, 4)),
            dma((3, chunks)), dma((3, chunks)), dma((2, chunks)),
        ],
        compiler_params=pltpu.CompilerParams(
            collective_id=2, has_side_effects=True, vmem_limit_bytes=61 * 2**20
        ),
        name="layer",
    )(
        *small,
        queries, keys, values, residual, out_proj,
        gate, up, down, shared_gate, shared_up, shared_down,
    )


def body(
    queries,
    keys,
    values,
    residual,
    out_proj,
    query_gain,
    key_gain,
    norm_gain,
    routes,
    route_weight,
    expert_gate,
    expert_up,
    expert_down,
    shared_gate,
    shared_up,
    shared_down,
):
    n_sp, n_tp = lax.axis_size("sp"), lax.axis_size("tp")
    rows_local, top_count = routes.shape
    expert_total = expert_gate.shape[0] * n_sp * n_tp
    capacity = max(2, 2 * rows_local * top_count // expert_total)
    if n_sp == 8 and n_tp == 4 and expert_gate.shape[0] == 1 and capacity % 16 == 0:
        return whole_layer(
            queries, keys, values, residual, out_proj, query_gain, key_gain, norm_gain,
            routes, route_weight, expert_gate, expert_up, expert_down,
            shared_gate, shared_up, shared_down, capacity,
        )
    all_heads = attention(n_sp, n_tp, queries, keys, values, query_gain, key_gain)
    projected = jnp.dot(all_heads, out_proj, preferred_element_type=jnp.float32)
    hidden1 = (residual.astype(jnp.float32) + projected).astype(jnp.bfloat16)
    hidden_f = hidden1.astype(jnp.float32)
    normed = (
        hidden_f
        * lax.rsqrt(jnp.mean(hidden_f * hidden_f, axis=-1, keepdims=True) + EPS)
        * norm_gain
    ).astype(jnp.bfloat16)
    pair_count = rows_local * top_count
    flat_routes = routes.reshape(pair_count)
    one_hot = (flat_routes[:, None] == jnp.arange(expert_total, dtype=jnp.int32)[None, :]).astype(
        jnp.float32
    )
    lower = (jnp.arange(pair_count)[:, None] >= jnp.arange(pair_count)[None, :]).astype(jnp.float32)
    running_count = jnp.dot(lower, one_hot, precision=lax.Precision.HIGHEST)
    slot_place = (jnp.sum(running_count * one_hot, axis=1) - 1.0).astype(jnp.int32)
    slot_index = flat_routes * capacity + slot_place
    slots = slot_index.reshape(rows_local, top_count).astype(jnp.float32)
    info = jnp.concatenate([slots.T, route_weight.T], axis=0)
    layer_out = routed_experts(
        info, normed, hidden1, expert_gate, expert_up, expert_down,
        shared_gate, shared_up, shared_down, capacity,
    )
    return layer_out.astype(jnp.bfloat16)


def solution(mesh):
    placed = (
        P("sp", "tp"),
        P("sp", "tp"),
        P("sp", "tp"),
        P(("sp", "tp"), None),
        P(),
        P(),
        P(),
        P(),
        P(("sp", "tp"), None),
        P(("sp", "tp"), None),
        P(("sp", "tp"), None, None),
        P(("sp", "tp"), None, None),
        P(("sp", "tp"), None, None),
        P(),
        P(),
        P(),
    )
    return jax.shard_map(
        body, mesh=mesh, in_specs=placed, out_specs=P(("sp", "tp"), None), check_vma=False
    )
```
